256 devices in a mesh: kv: 64 (over z, y, core), tp: 4 (over x).
Axes of the slice: x: 4, y: 4, z: 8, core: 2. Of those that a mesh axis runs over, the one named last changes fastest.
Arguments:
- queries: bfloat16 [24576, 2048], P('kv', 'tp'), may hold values from -3 to 3
- key_heads: bfloat16 [24576, 512], P('kv', 'tp'), may hold values from -3 to 3
- values: bfloat16 [24576, 512], P('kv', 'tp'), may hold values from -6 to 6
- log_sums: float32 [32, 24576], P('tp', 'kv'), may hold values from 4 to 6
- out_grad: bfloat16 [24576, 2048], P('kv', 'tp'), may hold values from -12 to 12
- inputs: bfloat16 [24576, 4096], P('kv', 'tp'), may hold values from -0.059814453 to 0.059814453
- chosen: int32 [8, 384, 16], P('tp'), may hold values from -1 to 383, as said below
Outputs:
- query_grad: float32 [24576, 2048], P('kv', 'tp')
- key_grad: float32 [24576, 512], P('kv', 'tp')
- value_grad: float32 [24576, 512], P('kv', 'tp')
- weight_grad: float32 [4096, 512], P('kv', 'tp')
The draws below stay inside these ranges and needn't reach their ends.
Inputs may be any that keep to these rules, and one draw needn't show every extreme that they name: `chosen`: for each key-value head and query block the used entries come first, are distinct, and none is above the query block's own number; -1 fills the rest. Up to 16 entries are used, all of them in some query blocks. For one key-value head, the query blocks held by one index of kv list at most one block of each other index of kv, and every index of kv but the first lists a block of the first.
All inputs are finite; a program needn't handle non-finite values.
Results may differ from the reference program's by a relative error of at most 0.014.
Values may be sent and summed in bfloat16 or wider, within the bound.
A program may use at most 128 MiB of HBM per device.

```python
import jax
import jax.numpy as jnp
from jax import lax

D = 4096
HEADS = 32
KV_HEADS = 8
HD = 64
BLOCK = 64
CHOSEN = 16
TOK_DEV = 384
TOKENS = 24576


def draw_chosen(key, part):
    per_device = TOK_DEV // BLOCK
    devices = TOKENS // TOK_DEV
    total_blocks = TOKENS // BLOCK
    subkeys = jax.random.split(jax.random.fold_in(key, 17), 4)
    designated = jax.random.randint(subkeys[0], (KV_HEADS, devices, devices), 0, per_device)
    requester_pos = jnp.arange(devices)[None, :, None]
    owner_pos = jnp.arange(devices)[None, None, :]
    designated = jnp.where(owner_pos == 0, 0, designated)
    designated = jnp.where(owner_pos == requester_pos - 1, per_device - 1, designated)
    query_block = jnp.arange(total_blocks)[:, None]
    other_block = jnp.arange(total_blocks)[None, :]
    requester = query_block // per_device
    owner_of = other_block // per_device
    within_dev = other_block % per_device
    chosen_here = designated[:, requester, owner_of]
    remote_ok = (owner_of < requester)[None] & (within_dev[None] == chosen_here)
    local_ok = ((owner_of == requester) & (other_block <= query_block))[None]
    allowed = remote_ok | local_ok
    last_local = query_block % per_device == per_device - 1
    forced = (other_block == 0) | (other_block == query_block) | (other_block == query_block - 1)
    forced = forced | (owner_of == requester - devices // 2) & last_local
    forced = forced[None] & allowed
    popularity = jax.random.randint(subkeys[1], (KV_HEADS, 1, total_blocks), 0, 4)
    noise_bits = jax.random.randint(subkeys[2], (KV_HEADS, total_blocks, total_blocks), 0, 65536)
    level = jnp.where(forced, 7, popularity)
    ranking = jnp.where(allowed, (level * 65536 + noise_bits) * total_blocks + other_block[None], -1 - other_block[None])
    top_score, top_index = lax.top_k(ranking, CHOSEN)
    list_length = CHOSEN // 2 + jax.random.randint(subkeys[3], (KV_HEADS, total_blocks, 1), 0, CHOSEN - CHOSEN // 2 + 1)
    list_length = jnp.where(last_local[None], CHOSEN, list_length)
    slot_pos = jnp.arange(CHOSEN)[None, None, :]
    keep_slot = (slot_pos < list_length) & (top_score >= 0)
    return jnp.where(keep_slot, top_index, -1).astype(jnp.int32)


def shard_levels(key, extent, cuts, smallest, high):
    gain, own = 1.0, jax.random.fold_in(key, 6)
    for axis_at, parts in cuts:
        heights = jnp.exp(jax.random.uniform(jax.random.fold_in(own, axis_at), (parts,), jnp.float32, smallest / len(cuts), high / len(cuts)))
        gain = gain * jnp.repeat(heights, extent[axis_at] // parts).reshape([-1 if axis == axis_at else 1 for axis in range(len(extent))])
    return gain


def normal_values(stream_key, extent, deviation, most, cuts=(), kind=jnp.bfloat16):
    loudness = shard_levels(stream_key, extent, cuts, -0.22, 0.18) if cuts else 1.0
    array = jax.random.normal(stream_key, extent, jnp.float32) * deviation * loudness
    return jnp.minimum(jnp.maximum(array, -most), most).astype(kind)


def setup_inputs(seed: int = 0) -> dict:
    splits = jax.random.split(jax.random.key(seed), 8)
    queries = normal_values(splits[0], (TOKENS, HEADS * HD), 1.0, 3.0, ((0, 64), (1, 4)))
    key_heads = normal_values(splits[1], (TOKENS, KV_HEADS * HD), 1.0, 3.0, ((0, 64), (1, 4)))
    values = normal_values(splits[2], (TOKENS, KV_HEADS * HD), 1.0, 6.0, ((0, 64), (1, 4)))
    log_sums = jnp.clip(4.0 + 2.0 * jax.random.uniform(splits[3], (HEADS, TOKENS), jnp.float32) ** shard_levels(splits[3], (HEADS, TOKENS), ((0, 4), (1, 64)), -0.2, 0.2), 4.0, 6.0)
    out_grad = normal_values(splits[4], (TOKENS, HEADS * HD), 2.0, 12.0, ((0, 64), (1, 4)))
    inputs = normal_values(splits[5], (TOKENS, D), 0.01, 0.059814453, ((0, 64), (1, 4)))
    chosen = draw_chosen(jax.random.fold_in(splits[7], 71), 0)
    return {"queries": queries, "key_heads": key_heads, "values": values, "log_sums": log_sums, "out_grad": out_grad, "inputs": inputs, "chosen": chosen}


def reference(queries, key_heads, values, log_sums, out_grad, inputs, chosen):
    total_blocks = TOKENS // BLOCK
    per_group = HEADS // KV_HEADS
    scaling = HD ** -0.5
    kv_pairs = jnp.concatenate(
        [key_heads.reshape(TOKENS, KV_HEADS, HD), values.reshape(TOKENS, KV_HEADS, HD)], axis=2
    ).reshape(total_blocks, BLOCK, KV_HEADS, 2 * HD)
    group_col = jnp.arange(KV_HEADS, dtype=jnp.int32)[:, None]
    offsets = jnp.arange(BLOCK, dtype=jnp.int32)

    def one_block(totals, block_pos):
        block_list = lax.dynamic_index_in_dim(chosen, block_pos, 1, keepdims=False)
        list_valid = block_list >= 0
        safe_list = jnp.maximum(block_list, 0)
        fetched = kv_pairs[safe_list, :, group_col, :].reshape(KV_HEADS, CHOSEN * BLOCK, 2 * HD)
        fetched = fetched.astype(jnp.float32)
        key_part = fetched[..., :HD]
        value_part = fetched[..., HD:]
        first_row = block_pos * BLOCK
        query_part = lax.dynamic_slice_in_dim(queries, first_row, BLOCK, 0)
        query_part = query_part.reshape(BLOCK, KV_HEADS, per_group, HD).astype(jnp.float32)
        grad_part = lax.dynamic_slice_in_dim(out_grad, first_row, BLOCK, 0)
        grad_part = grad_part.reshape(BLOCK, KV_HEADS, per_group, HD).astype(jnp.float32)
        sums_part = lax.dynamic_slice_in_dim(log_sums, first_row, BLOCK, 1).reshape(KV_HEADS, per_group, BLOCK)
        scores = jnp.einsum("igrd,gkd->grik", query_part, key_part) * scaling
        key_pos = (safe_list[:, :, None] * BLOCK + offsets).reshape(KV_HEADS, CHOSEN * BLOCK)
        key_valid = jnp.repeat(list_valid, BLOCK, axis=1)
        query_pos = first_row + offsets
        visible = key_valid[:, None, None, :] & (key_pos[:, None, None, :] <= query_pos[None, None, :, None])
        prob_rows = jnp.where(visible, jnp.exp(scores - sums_part[..., None]), 0.0)
        prob_grad = jnp.einsum("igrd,gkd->grik", grad_part, value_part)
        row_delta = jnp.sum(prob_rows * prob_grad, axis=-1, keepdims=True)
        score_grad = prob_rows * (prob_grad - row_delta)
        prob_half = prob_rows.astype(jnp.bfloat16).astype(jnp.float32)
        score_half = score_grad.astype(jnp.bfloat16).astype(jnp.float32)
        query_part_grad = jnp.einsum("grik,gkd->igrd", score_half, key_part) * scaling
        key_contrib = jnp.einsum("grik,igrd->gkd", score_half, query_part) * scaling
        value_contrib = jnp.einsum("grik,igrd->gkd", prob_half, grad_part)
        contribs = jnp.concatenate([key_contrib, value_contrib], axis=2).reshape(KV_HEADS, CHOSEN, BLOCK, 2 * HD)
        totals = totals.at[safe_list, :, group_col, :].add(contribs)
        return totals, query_part_grad.reshape(BLOCK, HEADS * HD)

    start_totals = jnp.zeros((total_blocks, BLOCK, KV_HEADS, 2 * HD), jnp.float32)
    totals, query_blocks = lax.scan(one_block, start_totals, jnp.arange(total_blocks, dtype=jnp.int32))
    query_grad = query_blocks.reshape(TOKENS, HEADS * HD)
    totals = totals.reshape(TOKENS, KV_HEADS, 2 * HD)
    key_grad = totals[..., :HD].reshape(TOKENS, KV_HEADS * HD)
    value_grad = totals[..., HD:].reshape(TOKENS, KV_HEADS * HD)
    weight_grad = jnp.dot(inputs.T, key_grad.astype(jnp.bfloat16), preferred_element_type=jnp.float32)
    return (query_grad, key_grad, value_grad, weight_grad)
```

```python
import functools

import jax
import jax.numpy as jnp
from jax import lax
from jax.experimental import pallas as pl
from jax.experimental.pallas import tpu as pltpu
from jax.sharding import PartitionSpec as P

HD = 64
BLOCK = 64
NEG = -1e30


def attention_kernel(
    slots, kinds, table, keys, vals, queries, out_grad, lse,
    query_grad, remote_tot, own_tot,
    tab, tot, bias, k_cat, v_cat, s_scr, dp_scr, p16, ds16, dk, dv,
    *, n_dev, n_blocks, n_list, per_group, groups,
):
    cols = per_group * BLOCK
    n_keys = n_list * BLOCK
    lane = lax.broadcasted_iota(jnp.int32, (BLOCK, 128), 1)
    tab[:n_dev] = table[...]
    for b in range(n_blocks):
        tab[n_dev + b, 0] = keys[b * BLOCK : (b + 1) * BLOCK, :]
        tab[n_dev + b, 1] = vals[b * BLOCK : (b + 1) * BLOCK, :]
    key_at = lax.broadcasted_iota(jnp.int32, (BLOCK, cols), 0)
    tok_at = lax.broadcasted_iota(jnp.int32, (BLOCK, cols), 1) % BLOCK
    bias[0] = jnp.zeros((BLOCK, cols), jnp.float32)
    bias[1] = jnp.where(key_at <= tok_at, 0.0, NEG)
    bias[2] = jnp.full((BLOCK, cols), NEG, jnp.float32)

    def clear(j, c):
        tot[j] = jnp.zeros((2, BLOCK, 128), jnp.float32)
        return c

    lax.fori_loop(0, n_dev + n_blocks, clear, 0)

    def masked_rows(ref, row, g, factor):
        mine = (lane >= HD) if g else (lane < HD)
        parts = []
        for r in range(per_group):
            col = (g * per_group + r) * HD
            tile = ref[pl.ds(row, BLOCK), col // 128 * 128 : col // 128 * 128 + 128]
            tile = tile.astype(jnp.float32) * factor
            if (r % 2) != g:
                tile = pltpu.roll(tile, HD, 1)
            parts.append(jnp.where(mine, tile, 0.0).astype(jnp.bfloat16))
        return jnp.concatenate(parts, axis=0)

    def one_position(p, c):
        row = pl.multiple_of(p * BLOCK, BLOCK)
        for g in range(groups):
            unit = p * groups + g
            q_rows = masked_rows(queries, row, g, HD ** -0.5)
            g_rows = masked_rows(out_grad, row, g, 1.0)
            for n in range(n_list):
                slot = slots[unit * n_list + n]
                k_cat[n * BLOCK : (n + 1) * BLOCK, :] = tab[slot, 0]
                v_cat[n * BLOCK : (n + 1) * BLOCK, :] = tab[slot, 1]
            nt = (((1,), (1,)), ((), ()))
            s_scr[...] = lax.dot_general(k_cat[...], q_rows, nt, preferred_element_type=jnp.float32)
            dp_scr[...] = lax.dot_general(v_cat[...], g_rows, nt, preferred_element_type=jnp.float32)
            lse_row = lse[pl.ds(unit, 1), :]

            def probs(n, acc):
                at = pl.ds(pl.multiple_of(n * BLOCK, BLOCK), BLOCK)
                pr = jnp.exp((s_scr[at, :] - lse_row) + bias[kinds[unit * n_list + n]])
                s_scr[at, :] = pr
                p16[at, :] = pr.astype(jnp.bfloat16)
                return acc + (pr * dp_scr[at, :]).reshape(BLOCK // 8, 8, cols).sum(axis=0)

            acc = lax.fori_loop(0, n_list, probs, jnp.zeros((8, cols), jnp.float32), unroll=4)
            delta = acc.sum(axis=0, keepdims=True)

            def grads(n, carry):
                at = pl.ds(pl.multiple_of(n * BLOCK, BLOCK), BLOCK)
                ds16[at, :] = (s_scr[at, :] * (dp_scr[at, :] - delta)).astype(jnp.bfloat16)
                return carry

            lax.fori_loop(0, n_list, grads, 0, unroll=4)
            nn = (((1,), (0,)), ((), ()))
            dk[...] = lax.dot_general(ds16[...], q_rows, nn, preferred_element_type=jnp.float32)
            dv[...] = lax.dot_general(p16[...], g_rows, nn, preferred_element_type=jnp.float32)
            dq_t = lax.dot_general(
                k_cat[...], ds16[...], (((0,), (0,)), ((), ())), preferred_element_type=jnp.float32
            )
            dq = dq_t.T * (HD ** -0.5)

            def spread(n, carry):
                at = pl.ds(pl.multiple_of(n * BLOCK, BLOCK), BLOCK)
                slot = slots[unit * n_list + n]
                tot[slot, 0] += dk[at, :]
                tot[slot, 1] += dv[at, :]
                return carry

            lax.fori_loop(0, n_list, spread, 0, unroll=2)
            for pair in range(per_group // 2):
                even = dq[(2 * pair) * BLOCK : (2 * pair + 1) * BLOCK]
                odd = dq[(2 * pair + 1) * BLOCK : (2 * pair + 2) * BLOCK]
                if g:
                    even = pltpu.roll(even, HD, 1)
                else:
                    odd = pltpu.roll(odd, HD, 1)
                col = g * per_group * HD + pair * 128
                query_grad[pl.ds(row, BLOCK), col : col + 128] = jnp.where(lane < HD, even, odd)
        return c

    lax.fori_loop(0, n_blocks, one_position, 0)

    def put(j, c):
        remote_tot[j] = tot[j].astype(jnp.bfloat16)
        return c

    lax.fori_loop(0, n_dev, put, 0)
    own_tot[...] = tot[n_dev:]


def attention(slots, kinds, table, keys, vals, queries, out_grad, lse, *, n_list):
    n_dev = table.shape[0]
    rows = keys.shape[0]
    n_blocks = rows // BLOCK
    groups = keys.shape[1] // HD
    per_group = queries.shape[1] // HD // groups
    cols = per_group * BLOCK
    n_keys = n_list * BLOCK
    vm = pl.BlockSpec(memory_space=pltpu.VMEM)
    sm = pl.BlockSpec(memory_space=pltpu.SMEM)
    f32, bf16 = jnp.float32, jnp.bfloat16
    return pl.pallas_call(
        functools.partial(
            attention_kernel, n_dev=n_dev, n_blocks=n_blocks, n_list=n_list,
            per_group=per_group, groups=groups,
        ),
        out_shape=(
            jax.ShapeDtypeStruct(queries.shape, f32),
            jax.ShapeDtypeStruct((n_dev, 2, BLOCK, 128), bf16),
            jax.ShapeDtypeStruct((n_blocks, 2, BLOCK, 128), f32),
        ),
        in_specs=[sm, sm] + [vm] * 6,
        out_specs=(vm, vm, vm),
        scratch_shapes=[
            pltpu.VMEM((n_dev + n_blocks, 2, BLOCK, 128), bf16),
            pltpu.VMEM((n_dev + n_blocks, 2, BLOCK, 128), f32),
            pltpu.VMEM((3, BLOCK, cols), f32),
            pltpu.VMEM((n_keys, 128), bf16),
            pltpu.VMEM((n_keys, 128), bf16),
            pltpu.VMEM((n_keys, cols), f32),
            pltpu.VMEM((n_keys, cols), f32),
            pltpu.VMEM((n_keys, cols), bf16),
            pltpu.VMEM((n_keys, cols), bf16),
            pltpu.VMEM((n_keys, 128), f32),
            pltpu.VMEM((n_keys, 128), f32),
        ],
        compiler_params=pltpu.CompilerParams(vmem_limit_bytes=48 * 1024 * 1024),
        cost_estimate=pl.CostEstimate(
            flops=10 * n_blocks * groups * n_keys * cols * 128,
            bytes_accessed=8 * 1024 * 1024,
            transcendentals=n_blocks * groups * n_keys * cols,
        ),
        name="attention",
    )(slots, kinds, table, keys, vals, queries, out_grad, lse)


def sum_at_owner(array, axis):
    count = lax.axis_size(axis)
    pieces = array.reshape(count, array.shape[0] // count, array.shape[1])
    arrived = lax.all_to_all(pieces, axis, split_axis=0, concat_axis=0, tiled=True)
    return arrived.astype(jnp.float32).sum(axis=0)


def local(queries, key_heads, values, log_sums, out_grad, inputs, chosen):
    n_dev = lax.axis_size("kv")
    me = lax.axis_index("kv")
    rows = queries.shape[0]
    n_blocks = rows // BLOCK
    groups = key_heads.shape[1] // HD
    per_group = log_sums.shape[0] // groups
    n_list = chosen.shape[2]

    my_lists = lax.dynamic_slice_in_dim(chosen, me * n_blocks, n_blocks, 1)
    owner = my_lists // n_blocks
    slot = jnp.where(owner == me, n_dev + my_lists % n_blocks, jnp.maximum(owner, 0))
    kind = jnp.where(
        my_lists < 0,
        2,
        (my_lists == me * n_blocks + jnp.arange(n_blocks)[None, :, None]).astype(jnp.int32),
    )
    slots = slot.transpose(1, 0, 2).reshape(-1)
    kinds = kind.transpose(1, 0, 2).reshape(-1)
    lse = log_sums.reshape(groups, per_group, n_blocks, BLOCK).transpose(2, 0, 1, 3)
    lse = lse.reshape(n_blocks * groups, per_group * BLOCK)

    entries = chosen.reshape(groups, n_dev, n_blocks * n_list)
    rel = entries - me * n_blocks
    mine = (rel >= 0) & (rel < n_blocks)
    sel = jnp.max(jnp.where(mine, rel, -1), axis=2)
    sel = jnp.where(jnp.arange(n_dev)[None] == me, -1, sel)
    sel_lane = jnp.repeat(sel.T, HD, axis=1)[:, None, None, :]
    own = jnp.stack([key_heads.reshape(n_blocks, BLOCK, -1), values.reshape(n_blocks, BLOCK, -1)], axis=1)
    outgoing = jnp.zeros((n_dev,) + own.shape[1:], jnp.bfloat16)
    for b in range(n_blocks):
        outgoing = jnp.where(sel_lane == b, own[b][None], outgoing)
    table = lax.all_to_all(outgoing, "kv", split_axis=0, concat_axis=0, tiled=True)

    query_grad, remote_tot, own_tot = attention(
        slots, kinds, table, key_heads, values, queries, out_grad, lse, n_list=n_list
    )
    returned = lax.all_to_all(remote_tot, "kv", split_axis=0, concat_axis=0, tiled=True)
    returned = returned.astype(jnp.float32)
    total = [
        own_tot[b] + jnp.sum(jnp.where(sel_lane == b, returned, 0.0), axis=0) for b in range(n_blocks)
    ]
    total = jnp.stack(total, axis=0)
    key_grad = total[:, 0].reshape(rows, -1)
    value_grad = total[:, 1].reshape(rows, -1)
    whole_inputs = lax.all_gather(inputs, "tp", axis=1, tiled=True)
    weight_grad = sum_at_owner(
        lax.dot_general(
            whole_inputs, key_grad.astype(jnp.bfloat16), (((0,), (0,)), ((), ())),
            preferred_element_type=jnp.float32,
        ).astype(jnp.bfloat16),
        "kv",
    )
    return (query_grad, key_grad, value_grad, weight_grad)


def solution(mesh):
    placed = (
        P("kv", "tp"),
        P("kv", "tp"),
        P("kv", "tp"),
        P("tp", "kv"),
        P("kv", "tp"),
        P("kv", "tp"),
        P("tp", None, None),
    )
    return jax.shard_map(
        local,
        mesh=mesh,
        in_specs=placed,
        out_specs=(P("kv", "tp"), P("kv", "tp"), P("kv", "tp"), P("kv", "tp")),
        check_vma=False,
    )
```

```python
import functools

import jax
import jax.numpy as jnp
from jax import lax
from jax.experimental import pallas as pl
from jax.experimental.pallas import tpu as pltpu
from jax.sharding import PartitionSpec as P

HD = 64
BLOCK = 64
NEG = -1e30


N_Y = 4
N_C = 2
PLANE = N_Y * N_C
MESH = pl.DeviceIdType.MESH


def place():
    me = lax.axis_index("kv")
    return me // PLANE, me % PLANE


def greet(partners):
    barrier = pltpu.get_barrier_semaphore()
    for who in partners:
        pl.semaphore_signal(barrier, inc=1, device_id=who, device_id_type=MESH)
    pl.semaphore_wait(barrier, len(partners))


def gather_kernel(
    sel, keys, vals, inputs, table, others,
    u1, u2, u3, u4, w1, w2, w3, picked,
    z_send, z_recv, y_send, y_recv, x_send, x_recv,
    *, n_z, n_x,
):
    z, q = place()
    x = lax.axis_index("tp")
    half = inputs.shape[0] // 2
    up_z = {"kv": (z + 1) % n_z * PLANE + q}
    dn_z = {"kv": (z + n_z - 1) % n_z * PLANE + q}
    right = {"tp": (x + 1) % n_x}
    left = {"tp": (x + n_x - 1) % n_x}
    plane = [{"kv": z * PLANE + (q + r) % PLANE} for r in range(1, PLANE)]
    greet([up_z, dn_z, right, left] + plane)

    ups = [None, u1, u2, u3, u4]
    downs = [None, w1, w2, w3]
    own = (keys, vals)

    def source(held, step, part):
        return own[part] if step == 0 else held[step].at[part]

    def z_copy(way, step, part):
        held, who = (ups, up_z) if way == 0 else (downs, dn_z)
        return pltpu.make_async_remote_copy(
            src_ref=source(held, step - 1, part),
            dst_ref=held[step].at[part],
            send_sem=z_send.at[way, step, part],
            recv_sem=z_recv.at[way, step, part],
            device_id=who,
            device_id_type=MESH,
        )

    def sends_up(step):
        return (z < n_z - 1) & (z - step + 1 >= 0)

    def gets_up(step):
        return z - step >= 0

    def sends_down(step):
        return (z + step - 1) % n_z < 3

    def gets_down(step):
        return (z + step) % n_z < 3

    def x_copy(to_right, rel, part):
        rows = pl.ds(part * half, half)
        slot = rel - 1 if to_right else n_x - 1 - rel
        src = inputs.at[rows] if rel == 1 else others.at[0 if to_right else n_x - 2, rows]
        return pltpu.make_async_remote_copy(
            src_ref=src,
            dst_ref=others.at[slot, rows],
            send_sem=x_send.at[0 if to_right else 1, rel, part],
            recv_sem=x_recv.at[0 if to_right else 1, rel, part],
            device_id=right if to_right else left,
            device_id_type=MESH,
        )

    @pl.when(sends_up(1))
    def _():
        z_copy(0, 1, 0).start()
        z_copy(0, 1, 1).start()

    @pl.when(sends_down(1))
    def _():
        z_copy(1, 1, 0).start()
        z_copy(1, 1, 1).start()

    for part in range(2):
        x_copy(True, 1, part).start()
        x_copy(False, 1, 1 - part).start()

    lane = lax.broadcasted_iota(jnp.int32, (BLOCK, 128), 1)

    def y_copy(order, z_from, r):
        to = (q + r) % PLANE
        return pltpu.make_async_remote_copy(
            src_ref=picked.at[order, r],
            dst_ref=table.at[z_from * PLANE + q],
            send_sem=y_send.at[order, r],
            recv_sem=y_recv.at[order, q],
            device_id={"kv": z * PLANE + to},
            device_id_type=MESH,
        )

    def pick(order, z_from, held):
        def chosen_rows(to, part):
            at = (z_from * PLANE + to) * 2
            ref = own[part] if held is None else held
            halves = []
            for g in range(2):
                b = sel[at + g]
                halves.append(ref[b] if held is None else ref[part, b])
            return jnp.where(lane < HD, halves[0], halves[1])

        def one(r, c):
            for part in range(2):
                picked[order, r, part] = chosen_rows((q + r) % PLANE, part)

            @pl.when(r > 1)
            def _():
                y_copy(order, z_from, r - 1).start()

            return c

        lax.fori_loop(1, PLANE, one, 0)
        for part in range(2):
            table[z_from * PLANE + q, part] = chosen_rows(q, part)
        y_copy(order, z_from, PLANE - 1).start()

    pick(0, z, None)
    for step in range(1, 5):
        for part in range(2):
            @pl.when(gets_up(step))
            def _():
                z_copy(0, step, part).wait_recv()

            if step < 4:
                @pl.when(sends_up(step + 1))
                def _():
                    z_copy(0, step + 1, part).start()

                @pl.when(gets_down(step))
                def _():
                    z_copy(1, step, part).wait_recv()

                if step < 3:
                    @pl.when(sends_down(step + 1))
                    def _():
                        z_copy(1, step + 1, part).start()

        @pl.when(gets_up(step))
        def _():
            pick(step, z - step, ups[step])

        if step < 4:
            @pl.when(gets_down(step) & (z + step >= n_z))
            def _():
                pick(4 + step, z + step - n_z, downs[step])

        if step == 2:
            x_copy(True, 1, 0).wait_recv()
            x_copy(True, 2, 0).start()
            x_copy(False, 1, 1).wait_recv()
            x_copy(False, 2, 1).start()

    def each_order(act):
        act(0, z)
        for step in range(1, 5):
            @pl.when(gets_up(step))
            def _():
                act(step, z - step)

            if step < 4:
                @pl.when(gets_down(step) & (z + step >= n_z))
                def _():
                    act(4 + step, z + step - n_z)

    def drain(order, z_from):
        def one(r, c):
            frm = (q + r) % PLANE
            got = pltpu.make_async_remote_copy(
                src_ref=picked.at[order, r],
                dst_ref=table.at[z_from * PLANE + frm],
                send_sem=y_send.at[order, r],
                recv_sem=y_recv.at[order, frm],
                device_id={"kv": z * PLANE + frm},
                device_id_type=MESH,
            )
            got.wait_recv()
            got.wait_send()
            return c

        lax.fori_loop(1, PLANE, one, 0)

    each_order(drain)
    for step in range(1, 5):
        for part in range(2):
            @pl.when(sends_up(step))
            def _():
                z_copy(0, step, part).wait_send()

            if step < 4:
                @pl.when(sends_down(step))
                def _():
                    z_copy(1, step, part).wait_send()
    x_copy(True, 1, 1).wait_recv()
    x_copy(False, 1, 0).wait_recv()
    x_copy(True, 2, 0).wait_recv()
    x_copy(False, 2, 1).wait_recv()
    for part in range(2):
        x_copy(True, 1, part).wait_send()
        x_copy(False, 1, part).wait_send()
    x_copy(True, 2, 0).wait_send()
    x_copy(False, 2, 1).wait_send()


def gather(sel, keys, vals, inputs):
    n_dev = lax.axis_size("kv")
    n_x = lax.axis_size("tp")
    n_z = n_dev // PLANE
    bf16 = jnp.bfloat16
    vm = pl.BlockSpec(memory_space=pltpu.VMEM)
    hbm = pl.BlockSpec(memory_space=pl.ANY)
    dma = pltpu.SemaphoreType.DMA
    held = pltpu.VMEM((2,) + keys.shape, bf16)
    return pl.pallas_call(
        functools.partial(gather_kernel, n_z=n_z, n_x=n_x),
        out_shape=(
            jax.ShapeDtypeStruct((n_dev, 2, BLOCK, 128), bf16),
            jax.ShapeDtypeStruct((n_x - 1,) + inputs.shape, bf16),
        ),
        in_specs=[pl.BlockSpec(memory_space=pltpu.SMEM), vm, vm, hbm],
        out_specs=(vm, hbm),
        scratch_shapes=[held] * 7
        + [
            pltpu.VMEM((8, PLANE, 2, BLOCK, 128), bf16),
            dma((2, 5, 2)),
            dma((2, 5, 2)),
            dma((8, PLANE)),
            dma((8, PLANE)),
            dma((2, 3, 2)),
            dma((2, 3, 2)),
        ],
        compiler_params=pltpu.CompilerParams(
            collective_id=0, has_side_effects=True, vmem_limit_bytes=32 * 1024 * 1024
        ),
        name="gather",
    )(sel, keys, vals, inputs)


def attention_kernel(
    slots, kinds, table, keys, vals, queries, out_grad, lse,
    query_grad, remote_tot, own_tot,
    tab, tot, bias, k_cat, v_cat, s_scr, dp_scr, p16, ds16, dk, dv,
    *, n_dev, n_blocks, n_list, per_group, groups,
):
    cols = per_group * BLOCK
    n_keys = n_list * BLOCK
    lane = lax.broadcasted_iota(jnp.int32, (BLOCK, 128), 1)
    tab[:n_dev] = table[...]
    for b in range(n_blocks):
        tab[n_dev + b, 0] = keys[b * BLOCK : (b + 1) * BLOCK, :]
        tab[n_dev + b, 1] = vals[b * BLOCK : (b + 1) * BLOCK, :]
    key_at = lax.broadcasted_iota(jnp.int32, (BLOCK, cols), 0)
    tok_at = lax.broadcasted_iota(jnp.int32, (BLOCK, cols), 1) % BLOCK
    bias[0] = jnp.zeros((BLOCK, cols), jnp.float32)
    bias[1] = jnp.where(key_at <= tok_at, 0.0, NEG)
    bias[2] = jnp.full((BLOCK, cols), NEG, jnp.float32)

    def clear(j, c):
        tot[j] = jnp.zeros((2, BLOCK, 128), jnp.float32)
        return c

    lax.fori_loop(0, n_dev + n_blocks, clear, 0)

    def masked_rows(ref, row, g, factor):
        mine = (lane >= HD) if g else (lane < HD)
        parts = []
        for r in range(per_group):
            col = (g * per_group + r) * HD
            tile = ref[pl.ds(row, BLOCK), col // 128 * 128 : col // 128 * 128 + 128]
            tile = tile.astype(jnp.float32) * factor
            if (r % 2) != g:
                tile = pltpu.roll(tile, HD, 1)
            parts.append(jnp.where(mine, tile, 0.0).astype(jnp.bfloat16))
        return jnp.concatenate(parts, axis=0)

    def one_position(p, c):
        row = pl.multiple_of(p * BLOCK, BLOCK)
        for g in range(groups):
            unit = p * groups + g
            q_rows = masked_rows(queries, row, g, HD ** -0.5)
            g_rows = masked_rows(out_grad, row, g, 1.0)
            for n in range(n_list):
                slot = slots[unit * n_list + n]
                k_cat[n * BLOCK : (n + 1) * BLOCK, :] = tab[slot, 0]
                v_cat[n * BLOCK : (n + 1) * BLOCK, :] = tab[slot, 1]
            nt = (((1,), (1,)), ((), ()))
            s_scr[...] = lax.dot_general(k_cat[...], q_rows, nt, preferred_element_type=jnp.float32)
            dp_scr[...] = lax.dot_general(v_cat[...], g_rows, nt, preferred_element_type=jnp.float32)
            lse_row = lse[pl.ds(unit, 1), :]

            def probs(n, acc):
                at = pl.ds(pl.multiple_of(n * BLOCK, BLOCK), BLOCK)
                pr = jnp.exp((s_scr[at, :] - lse_row) + bias[kinds[unit * n_list + n]])
                s_scr[at, :] = pr
                p16[at, :] = pr.astype(jnp.bfloat16)
                return acc + (pr * dp_scr[at, :]).reshape(BLOCK // 8, 8, cols).sum(axis=0)

            acc = lax.fori_loop(0, n_list, probs, jnp.zeros((8, cols), jnp.float32), unroll=4)
            delta = acc.sum(axis=0, keepdims=True)

            def grads(n, carry):
                at = pl.ds(pl.multiple_of(n * BLOCK, BLOCK), BLOCK)
                ds16[at, :] = (s_scr[at, :] * (dp_scr[at, :] - delta)).astype(jnp.bfloat16)
                return carry

            lax.fori_loop(0, n_list, grads, 0, unroll=4)
            nn = (((1,), (0,)), ((), ()))
            dk[...] = lax.dot_general(ds16[...], q_rows, nn, preferred_element_type=jnp.float32)
            dv[...] = lax.dot_general(p16[...], g_rows, nn, preferred_element_type=jnp.float32)
            dq_t = lax.dot_general(
                k_cat[...], ds16[...], (((0,), (0,)), ((), ())), preferred_element_type=jnp.float32
            )
            dq = dq_t.T * (HD ** -0.5)

            def spread(n, carry):
                at = pl.ds(pl.multiple_of(n * BLOCK, BLOCK), BLOCK)
                slot = slots[unit * n_list + n]
                tot[slot, 0] += dk[at, :]
                tot[slot, 1] += dv[at, :]
                return carry

            lax.fori_loop(0, n_list, spread, 0, unroll=2)
            for pair in range(per_group // 2):
                even = dq[(2 * pair) * BLOCK : (2 * pair + 1) * BLOCK]
                odd = dq[(2 * pair + 1) * BLOCK : (2 * pair + 2) * BLOCK]
                if g:
                    even = pltpu.roll(even, HD, 1)
                else:
                    odd = pltpu.roll(odd, HD, 1)
                col = g * per_group * HD + pair * 128
                query_grad[pl.ds(row, BLOCK), col : col + 128] = jnp.where(lane < HD, even, odd)
        return c

    lax.fori_loop(0, n_blocks, one_position, 0)

    def put(j, c):
        remote_tot[j] = tot[j].astype(jnp.bfloat16)
        return c

    lax.fori_loop(0, n_dev, put, 0)
    own_tot[...] = tot[n_dev:]


def attention(slots, kinds, table, keys, vals, queries, out_grad, lse, *, n_list):
    n_dev = table.shape[0]
    rows = keys.shape[0]
    n_blocks = rows // BLOCK
    groups = keys.shape[1] // HD
    per_group = queries.shape[1] // HD // groups
    cols = per_group * BLOCK
    n_keys = n_list * BLOCK
    vm = pl.BlockSpec(memory_space=pltpu.VMEM)
    sm = pl.BlockSpec(memory_space=pltpu.SMEM)
    f32, bf16 = jnp.float32, jnp.bfloat16
    return pl.pallas_call(
        functools.partial(
            attention_kernel, n_dev=n_dev, n_blocks=n_blocks, n_list=n_list,
            per_group=per_group, groups=groups,
        ),
        out_shape=(
            jax.ShapeDtypeStruct(queries.shape, f32),
            jax.ShapeDtypeStruct((n_dev, 2, BLOCK, 128), bf16),
            jax.ShapeDtypeStruct((n_blocks, 2, BLOCK, 128), f32),
        ),
        in_specs=[sm, sm] + [vm] * 6,
        out_specs=(vm, vm, vm),
        scratch_shapes=[
            pltpu.VMEM((n_dev + n_blocks, 2, BLOCK, 128), bf16),
            pltpu.VMEM((n_dev + n_blocks, 2, BLOCK, 128), f32),
            pltpu.VMEM((3, BLOCK, cols), f32),
            pltpu.VMEM((n_keys, 128), bf16),
            pltpu.VMEM((n_keys, 128), bf16),
            pltpu.VMEM((n_keys, cols), f32),
            pltpu.VMEM((n_keys, cols), f32),
            pltpu.VMEM((n_keys, cols), bf16),
            pltpu.VMEM((n_keys, cols), bf16),
            pltpu.VMEM((n_keys, 128), f32),
            pltpu.VMEM((n_keys, 128), f32),
        ],
        compiler_params=pltpu.CompilerParams(vmem_limit_bytes=48 * 1024 * 1024),
        cost_estimate=pl.CostEstimate(
            flops=10 * n_blocks * groups * n_keys * cols * 128,
            bytes_accessed=8 * 1024 * 1024,
            transcendentals=n_blocks * groups * n_keys * cols,
        ),
        name="attention",
    )(slots, kinds, table, keys, vals, queries, out_grad, lse)


def sum_at_owner(array, axis):
    count = lax.axis_size(axis)
    pieces = array.reshape(count, array.shape[0] // count, array.shape[1])
    arrived = lax.all_to_all(pieces, axis, split_axis=0, concat_axis=0, tiled=True)
    return arrived.astype(jnp.float32).sum(axis=0)


def local(queries, key_heads, values, log_sums, out_grad, inputs, chosen):
    n_dev = lax.axis_size("kv")
    me = lax.axis_index("kv")
    rows = queries.shape[0]
    n_blocks = rows // BLOCK
    groups = key_heads.shape[1] // HD
    per_group = log_sums.shape[0] // groups
    n_list = chosen.shape[2]

    my_lists = lax.dynamic_slice_in_dim(chosen, me * n_blocks, n_blocks, 1)
    owner = my_lists // n_blocks
    slot = jnp.where(owner == me, n_dev + my_lists % n_blocks, jnp.maximum(owner, 0))
    kind = jnp.where(
        my_lists < 0,
        2,
        (my_lists == me * n_blocks + jnp.arange(n_blocks)[None, :, None]).astype(jnp.int32),
    )
    slots = slot.transpose(1, 0, 2).reshape(-1)
    kinds = kind.transpose(1, 0, 2).reshape(-1)
    lse = log_sums.reshape(groups, per_group, n_blocks, BLOCK).transpose(2, 0, 1, 3)
    lse = lse.reshape(n_blocks * groups, per_group * BLOCK)

    entries = chosen.reshape(groups, n_dev, n_blocks * n_list)
    rel = entries - me * n_blocks
    mine = (rel >= 0) & (rel < n_blocks)
    sel = jnp.max(jnp.where(mine, rel, -1), axis=2)
    sel = jnp.where(jnp.arange(n_dev)[None] == me, -1, sel)
    sel_lane = jnp.repeat(sel.T, HD, axis=1)[:, None, None, :]
    z, q = place()
    plane_lists = lax.dynamic_slice_in_dim(chosen, z * PLANE * n_blocks, PLANE * n_blocks, 1)
    own_col = (jnp.arange(n_dev // PLANE) * PLANE + q) * n_blocks
    offs = plane_lists[..., None] - own_col
    offs = jnp.where((offs >= 0) & (offs < n_blocks), offs, 0)
    picks = jnp.max(offs.reshape(groups, PLANE, n_blocks * n_list, -1), axis=2)
    picks = picks.transpose(2, 1, 0).reshape(-1)
    key_blocks = key_heads.reshape(n_blocks, BLOCK, -1)
    value_blocks = values.reshape(n_blocks, BLOCK, -1)
    table, others = gather(picks, key_blocks, value_blocks, inputs)

    query_grad, remote_tot, own_tot = attention(
        slots, kinds, table, key_heads, values, queries, out_grad, lse, n_list=n_list
    )
    returned = lax.all_to_all(remote_tot, "kv", split_axis=0, concat_axis=0, tiled=True)
    returned = returned.astype(jnp.float32)
    total = [
        own_tot[b] + jnp.sum(jnp.where(sel_lane == b, returned, 0.0), axis=0) for b in range(n_blocks)
    ]
    total = jnp.stack(total, axis=0)
    key_grad = total[:, 0].reshape(rows, -1)
    value_grad = total[:, 1].reshape(rows, -1)
    x, n_x = lax.axis_index("tp"), lax.axis_size("tp")
    key_half = key_grad.astype(jnp.bfloat16)
    parts = jnp.zeros((n_x, inputs.shape[1], key_half.shape[1]), jnp.bfloat16)
    for rel in range(n_x):
        piece = inputs if rel == 0 else others[rel - 1]
        part = lax.dot_general(
            piece, key_half, (((0,), (0,)), ((), ())), preferred_element_type=jnp.float32
        ).astype(jnp.bfloat16)
        parts = lax.dynamic_update_index_in_dim(parts, part, (x + n_x - rel) % n_x, 0)
    weight_grad = sum_at_owner(parts.reshape(-1, key_half.shape[1]), "kv")
    return (query_grad, key_grad, value_grad, weight_grad)


def solution(mesh):
    placed = (
        P("kv", "tp"),
        P("kv", "tp"),
        P("kv", "tp"),
        P("tp", "kv"),
        P("kv", "tp"),
        P("kv", "tp"),
        P("tp", None, None),
    )
    return jax.shard_map(
        local,
        mesh=mesh,
        in_specs=placed,
        out_specs=(P("kv", "tp"), P("kv", "tp"), P("kv", "tp"), P("kv", "tp")),
        check_vma=False,
    )
```

```python
import functools

import jax
import jax.numpy as jnp
from jax import lax
from jax.experimental import pallas as pl
from jax.experimental.pallas import tpu as pltpu
from jax.sharding import PartitionSpec as P

HD = 64
BLOCK = 64
NEG = -1e30
N_Y = 4
N_C = 2
PLANE = N_Y * N_C
MESH = pl.DeviceIdType.MESH
RETURN_ORDER = (4, 5, 3, 6, 2, 7, 1, 0)
F32, BF16 = jnp.float32, jnp.bfloat16


def place():
    me = lax.axis_index("kv")
    return me // PLANE, me % PLANE


def scratch_list(rows, n_dev, n_x, n_list, feats, heads):
    n_b = rows // BLOCK
    tile = (BLOCK, 128)
    cols = heads // 2 * BLOCK
    dma = pltpu.SemaphoreType.DMA
    out = [
        ("kraw", pltpu.VMEM((n_b,) + tile, BF16)),
        ("vraw", pltpu.VMEM((n_b,) + tile, BF16)),
        ("qraw", pltpu.VMEM((rows, heads * HD), BF16)),
        ("graw", pltpu.VMEM((rows, heads * HD), BF16)),
        ("lraw", pltpu.VMEM((heads, rows), F32)),
        ("xraw", pltpu.VMEM((n_x, rows, feats), BF16)),
        ("lse", pltpu.VMEM((n_b * 2, 1, cols), F32)),
        ("bias", pltpu.VMEM((3,) + (BLOCK, cols), F32)),
        ("picked", pltpu.VMEM((2, 8, PLANE) + tile, BF16)),
        ("qd", pltpu.VMEM((2 * cols, 128), BF16)),
        ("cat", pltpu.VMEM((n_list,) + tile, BF16)),
        ("sdp", pltpu.VMEM((n_list, BLOCK, 2 * cols), F32)),
        ("pd", pltpu.VMEM((n_list, BLOCK, 2 * cols), BF16)),
        ("terms", pltpu.VMEM((n_b, n_list + 1) + tile, F32)),
        ("ret", pltpu.VMEM((2, n_dev) + tile, BF16)),
        ("own_tot", pltpu.VMEM((2, n_b) + tile, F32)),
        ("back", pltpu.VMEM((2, 8, PLANE) + tile, BF16)),
        ("acc", pltpu.VMEM((2, n_b) + tile, F32)),
        ("zs", pltpu.VMEM((2, 8, n_b) + tile, BF16)),
        ("zr_dn", pltpu.VMEM((2, 4, n_b) + tile, BF16)),
        ("zr_up", pltpu.VMEM((2, 3, n_b) + tile, BF16)),
        ("kg", pltpu.VMEM((rows, 128), BF16)),
        ("wpart", pltpu.VMEM((8, N_C, N_Y) + tile, BF16)),
        ("crecv", pltpu.VMEM((8, N_Y) + tile, BF16)),
        ("wy", pltpu.VMEM((N_Y, 8) + tile, BF16)),
        ("wy_own", pltpu.VMEM((8,) + tile, F32)),
        ("wyr", pltpu.VMEM((N_Y, 8) + tile, BF16)),
        ("wz", pltpu.VMEM((8,) + tile, BF16)),
        ("wz_own", pltpu.VMEM((8,) + tile, F32)),
        ("wzr", pltpu.VMEM((8,) + tile, BF16)),
        ("in_sem", dma((6,))),
        ("z_send", dma((2, 2, 5))),
        ("z_recv", dma((2, 2, 5))),
        ("y_send", dma((2, 8, PLANE))),
        ("y_recv", dma((2, 8, PLANE))),
        ("x_send", dma((2, 3, 2))),
        ("x_recv", dma((2, 3, 2))),
        ("b_send", dma((2, 8, PLANE))),
        ("b_recv", dma((2, 8, PLANE))),
        ("r_send", dma((2, 8))),
        ("r_recv_dn", dma((2, 4))),
        ("r_recv_up", dma((2, 3))),
        ("c_send", dma((8,))),
        ("c_recv", dma((8,))),
        ("wy_send", dma((N_Y,))),
        ("wy_recv", dma((N_Y,))),
        ("wz_send", dma((8,))),
        ("wz_recv", dma((8,))),
    ]
    for g in range(2):
        out.append((f"own{g}", pltpu.VMEM((n_b,) + tile, BF16)))
        out.append((f"tab{g}", pltpu.VMEM((n_dev + n_b,) + tile, BF16)))
        for step in range(1, 5):
            out.append((f"held{g}0{step}", pltpu.VMEM((n_b,) + tile, BF16)))
        for step in range(1, 4):
            out.append((f"held{g}1{step}", pltpu.VMEM((n_b,) + tile, BF16)))
    return out


def fused_kernel(names, n_z, n_x, n_list, *refs):
    idx, keys, vals, queries, out_grad, log_sums, inputs = refs[:7]
    query_grad, key_grad, value_grad, weight_grad = refs[7:11]
    m = dict(zip(names, refs[11:]))
    n_b = m["kraw"].shape[0]
    n_dev = n_z * PLANE
    heads = m["lraw"].shape[0]
    per_group = heads // 2
    cols = per_group * BLOCK
    at_picks = 0
    at_slots = at_picks + n_z * PLANE * 2
    at_kinds = at_slots + n_b * 2 * n_list
    at_inv = at_kinds + n_b * 2 * n_list
    z, q = place()
    y, c = q // N_C, q % N_C
    x = lax.axis_index("tp")

    barrier = pltpu.get_barrier_semaphore()
    partners = [{"kv": (z + r) % n_z * PLANE + q} for r in range(1, n_z)]
    partners += [{"kv": z * PLANE + (q + r) % PLANE} for r in range(1, PLANE)]
    right, left = {"tp": (x + 1) % n_x}, {"tp": (x + n_x - 1) % n_x}
    partners += [right, left]
    for who in partners:
        pl.semaphore_signal(barrier, inc=1, device_id=who, device_id_type=MESH)

    loads = [
        pltpu.make_async_copy(src, dst, m["in_sem"].at[i])
        for i, (src, dst) in enumerate(
            [
                (keys, m["kraw"]),
                (vals, m["vraw"]),
                (queries, m["qraw"]),
                (out_grad, m["graw"]),
                (log_sums, m["lraw"]),
                (inputs, m["xraw"].at[0]),
            ]
        )
    ]
    for copy in loads:
        copy.start()
    up_z = {"kv": (z + 1) % n_z * PLANE + q}
    dn_z = {"kv": (z + n_z - 1) % n_z * PLANE + q}
    lane = lax.broadcasted_iota(jnp.int32, (BLOCK, 128), 1)
    low = lane < HD
    loads[0].wait()
    loads[1].wait()
    for b in range(n_b):
        k = m["kraw"][b].astype(F32)
        v = m["vraw"][b].astype(F32)
        kv0 = jnp.where(low, k, pltpu.roll(v, HD, 1)).astype(BF16)
        kv1 = jnp.where(low, pltpu.roll(k, HD, 1), v).astype(BF16)
        m["own0"][b] = kv0
        m["own1"][b] = kv1
        m["tab0"][n_dev + b] = kv0
        m["tab1"][n_dev + b] = kv1
    pl.semaphore_wait(barrier, len(partners))

    def held(g, way, step):
        return m[f"own{g}"] if step == 0 else m[f"held{g}{way}{step}"]

    def z_copy(g, way, step):
        return pltpu.make_async_remote_copy(
            src_ref=held(g, way, step - 1),
            dst_ref=held(g, way, step),
            send_sem=m["z_send"].at[g, way, step],
            recv_sem=m["z_recv"].at[g, way, step],
            device_id=dn_z if way else up_z,
            device_id_type=MESH,
        )

    def sends(way, step):
        if way:
            return (z + step - 1) % n_z < 3
        return (z < n_z - 1) & (z - step + 1 >= 0)

    def gets(way, step):
        if way:
            return (z + step) % n_z < 3
        return z - step >= 0

    def steps(way):
        return 3 if way else 4

    def x_copy(to_right, rel, part):
        half = inputs.shape[0] // 2
        rows = pl.ds(part * half, half)
        slot = rel if to_right else n_x - rel
        if rel == 1:
            src = inputs.at[rows]
        else:
            src = m["xraw"].at[1 if to_right else n_x - 1, rows]
        side = 0 if to_right else 1
        return pltpu.make_async_remote_copy(
            src_ref=src,
            dst_ref=m["xraw"].at[slot, rows],
            send_sem=m["x_send"].at[side, rel, part],
            recv_sem=m["x_recv"].at[side, rel, part],
            device_id=right if to_right else left,
            device_id_type=MESH,
        )

    def y_copy(g, order, z_from, r, receiving=False):
        other = (q + r) % PLANE
        at = other if receiving else q
        return pltpu.make_async_remote_copy(
            src_ref=m["picked"].at[g, order, r],
            dst_ref=m[f"tab{g}"].at[z_from * PLANE + at],
            send_sem=m["y_send"].at[g, order, r],
            recv_sem=m["y_recv"].at[g, order, at],
            device_id={"kv": z * PLANE + other},
            device_id_type=MESH,
        )

    def pick(g, order, z_from, ref):
        def one(r, carry):
            to = (q + r) % PLANE
            m["picked"][g, order, r] = ref[idx[at_picks + (z_from * PLANE + to) * 2 + g]]

            @pl.when(r > 1)
            def _():
                y_copy(g, order, z_from, r - 1).start()

            return carry

        lax.fori_loop(1, PLANE, one, 0)
        m[f"tab{g}"][z_from * PLANE + q] = ref[idx[at_picks + (z_from * PLANE + q) * 2 + g]]
        y_copy(g, order, z_from, PLANE - 1).start()

    def each_piece(g, step, act):
        @pl.when(gets(0, step))
        def _():
            act(g, step, z - step, held(g, 0, step))

        if step < 4:
            @pl.when(gets(1, step) & (z + step >= n_z))
            def _():
                act(g, 4 + step, z + step - n_z, held(g, 1, step))

    for g in range(2):
        for way in range(2):
            @pl.when(sends(way, 1))
            def _():
                z_copy(g, way, 1).start()

    for part in range(2):
        x_copy(True, 1, part).start()
        x_copy(False, 1, 1 - part).start()
    pick(0, 0, z, m["own0"])
    pick(1, 0, z, m["own1"])

    def relay(g, step):
        for way in range(2):
            if step <= steps(way):
                @pl.when(gets(way, step))
                def _():
                    z_copy(g, way, step).wait_recv()

            if step + 1 <= steps(way):
                @pl.when(sends(way, step + 1))
                def _():
                    z_copy(g, way, step + 1).start()

    key_at = lax.broadcasted_iota(jnp.int32, (BLOCK, cols), 0)
    tok_at = lax.broadcasted_iota(jnp.int32, (BLOCK, cols), 1) % BLOCK
    m["bias"][0] = jnp.zeros((BLOCK, cols), F32)
    m["bias"][1] = jnp.where(key_at <= tok_at, 0.0, NEG)
    m["bias"][2] = jnp.full((BLOCK, cols), NEG, F32)
    for p in range(n_b):
        m["terms"][p, n_list] = jnp.zeros((BLOCK, 128), F32)
    loads[4].wait()
    for p in range(n_b):
        for g in range(2):
            row = [
                m["lraw"][g * per_group + r : g * per_group + r + 1, p * BLOCK : (p + 1) * BLOCK]
                for r in range(per_group)
            ]
            m["lse"][p * 2 + g] = jnp.concatenate(row, axis=1)

    for step in range(1, 5):
        relay(0, step)
        each_piece(0, step, pick)
        relay(1, step)
        if step > 1:
            each_piece(1, step - 1, pick)
        if step == 2:
            x_copy(True, 1, 0).wait_recv()
            x_copy(True, 2, 0).start()
            x_copy(False, 1, 1).wait_recv()
            x_copy(False, 2, 1).start()
    each_piece(1, 4, pick)

    def landed(g, order, z_from, ref):
        def one(r, carry):
            y_copy(g, order, z_from, r, receiving=True).wait_recv()
            return carry

        lax.fori_loop(1, PLANE, one, 0)

    def masked_rows(ref, row, g, factor, side):
        parts = []
        for r in range(per_group):
            col = (g * per_group + r) * HD
            part = ref[pl.ds(row, BLOCK), col // 128 * 128 : col // 128 * 128 + 128]
            part = part.astype(F32) * factor
            if r % 2 != side:
                part = pltpu.roll(part, HD, 1)
            parts.append(jnp.where(low != (side == 1), part, 0.0).astype(BF16))
        return parts

    def attention(g):
        tab = m[f"tab{g}"]
        sdp, pd, qd, cat = m["sdp"], m["pd"], m["qd"], m["cat"]

        def one_position(p, carry):
            row = pl.multiple_of(p * BLOCK, BLOCK)
            unit = (p * 2 + g) * n_list
            for r, part in enumerate(masked_rows(m["qraw"], row, g, HD ** -0.5, 0)):
                qd[r * BLOCK : (r + 1) * BLOCK, :] = part
            for r, part in enumerate(masked_rows(m["graw"], row, g, 1.0, 1)):
                qd[cols + r * BLOCK : cols + (r + 1) * BLOCK, :] = part
            for n in range(n_list):
                cat[n] = tab[idx[at_slots + unit + n]]
            keys_all = cat[...].reshape(n_list * BLOCK, 128)
            nt = (((1,), (1,)), ((), ()))
            sdp[...] = lax.dot_general(
                keys_all, qd[...], nt, preferred_element_type=F32
            ).reshape(n_list, BLOCK, 2 * cols)
            lse_row = m["lse"][p * 2 + g]

            def probs(n, acc):
                kind = m["bias"][idx[at_kinds + unit + n]]
                pr = jnp.exp((sdp[n, :, :cols] - lse_row) + kind)
                sdp[n, :, :cols] = pr
                pd[n, :, cols:] = pr.astype(BF16)
                pr = pr * sdp[n, :, cols:]
                return acc + pr.reshape(BLOCK // 8, 8, cols).sum(axis=0)

            acc = lax.fori_loop(0, n_list, probs, jnp.zeros((8, cols), F32), unroll=4)
            delta = acc.sum(axis=0, keepdims=True)

            def grads(n, carry):
                ds = sdp[n, :, :cols] * (sdp[n, :, cols:] - delta)
                pd[n, :, :cols] = ds.astype(BF16)
                return carry

            lax.fori_loop(0, n_list, grads, 0, unroll=4)
            nn = (((1,), (0,)), ((), ()))
            both = pd[...].reshape(n_list * BLOCK, 2 * cols)
            m["terms"][p, :n_list] = lax.dot_general(
                both, qd[...], nn, preferred_element_type=F32
            ).reshape(n_list, BLOCK, 128)
            dq_t = lax.dot_general(
                keys_all, both[:, :cols], (((0,), (0,)), ((), ())), preferred_element_type=F32
            )
            dq = dq_t.T * (HD ** -0.5)
            for pair in range(per_group // 2):
                even = dq[(2 * pair) * BLOCK : (2 * pair + 1) * BLOCK]
                odd = dq[(2 * pair + 1) * BLOCK : (2 * pair + 2) * BLOCK]
                col = g * per_group * HD + pair * 128
                query_grad[pl.ds(row, BLOCK), col : col + 128] = jnp.where(
                    low, even, pltpu.roll(odd, HD, 1)
                )
            return carry

        lax.fori_loop(0, n_b, one_position, 0)

    def summed_terms(g, j):
        at = at_inv + (g * (n_dev + n_b) + j) * n_b
        total = m["terms"][0, idx[at]]
        for p in range(1, n_b):
            total = total + m["terms"][p, idx[at + p]]
        return total

    def b_copy(g, d, r, receiving=False):
        other = (q + r) % PLANE
        at = other if receiving else q
        return pltpu.make_async_remote_copy(
            src_ref=m["ret"].at[g, (z - d) * PLANE + other],
            dst_ref=m["back"].at[g, d, at],
            send_sem=m["b_send"].at[g, d, r],
            recv_sem=m["b_recv"].at[g, d, at],
            device_id={"kv": z * PLANE + other},
            device_id_type=MESH,
        )

    def give_back(g):
        for d in RETURN_ORDER:
            @pl.when(z - d >= 0)
            def _():
                def one(r, carry):
                    j = (z - d) * PLANE + (q + r) % PLANE
                    m["ret"][g, j] = summed_terms(g, j).astype(BF16)

                    @pl.when(r > 1)
                    def _():
                        b_copy(g, d, r - 1).start()

                    return carry

                lax.fori_loop(1, PLANE, one, 0)
                j = (z - d) * PLANE + q
                m["ret"][g, j] = summed_terms(g, j).astype(BF16)
                b_copy(g, d, PLANE - 1).start()

        def own(b, carry):
            m["own_tot"][g, b] = summed_terms(g, n_dev + b)
            return carry

        lax.fori_loop(0, n_b, own, 0)

    def accumulate(g, d):
        def arrived(r, carry):
            b_copy(g, d, r, receiving=True).wait_recv()
            return carry

        lax.fori_loop(1, PLANE, arrived, 0)

        def rows_of(part, carry):
            rows = pl.ds(pl.multiple_of(part * 32, 32), 32)
            accs = [jnp.zeros((32, 128), F32) for _ in range(n_b)]
            for r in range(PLANE):
                frm = (q + r) % PLANE
                if r == 0:
                    val = m["ret"][g, (z - d) * PLANE + q, rows, :]
                else:
                    val = m["back"][g, d, frm, rows, :]
                val = val.astype(F32)
                block = idx[at_picks + ((z - d) * PLANE + frm) * 2 + g]
                for b in range(n_b):
                    accs[b] = accs[b] + jnp.where(block == b, val, 0.0)
            for b in range(n_b):
                m["acc"][g, b, rows, :] = accs[b]
            return carry

        lax.fori_loop(0, 2, rows_of, 0)

    def add_to_acc(g, ref):
        for b in range(n_b):
            m["acc"][g, b] += ref[b].astype(F32)

    def dn_copy(g, d):
        return pltpu.make_async_remote_copy(
            src_ref=m["zs"].at[g, d],
            dst_ref=m["zr_dn"].at[g, d - 1],
            send_sem=m["r_send"].at[g, d],
            recv_sem=m["r_recv_dn"].at[g, d - 1],
            device_id=dn_z,
            device_id_type=MESH,
        )

    def up_copy(g, e, passing=False):
        return pltpu.make_async_remote_copy(
            src_ref=m["zr_up"].at[g, e] if passing else m["zs"].at[g, n_z - e],
            dst_ref=m["zr_up"].at[g, e - 1],
            send_sem=m["r_send"].at[g, n_z - e],
            recv_sem=m["r_recv_up"].at[g, e - 1],
            device_id=up_z,
            device_id_type=MESH,
        )

    def dn_arrival(g, d):
        dn_copy(g, d + 1).wait_recv()
        add_to_acc(g, m["zr_dn"].at[g, d])

    def up_arrival(g, e):
        up_copy(g, e + 1).wait_recv()
        add_to_acc(g, m["zr_up"].at[g, e])

    def store_out(g, d):
        for b in range(n_b):
            m["zs"][g, d, b] = m["acc"][g, b].astype(BF16)

    def collect(g):
        for d in RETURN_ORDER:
            e = n_z - d
            if d > 4:
                @pl.when(z - d >= 0)
                def _():
                    accumulate(g, d)
                    if e < 3:
                        up_arrival(g, e)
                    store_out(g, d)
                    up_copy(g, e).start()

                if e < 3:
                    @pl.when(z < 3 - e)
                    def _():
                        up_copy(g, e + 1).wait_recv()
                        up_copy(g, e, passing=True).start()
            else:
                @pl.when(z - d >= 0)
                def _():
                    accumulate(g, d)
                    if d < 4:
                        @pl.when(z < n_z - 1)
                        def _():
                            dn_arrival(g, d)
                    if d > 0:
                        store_out(g, d)
                        dn_copy(g, d).start()
        @pl.when(z < 3)
        def _():
            up_arrival(g, 0)

    def wait_fetch(g):
        landed(g, 0, z, None)
        for step in range(1, 5):
            each_piece(g, step, landed)

    loads[2].wait()
    loads[3].wait()
    wait_fetch(0)
    attention(0)
    give_back(0)
    wait_fetch(1)
    attention(1)
    give_back(1)
    collect(0)
    collect(1)

    for b in range(n_b):
        rows = slice(b * BLOCK, (b + 1) * BLOCK)
        t0 = m["acc"][0, b] + m["own_tot"][0, b]
        t1 = m["acc"][1, b] + m["own_tot"][1, b]
        kg = jnp.where(low, t0, pltpu.roll(t1, HD, 1))
        key_grad[rows, :] = kg
        value_grad[rows, :] = jnp.where(low, pltpu.roll(t0, HD, 1), t1)
        m["kg"][rows, :] = kg.astype(BF16)

    def c_copy(i):
        return pltpu.make_async_remote_copy(
            src_ref=m["wpart"].at[i, 1 - c],
            dst_ref=m["crecv"].at[i],
            send_sem=m["c_send"].at[i],
            recv_sem=m["c_recv"].at[i],
            device_id={"kv": z * PLANE + y * N_C + (1 - c)},
            device_id_type=MESH,
        )

    x_copy(True, 1, 1).wait_recv()
    x_copy(False, 1, 0).wait_recv()
    x_copy(True, 2, 0).wait_recv()
    x_copy(False, 2, 1).wait_recv()
    loads[5].wait()
    kg_t = m["kg"][...].T
    feats = inputs.shape[1]
    half = feats // 2
    for i in range(2 * n_x):
        rel, h = i // 2, i % 2
        w_t = lax.dot_general(
            kg_t, m["xraw"][rel, :, h * half : (h + 1) * half], (((1,), (0,)), ((), ())),
            preferred_element_type=F32,
        )
        w = w_t.T.astype(BF16)
        for yy in range(N_Y):
            for cc in range(N_C):
                first = (yy * N_C + cc) * BLOCK
                m["wpart"][i, cc, yy] = w[first : first + BLOCK]
        if i:
            c_copy(i - 1).start()
    c_copy(2 * n_x - 1).start()

    def wy_copy(r):
        to = (y + r) % N_Y
        return pltpu.make_async_remote_copy(
            src_ref=m["wy"].at[r],
            dst_ref=m["wyr"].at[r],
            send_sem=m["wy_send"].at[r],
            recv_sem=m["wy_recv"].at[r],
            device_id={"kv": z * PLANE + to * N_C + c},
            device_id_type=MESH,
        )

    for i in range(2 * n_x):
        c_copy(i).wait_recv()
        for r in range(N_Y):
            yy = (y + r) % N_Y
            both = m["wpart"][i, c, yy].astype(F32) + m["crecv"][i, yy].astype(F32)
            if r:
                m["wy"][r, i] = both.astype(BF16)
            else:
                m["wy_own"][i] = both
    for r in (2, 1, 3):
        wy_copy(r).start()

    def z_of(i):
        return 2 * ((x + n_x - i // 2) % n_x) + i % 2

    def wz_copy(i):
        return pltpu.make_async_remote_copy(
            src_ref=m["wz"].at[i],
            dst_ref=m["wzr"].at[z],
            send_sem=m["wz_send"].at[i],
            recv_sem=m["wz_recv"].at[z],
            device_id={"kv": z_of(i) * PLANE + q},
            device_id_type=MESH,
        )

    for r in (1, 3, 2):
        wy_copy(r).wait_recv()
    for i in range(2 * n_x):
        total = m["wy_own"][i]
        for r in range(1, N_Y):
            total = total + m["wyr"][r, i].astype(F32)
        m["wz_own"][i] = total
        m["wz"][i] = total.astype(BF16)
    for i in range(2 * n_x):
        @pl.when(z_of(i) != z)
        def _():
            wz_copy(i).start()
    mine = 2 * ((x + n_x - z // 2) % n_x) + z % 2
    total = m["wz_own"][mine]
    for r in range(1, n_z):
        frm = (z + r) % n_z
        pltpu.make_async_remote_copy(
            src_ref=m["wz"].at[0],
            dst_ref=m["wzr"].at[frm],
            send_sem=m["wz_send"].at[0],
            recv_sem=m["wz_recv"].at[frm],
            device_id={"kv": frm * PLANE + q},
            device_id_type=MESH,
        ).wait_recv()
        total = total + m["wzr"][frm].astype(F32)
    weight_grad[...] = total

    def sent(g, order, z_from, ref):
        def one(r, carry):
            y_copy(g, order, z_from, r).wait_send()
            return carry

        lax.fori_loop(1, PLANE, one, 0)

    for g in range(2):
        for way in range(2):
            for step in range(1, steps(way) + 1):
                @pl.when(sends(way, step))
                def _():
                    z_copy(g, way, step).wait_send()

        sent(g, 0, z, None)
        for step in range(1, 5):
            each_piece(g, step, sent)
        for d in range(8):
            @pl.when(z - d >= 0)
            def _():
                def one(r, carry):
                    b_copy(g, d, r).wait_send()
                    return carry

                lax.fori_loop(1, PLANE, one, 0)

            if 0 < d < 5:
                @pl.when(z - d >= 0)
                def _():
                    dn_copy(g, d).wait_send()
            elif d:
                e = n_z - d
                @pl.when((z - d >= 0) | (z < 3 - e))
                def _():
                    up_copy(g, e).wait_send()

    for part in range(2):
        x_copy(True, 1, part).wait_send()
        x_copy(False, 1, part).wait_send()
    x_copy(True, 2, 0).wait_send()
    x_copy(False, 2, 1).wait_send()
    for i in range(2 * n_x):
        c_copy(i).wait_send()
        @pl.when(z_of(i) != z)
        def _():
            wz_copy(i).wait_send()
    for r in range(1, N_Y):
        wy_copy(r).wait_send()


def index_table(chosen, n_b, n_dev):
    groups, _, n_list = chosen.shape
    me = lax.axis_index("kv")
    z, q = place()
    plane = lax.dynamic_slice_in_dim(chosen, z * PLANE * n_b, PLANE * n_b, 1)
    column = (jnp.arange(n_dev // PLANE) * PLANE + q) * n_b
    offs = plane[..., None] - column
    offs = jnp.where((offs >= 0) & (offs < n_b), offs, 0)
    picks = jnp.max(offs.reshape(groups, PLANE, n_b * n_list, -1), axis=2)
    picks = picks.transpose(2, 1, 0).reshape(-1)
    lists = lax.dynamic_slice_in_dim(chosen, me * n_b, n_b, 1)
    owner = lists // n_b
    slot = jnp.where(owner == me, n_dev + lists % n_b, jnp.maximum(owner, 0))
    at_diag = lists == me * n_b + jnp.arange(n_b)[None, :, None]
    kind = jnp.where(lists < 0, 2, at_diag.astype(jnp.int32))
    listed = (slot[..., None] == jnp.arange(n_dev + n_b)) & (lists >= 0)[..., None]
    inverse = jnp.min(
        jnp.where(listed, jnp.arange(n_list)[:, None], n_list), axis=2
    )
    slots = slot.transpose(1, 0, 2).reshape(-1)
    kinds = kind.transpose(1, 0, 2).reshape(-1)
    inverse = inverse.transpose(0, 2, 1).reshape(-1)
    return jnp.concatenate([picks, slots, kinds, inverse]).astype(jnp.int32)


def local(queries, key_heads, values, log_sums, out_grad, inputs, chosen):
    n_dev = lax.axis_size("kv")
    n_x = lax.axis_size("tp")
    rows, feats = inputs.shape
    n_b = rows // BLOCK
    heads = log_sums.shape[0]
    n_list = chosen.shape[2]
    idx = index_table(chosen, n_b, n_dev)
    scratch = scratch_list(rows, n_dev, n_x, n_list, feats, heads)
    hbm = pl.BlockSpec(memory_space=pl.ANY)
    vm = pl.BlockSpec(memory_space=pltpu.VMEM)
    return pl.pallas_call(
        functools.partial(
            fused_kernel, [name for name, _ in scratch], n_dev // PLANE, n_x, n_list
        ),
        out_shape=(
            jax.ShapeDtypeStruct(queries.shape, F32),
            jax.ShapeDtypeStruct(key_heads.shape, F32),
            jax.ShapeDtypeStruct(values.shape, F32),
            jax.ShapeDtypeStruct((feats * n_x // n_dev, 128), F32),
        ),
        in_specs=[pl.BlockSpec(memory_space=pltpu.SMEM)] + [hbm] * 6,
        out_specs=(vm, vm, vm, vm),
        scratch_shapes=[kind for _, kind in scratch],
        compiler_params=pltpu.CompilerParams(
            collective_id=0, has_side_effects=True, vmem_limit_bytes=60 * 1024 * 1024
        ),
        name="fused",
    )(
        idx,
        key_heads.reshape(n_b, BLOCK, -1),
        values.reshape(n_b, BLOCK, -1),
        queries,
        out_grad,
        log_sums,
        inputs,
    )


def solution(mesh):
    placed = (
        P("kv", "tp"),
        P("kv", "tp"),
        P("kv", "tp"),
        P("tp", "kv"),
        P("kv", "tp"),
        P("kv", "tp"),
        P("tp", None, None),
    )
    return jax.shard_map(
        local,
        mesh=mesh,
        in_specs=placed,
        out_specs=(P("kv", "tp"), P("kv", "tp"), P("kv", "tp"), P("kv", "tp")),
        check_vma=False,
    )
```

```python
import functools

import jax
import jax.numpy as jnp
from jax import lax
from jax.experimental import pallas as pl
from jax.experimental.pallas import tpu as pltpu
from jax.sharding import PartitionSpec as P

HD = 64
BLOCK = 64
NEG = -1e30
LOG2E = 1.4426950408889634
CHUNK = 4
N_Y = 4
N_C = 2
PLANE = N_Y * N_C
MESH = pl.DeviceIdType.MESH
RETURN_ORDER = (4, 5, 3, 6, 2, 7, 1, 0)
F32, BF16 = jnp.float32, jnp.bfloat16


def place():
    me = lax.axis_index("kv")
    return me // PLANE, me % PLANE


def scratch_list(rows, n_dev, n_x, n_list, feats, heads):
    n_b = rows // BLOCK
    tile = (BLOCK, 128)
    cols = heads // 2 * BLOCK
    dma = pltpu.SemaphoreType.DMA
    out = [
        ("kraw", pltpu.VMEM((n_b,) + tile, BF16)),
        ("vraw", pltpu.VMEM((n_b,) + tile, BF16)),
        ("qraw", pltpu.VMEM((rows, heads * HD), BF16)),
        ("graw", pltpu.VMEM((rows, heads * HD), BF16)),
        ("lraw", pltpu.VMEM((heads, rows), F32)),
        ("xraw", pltpu.VMEM((n_x, rows, feats), BF16)),
        ("lse", pltpu.VMEM((n_b * 2, 1, cols), F32)),
        ("bias", pltpu.VMEM((3,) + (BLOCK, cols), F32)),
        ("shift", pltpu.VMEM((3,) + (BLOCK, cols), F32)),
        ("qg", pltpu.VMEM((rows, heads * HD), F32)),
        ("kgo", pltpu.VMEM((rows, 128), F32)),
        ("vgo", pltpu.VMEM((rows, 128), F32)),
        ("wgo", pltpu.VMEM(tile, F32)),
        ("picked", pltpu.VMEM((2, 8, PLANE) + tile, BF16)),
        ("qd", pltpu.VMEM((2 * cols, 128), BF16)),
        ("cat", pltpu.VMEM((n_list,) + tile, BF16)),
        ("sdp", pltpu.VMEM((n_list, BLOCK, 2 * cols), F32)),
        ("pd", pltpu.VMEM((n_list, BLOCK, 2 * cols), BF16)),
        ("terms", pltpu.VMEM((n_b, n_list + 1) + tile, F32)),
        ("ret", pltpu.VMEM((2, n_dev) + tile, BF16)),
        ("own_tot", pltpu.VMEM((2, n_b) + tile, F32)),
        ("back", pltpu.VMEM((2, 8, PLANE) + tile, BF16)),
        ("acc", pltpu.VMEM((2, n_b) + tile, F32)),
        ("zs", pltpu.VMEM((2, 8, 2, n_b, BLOCK // 2, 128), BF16)),
        ("zr_dn", pltpu.VMEM((2, 4, 2, n_b, BLOCK // 2, 128), BF16)),
        ("zr_up", pltpu.VMEM((2, 3, 2, n_b, BLOCK // 2, 128), BF16)),
        ("kg", pltpu.VMEM((rows, 128), BF16)),
        ("wpart", pltpu.VMEM((8, N_C, N_Y) + tile, BF16)),
        ("crecv", pltpu.VMEM((8, N_Y) + tile, BF16)),
        ("wy", pltpu.VMEM((2, N_Y, 4) + tile, BF16)),
        ("wy_own", pltpu.VMEM((8,) + tile, F32)),
        ("wyr", pltpu.VMEM((2, N_Y, 4) + tile, BF16)),
        ("wz", pltpu.VMEM((8,) + tile, BF16)),
        ("wz_own", pltpu.VMEM((8,) + tile, F32)),
        ("wzr", pltpu.VMEM((8,) + tile, BF16)),
        ("in_sem", dma((6,))),
        ("out_sem", dma((4,))),
        ("z_send", dma((2, 2, 5, 2))),
        ("z_recv", dma((2, 2, 5, 2))),
        ("y_send", dma((2, 8))),
        ("y_recv", dma((2, 8))),
        ("x_send", dma((2, 3, 2))),
        ("x_recv", dma((2, 3, 2))),
        ("b_send", dma((2, 8))),
        ("b_recv", dma((2, 8))),
        ("r_send", dma((2, 8, 2))),
        ("r_recv_dn", dma((2, 4, 2))),
        ("r_recv_up", dma((2, 3, 2))),
        ("c_send", dma((8,))),
        ("c_recv", dma((8,))),
        ("wy_send", dma((2, N_Y))),
        ("wy_recv", dma((2, N_Y))),
        ("wz_send", dma((8,))),
        ("wz_recv", dma((8,))),
    ]
    for g in range(2):
        out.append((f"own{g}", pltpu.VMEM((n_b,) + tile, BF16)))
        out.append((f"tab{g}", pltpu.VMEM((n_dev + n_b,) + tile, BF16)))
        for step in range(1, 5):
            out.append((f"held{g}0{step}", pltpu.VMEM((n_b,) + tile, BF16)))
        for step in range(1, 4):
            out.append((f"held{g}1{step}", pltpu.VMEM((n_b,) + tile, BF16)))
    return out


def fused_kernel(names, n_z, n_x, n_list, *refs):
    idx, keys, vals, queries, out_grad, log_sums, inputs = refs[:7]
    query_grad, key_grad, value_grad, weight_grad = refs[7:11]
    m = dict(zip(names, refs[11:]))
    n_b = m["kraw"].shape[0]
    n_dev = n_z * PLANE
    heads = m["lraw"].shape[0]
    per_group = heads // 2
    cols = per_group * BLOCK
    at_picks = 0
    at_slots = at_picks + n_z * PLANE * 2
    at_kinds = at_slots + n_b * 2 * n_list
    at_inv = at_kinds + n_b * 2 * n_list
    z, q = place()
    y, c = q // N_C, q % N_C
    x = lax.axis_index("tp")

    barrier = pltpu.get_barrier_semaphore()
    partners = [{"kv": (z + r) % n_z * PLANE + q} for r in range(1, n_z)]
    partners += [{"kv": z * PLANE + (q + r) % PLANE} for r in range(1, PLANE)]
    right, left = {"tp": (x + 1) % n_x}, {"tp": (x + n_x - 1) % n_x}
    partners += [right, left]
    for who in partners:
        pl.semaphore_signal(barrier, inc=1, device_id=who, device_id_type=MESH)

    loads = [
        pltpu.make_async_copy(src, dst, m["in_sem"].at[i])
        for i, (src, dst) in enumerate(
            [
                (keys, m["kraw"]),
                (vals, m["vraw"]),
                (queries, m["qraw"]),
                (out_grad, m["graw"]),
                (log_sums, m["lraw"]),
                (inputs, m["xraw"].at[0]),
            ]
        )
    ]
    for copy in loads:
        copy.start()
    up_z = {"kv": (z + 1) % n_z * PLANE + q}
    dn_z = {"kv": (z + n_z - 1) % n_z * PLANE + q}
    lane = lax.broadcasted_iota(jnp.int32, (BLOCK, 128), 1)
    low = lane < HD
    loads[0].wait()
    loads[1].wait()
    for b in range(n_b):
        k = m["kraw"][b].astype(F32)
        v = m["vraw"][b].astype(F32)
        kv0 = jnp.where(low, k, pltpu.roll(v, HD, 1)).astype(BF16)
        kv1 = jnp.where(low, pltpu.roll(k, HD, 1), v).astype(BF16)
        m["own0"][b] = kv0
        m["own1"][b] = kv1
        m["tab0"][n_dev + b] = kv0
        m["tab1"][n_dev + b] = kv1
    pl.semaphore_wait(barrier, len(partners))

    def held(g, way, step):
        return m[f"own{g}"] if step == 0 else m[f"held{g}{way}{step}"]

    def z_copy(g, way, step, part):
        blocks = pl.ds(part * (n_b // 2), n_b // 2)
        return pltpu.make_async_remote_copy(
            src_ref=held(g, way, step - 1).at[blocks],
            dst_ref=held(g, way, step).at[blocks],
            send_sem=m["z_send"].at[g, way, step, part],
            recv_sem=m["z_recv"].at[g, way, step, part],
            device_id=dn_z if way else up_z,
            device_id_type=MESH,
        )

    def sends(way, step):
        if way:
            return (z + step - 1) % n_z < 3
        return (z < n_z - 1) & (z - step + 1 >= 0)

    def gets(way, step):
        if way:
            return (z + step) % n_z < 3
        return z - step >= 0

    def steps(way):
        return 3 if way else 4

    def x_copy(to_right, rel, part):
        half = inputs.shape[0] // 2
        rows = pl.ds(part * half, half)
        slot = rel if to_right else n_x - rel
        if rel == 1:
            src = inputs.at[rows]
        else:
            src = m["xraw"].at[1 if to_right else n_x - 1, rows]
        side = 0 if to_right else 1
        return pltpu.make_async_remote_copy(
            src_ref=src,
            dst_ref=m["xraw"].at[slot, rows],
            send_sem=m["x_send"].at[side, rel, part],
            recv_sem=m["x_recv"].at[side, rel, part],
            device_id=right if to_right else left,
            device_id_type=MESH,
        )

    def y_copy(g, order, z_from, r):
        to = (q + r) % PLANE
        return pltpu.make_async_remote_copy(
            src_ref=m["picked"].at[g, order, r],
            dst_ref=m[f"tab{g}"].at[z_from * PLANE + q],
            send_sem=m["y_send"].at[g, order],
            recv_sem=m["y_recv"].at[g, order],
            device_id={"kv": z * PLANE + to},
            device_id_type=MESH,
        )

    others = pl.ds(1, PLANE - 1)

    def wait_group(ref, sem):
        pltpu.make_async_copy(ref, ref, sem).wait()

    def pick(g, order, z_from, ref):
        def one(r, carry):
            to = (q + r) % PLANE
            m["picked"][g, order, r] = ref[idx[at_picks + (z_from * PLANE + to) * 2 + g]]

            @pl.when(r > 1)
            def _():
                y_copy(g, order, z_from, r - 1).start()

            return carry

        lax.fori_loop(1, PLANE, one, 0)
        m[f"tab{g}"][z_from * PLANE + q] = ref[idx[at_picks + (z_from * PLANE + q) * 2 + g]]
        y_copy(g, order, z_from, PLANE - 1).start()

    def each_piece(g, step, act):
        @pl.when(gets(0, step))
        def _():
            act(g, step, z - step, held(g, 0, step))

        if step < 4:
            @pl.when(gets(1, step) & (z + step >= n_z))
            def _():
                act(g, 4 + step, z + step - n_z, held(g, 1, step))

    def set_out(g):
        for part in range(2):
            for way in range(2):
                @pl.when(sends(way, 1))
                def _():
                    z_copy(g, way, 1, part).start()

    set_out(0)
    for part in range(2):
        x_copy(True, 1, part).start()
        x_copy(False, 1, 1 - part).start()
    pick(0, 0, z, m["own0"])
    pick(1, 0, z, m["own1"])

    def relay(g, step):
        for part in range(2):
            for way in range(2):
                if step <= steps(way):
                    @pl.when(gets(way, step))
                    def _():
                        z_copy(g, way, step, part).wait_recv()

                if step + 1 <= steps(way):
                    @pl.when(sends(way, step + 1))
                    def _():
                        z_copy(g, way, step + 1, part).start()

    key_at = lax.broadcasted_iota(jnp.int32, (BLOCK, cols), 0)
    tok_at = lax.broadcasted_iota(jnp.int32, (BLOCK, cols), 1) % BLOCK
    m["bias"][0] = jnp.zeros((BLOCK, cols), F32)
    m["bias"][1] = jnp.where(key_at <= tok_at, 0.0, NEG)
    m["bias"][2] = jnp.full((BLOCK, cols), NEG, F32)
    for p in range(n_b):
        m["terms"][p, n_list] = jnp.zeros((BLOCK, 128), F32)
    loads[4].wait()
    for p in range(n_b):
        for g in range(2):
            row = [
                m["lraw"][g * per_group + r : g * per_group + r + 1, p * BLOCK : (p + 1) * BLOCK]
                for r in range(per_group)
            ]
            m["lse"][p * 2 + g] = jnp.concatenate(row, axis=1)

    for step in range(1, 5):
        relay(0, step)
        if step == 3:
            set_out(1)
        each_piece(0, step, pick)

    def relay_and_pick(g, step):
        relay(g, step)
        each_piece(g, step, pick)

    def relay_x():
        x_copy(True, 1, 0).wait_recv()
        x_copy(True, 2, 0).start()
        x_copy(False, 1, 1).wait_recv()
        x_copy(False, 2, 1).start()

    def landed(g, order, z_from, ref):
        wait_group(m["picked"].at[g, order, others], m["y_recv"].at[g, order])

    def masked_rows(ref, row, g, factor, side):
        parts = []
        for r in range(per_group):
            col = (g * per_group + r) * HD
            part = ref[pl.ds(row, BLOCK), col // 128 * 128 : col // 128 * 128 + 128]
            part = part.astype(F32) * factor
            if r % 2 != side:
                part = pltpu.roll(part, HD, 1)
            parts.append(jnp.where(low != (side == 1), part, 0.0).astype(BF16))
        return parts

    def attention(g, between):
        tab = m[f"tab{g}"]
        sdp, pd, qd, cat, shift = m["sdp"], m["pd"], m["qd"], m["cat"], m["shift"]
        chunks = [slice(n, n + CHUNK) for n in range(0, n_list, CHUNK)]
        nt = (((1,), (1,)), ((), ()))
        nn = (((1,), (0,)), ((), ()))

        def one_position(p, carry):
            row = pl.multiple_of(p * BLOCK, BLOCK)
            unit = (p * 2 + g) * n_list
            for r, part in enumerate(masked_rows(m["qraw"], row, g, HD ** -0.5, 0)):
                qd[r * BLOCK : (r + 1) * BLOCK, :] = part
            for r, part in enumerate(masked_rows(m["graw"], row, g, 1.0, 1)):
                qd[cols + r * BLOCK : cols + (r + 1) * BLOCK, :] = part
            for n in range(n_list):
                cat[n] = tab[idx[at_slots + unit + n]]
            for kind in range(3):
                shift[kind] = m["bias"][kind] - m["lse"][p * 2 + g] * LOG2E

            def products(ch):
                sdp[ch] = lax.dot_general(
                    cat[ch].reshape(CHUNK * BLOCK, 128), qd[...], nt, preferred_element_type=F32
                ).reshape(CHUNK, BLOCK, 2 * cols)

            acc = jnp.zeros((8, cols), F32)
            products(chunks[0])
            for i, ch in enumerate(chunks):
                if i + 1 < len(chunks):
                    products(chunks[i + 1])
                for n in range(ch.start, ch.stop):
                    pr = jnp.exp2(sdp[n, :, :cols] * LOG2E + shift[idx[at_kinds + unit + n]])
                    sdp[n, :, :cols] = pr
                    pd[n, :, cols:] = pr.astype(BF16)
                    pr = pr * sdp[n, :, cols:]
                    acc = acc + pr.reshape(BLOCK // 8, 8, cols).sum(axis=0)
            delta = acc.sum(axis=0, keepdims=True)
            for ch in chunks:
                for n in range(ch.start, ch.stop):
                    ds = sdp[n, :, :cols] * (sdp[n, :, cols:] - delta)
                    pd[n, :, :cols] = ds.astype(BF16)
                m["terms"][p, ch] = lax.dot_general(
                    pd[ch].reshape(CHUNK * BLOCK, 2 * cols), qd[...], nn, preferred_element_type=F32
                ).reshape(CHUNK, BLOCK, 128)
            dq_t = lax.dot_general(
                cat[...].reshape(n_list * BLOCK, 128),
                pd[:, :, :cols].reshape(n_list * BLOCK, cols),
                (((0,), (0,)), ((), ())),
                preferred_element_type=F32,
            )
            dq = dq_t.T * (HD ** -0.5)
            for pair in range(per_group // 2):
                even = dq[(2 * pair) * BLOCK : (2 * pair + 1) * BLOCK]
                odd = dq[(2 * pair + 1) * BLOCK : (2 * pair + 2) * BLOCK]
                col = g * per_group * HD + pair * 128
                m["qg"][pl.ds(row, BLOCK), col : col + 128] = jnp.where(
                    low, even, pltpu.roll(odd, HD, 1)
                )
            for at, act in between.items():
                @pl.when(p == at)
                def _():
                    act()

            return carry

        lax.fori_loop(0, n_b, one_position, 0)

    def summed_terms(g, j):
        at = at_inv + (g * (n_dev + n_b) + j) * n_b
        total = m["terms"][0, idx[at]]
        for p in range(1, n_b):
            total = total + m["terms"][p, idx[at + p]]
        return total

    def b_copy(g, d, r):
        to = (q + r) % PLANE
        return pltpu.make_async_remote_copy(
            src_ref=m["ret"].at[g, (z - d) * PLANE + to],
            dst_ref=m["back"].at[g, d, q],
            send_sem=m["b_send"].at[g, d],
            recv_sem=m["b_recv"].at[g, d],
            device_id={"kv": z * PLANE + to},
            device_id_type=MESH,
        )

    def give_back(g):
        for d in RETURN_ORDER:
            @pl.when(z - d >= 0)
            def _():
                def one(r, carry):
                    j = (z - d) * PLANE + (q + r) % PLANE
                    m["ret"][g, j] = summed_terms(g, j).astype(BF16)

                    @pl.when(r > 1)
                    def _():
                        b_copy(g, d, r - 1).start()

                    return carry

                lax.fori_loop(1, PLANE, one, 0)
                j = (z - d) * PLANE + q
                m["ret"][g, j] = summed_terms(g, j).astype(BF16)
                b_copy(g, d, PLANE - 1).start()

        def own(b, carry):
            m["own_tot"][g, b] = summed_terms(g, n_dev + b)
            return carry

        lax.fori_loop(0, n_b, own, 0)

    def accumulate(g, d, part):
        rows = slice(part * 32, part * 32 + 32)
        accs = [jnp.zeros((32, 128), F32) for _ in range(n_b)]
        for r in range(PLANE):
            frm = (q + r) % PLANE
            if r == 0:
                val = m["ret"][g, (z - d) * PLANE + q, rows, :]
            else:
                val = m["back"][g, d, frm, rows, :]
            val = val.astype(F32)
            block = idx[at_picks + ((z - d) * PLANE + frm) * 2 + g]
            for b in range(n_b):
                accs[b] = accs[b] + jnp.where(block == b, val, 0.0)
        for b in range(n_b):
            m["acc"][g, b, rows, :] = accs[b]

    def dn_copy(g, d, part):
        return pltpu.make_async_remote_copy(
            src_ref=m["zs"].at[g, d, part],
            dst_ref=m["zr_dn"].at[g, d - 1, part],
            send_sem=m["r_send"].at[g, d, part],
            recv_sem=m["r_recv_dn"].at[g, d - 1, part],
            device_id=dn_z,
            device_id_type=MESH,
        )

    def up_copy(g, e, part, passing=False):
        return pltpu.make_async_remote_copy(
            src_ref=m["zr_up"].at[g, e, part] if passing else m["zs"].at[g, n_z - e, part],
            dst_ref=m["zr_up"].at[g, e - 1, part],
            send_sem=m["r_send"].at[g, n_z - e, part],
            recv_sem=m["r_recv_up"].at[g, e - 1, part],
            device_id=up_z,
            device_id_type=MESH,
        )

    def add_arrival(g, copy, ref, part):
        copy.wait_recv()
        rows = slice(part * 32, part * 32 + 32)
        for b in range(n_b):
            m["acc"][g, b, rows, :] += ref[b].astype(F32)

    def dn_arrival(g, d, part):
        add_arrival(g, dn_copy(g, d + 1, part), m["zr_dn"].at[g, d, part], part)

    def up_arrival(g, e, part):
        add_arrival(g, up_copy(g, e + 1, part), m["zr_up"].at[g, e, part], part)

    def store_out(g, d, part):
        rows = slice(part * 32, part * 32 + 32)
        for b in range(n_b):
            m["zs"][g, d, part, b] = m["acc"][g, b, rows, :].astype(BF16)

    def collect(g, d):
        e = n_z - d

        @pl.when(z - d >= 0)
        def _():
            wait_group(m["back"].at[g, d, others], m["b_recv"].at[g, d])
            for part in range(2):
                accumulate(g, d, part)
                if d > 4:
                    if e < 3:
                        up_arrival(g, e, part)
                    store_out(g, d, part)
                    up_copy(g, e, part).start()
                else:
                    if d < 4:
                        @pl.when(z < n_z - 1)
                        def _():
                            dn_arrival(g, d, part)
                    if d > 0:
                        store_out(g, d, part)
                        dn_copy(g, d, part).start()

        if d > 4 and e < 3:
            @pl.when(z < 3 - e)
            def _():
                for part in range(2):
                    up_copy(g, e + 1, part).wait_recv()
                    up_copy(g, e, part, passing=True).start()

        if d == 0:
            @pl.when(z < 3)
            def _():
                for part in range(2):
                    up_arrival(g, 0, part)

    def wait_fetch(g):
        landed(g, 0, z, None)
        for step in range(1, 5):
            each_piece(g, step, landed)

    relay_and_pick(1, 1)
    relay_and_pick(1, 2)
    loads[2].wait()
    loads[3].wait()
    wait_fetch(0)
    attention(
        0,
        {
            0: functools.partial(relay_and_pick, 1, 3),
            1: functools.partial(relay_and_pick, 1, 4),
            2: relay_x,
        },
    )
    give_back(0)
    wait_fetch(1)
    attention(1, {i: functools.partial(collect, 0, RETURN_ORDER[i]) for i in range(6)})
    give_back(1)
    out_q = pltpu.make_async_copy(m["qg"], query_grad, m["out_sem"].at[0])
    out_q.start()
    collect(0, 1)
    collect(1, 4)
    collect(1, 5)
    collect(0, 0)
    for d in RETURN_ORDER[2:]:
        collect(1, d)

    for b in range(n_b):
        rows = slice(b * BLOCK, (b + 1) * BLOCK)
        t0 = m["acc"][0, b] + m["own_tot"][0, b]
        t1 = m["acc"][1, b] + m["own_tot"][1, b]
        kg = jnp.where(low, t0, pltpu.roll(t1, HD, 1))
        m["kgo"][rows, :] = kg
        m["vgo"][rows, :] = jnp.where(low, pltpu.roll(t0, HD, 1), t1)
        m["kg"][rows, :] = kg.astype(BF16)

    def c_copy(i):
        return pltpu.make_async_remote_copy(
            src_ref=m["wpart"].at[i, 1 - c],
            dst_ref=m["crecv"].at[i],
            send_sem=m["c_send"].at[i],
            recv_sem=m["c_recv"].at[i],
            device_id={"kv": z * PLANE + y * N_C + (1 - c)},
            device_id_type=MESH,
        )

    x_copy(True, 1, 1).wait_recv()
    x_copy(False, 1, 0).wait_recv()
    x_copy(True, 2, 0).wait_recv()
    x_copy(False, 2, 1).wait_recv()
    loads[5].wait()
    kg_t = m["kg"][...].T
    half = inputs.shape[1] // 2
    n_i = 2 * n_x

    def wy_copy(part, r):
        to = (y + r) % N_Y
        return pltpu.make_async_remote_copy(
            src_ref=m["wy"].at[part, r],
            dst_ref=m["wyr"].at[part, r],
            send_sem=m["wy_send"].at[part, r],
            recv_sem=m["wy_recv"].at[part, r],
            device_id={"kv": z * PLANE + to * N_C + c},
            device_id_type=MESH,
        )

    def own_terms(i):
        rel, h = i // 2, i % 2
        w_t = lax.dot_general(
            kg_t, m["xraw"][rel, :, h * half : (h + 1) * half], (((1,), (0,)), ((), ())),
            preferred_element_type=F32,
        )
        w = w_t.T.astype(BF16)
        for yy in range(N_Y):
            for cc in range(N_C):
                first = (yy * N_C + cc) * BLOCK
                m["wpart"][i, cc, yy] = w[first : first + BLOCK]

    def core_sum(i):
        c_copy(i).wait_recv()
        for r in range(N_Y):
            yy = (y + r) % N_Y
            both = m["wpart"][i, c, yy].astype(F32) + m["crecv"][i, yy].astype(F32)
            if r:
                m["wy"][i // 4, r, i % 4] = both.astype(BF16)
            else:
                m["wy_own"][i] = both

    out_k = pltpu.make_async_copy(m["kgo"], key_grad, m["out_sem"].at[1])
    out_v = pltpu.make_async_copy(m["vgo"], value_grad, m["out_sem"].at[2])
    for i in range(n_i + 4):
        if i < n_i:
            own_terms(i)
        if 0 < i <= n_i:
            c_copy(i - 1).start()
        if i >= 4:
            core_sum(i - 4)
        if i == n_i - 1:
            for r in (2, 1, 3):
                wy_copy(0, r).start()
    for r in (2, 1, 3):
        wy_copy(1, r).start()
    out_k.start()
    out_v.start()

    def z_of(i):
        return 2 * ((x + n_x - i // 2) % n_x) + i % 2

    def wz_copy(i):
        return pltpu.make_async_remote_copy(
            src_ref=m["wz"].at[i],
            dst_ref=m["wzr"].at[z],
            send_sem=m["wz_send"].at[i],
            recv_sem=m["wz_recv"].at[z],
            device_id={"kv": z_of(i) * PLANE + q},
            device_id_type=MESH,
        )

    def sent(g, order, z_from, ref):
        wait_group(m["picked"].at[g, order, others], m["y_send"].at[g, order])

    for g in range(2):
        for way in range(2):
            for step in range(1, steps(way) + 1):
                @pl.when(sends(way, step))
                def _():
                    for part in range(2):
                        z_copy(g, way, step, part).wait_send()

        sent(g, 0, z, None)
        for step in range(1, 5):
            each_piece(g, step, sent)
        for d in range(8):
            @pl.when(z - d >= 0)
            def _():
                wait_group(m["back"].at[g, d, others], m["b_send"].at[g, d])

            for part in range(2):
                if 0 < d < 5:
                    @pl.when(z - d >= 0)
                    def _():
                        dn_copy(g, d, part).wait_send()
                elif d:
                    e = n_z - d
                    @pl.when((z - d >= 0) | (z < 3 - e))
                    def _():
                        up_copy(g, e, part).wait_send()

    for part in range(2):
        x_copy(True, 1, part).wait_send()
        x_copy(False, 1, part).wait_send()
    x_copy(True, 2, 0).wait_send()
    x_copy(False, 2, 1).wait_send()
    for i in range(n_i):
        c_copy(i).wait_send()
    out_q.wait()

    for part in range(2):
        for r in (1, 3, 2):
            wy_copy(part, r).wait_recv()
        for i in range(part * 4, part * 4 + 4):
            total = m["wy_own"][i]
            for r in range(1, N_Y):
                total = total + m["wyr"][part, r, i % 4].astype(F32)
            m["wz_own"][i] = total
            m["wz"][i] = total.astype(BF16)
        for i in range(part * 4, part * 4 + 4):
            @pl.when(z_of(i) != z)
            def _():
                wz_copy(i).start()
    for part in range(2):
        for r in range(1, N_Y):
            wy_copy(part, r).wait_send()
    out_k.wait()
    out_v.wait()
    mine = 2 * ((x + n_x - z // 2) % n_x) + z % 2
    total = m["wz_own"][mine]
    for r in range(1, n_z):
        frm = (z + r) % n_z
        pltpu.make_async_remote_copy(
            src_ref=m["wz"].at[0],
            dst_ref=m["wzr"].at[frm],
            send_sem=m["wz_send"].at[0],
            recv_sem=m["wz_recv"].at[frm],
            device_id={"kv": frm * PLANE + q},
            device_id_type=MESH,
        ).wait_recv()
        total = total + m["wzr"][frm].astype(F32)
    m["wgo"][...] = total
    for i in range(n_i):
        @pl.when(z_of(i) != z)
        def _():
            wz_copy(i).wait_send()
    out_w = pltpu.make_async_copy(m["wgo"], weight_grad, m["out_sem"].at[3])
    out_w.start()
    out_w.wait()


def index_table(chosen, n_b, n_dev):
    groups, _, n_list = chosen.shape
    me = lax.axis_index("kv")
    z, q = place()
    plane = lax.dynamic_slice_in_dim(chosen, z * PLANE * n_b, PLANE * n_b, 1)
    column = (jnp.arange(n_dev // PLANE) * PLANE + q) * n_b
    offs = plane[..., None] - column
    offs = jnp.where((offs >= 0) & (offs < n_b), offs, 0)
    picks = jnp.max(offs.reshape(groups, PLANE, n_b * n_list, -1), axis=2)
    picks = picks.transpose(2, 1, 0).reshape(-1)
    lists = lax.dynamic_slice_in_dim(chosen, me * n_b, n_b, 1)
    owner = lists // n_b
    slot = jnp.where(owner == me, n_dev + lists % n_b, jnp.maximum(owner, 0))
    at_diag = lists == me * n_b + jnp.arange(n_b)[None, :, None]
    kind = jnp.where(lists < 0, 2, at_diag.astype(jnp.int32))
    listed = (slot[..., None] == jnp.arange(n_dev + n_b)) & (lists >= 0)[..., None]
    inverse = jnp.min(
        jnp.where(listed, jnp.arange(n_list)[:, None], n_list), axis=2
    )
    slots = slot.transpose(1, 0, 2).reshape(-1)
    kinds = kind.transpose(1, 0, 2).reshape(-1)
    inverse = inverse.transpose(0, 2, 1).reshape(-1)
    return jnp.concatenate([picks, slots, kinds, inverse]).astype(jnp.int32)


def local(queries, key_heads, values, log_sums, out_grad, inputs, chosen):
    n_dev = lax.axis_size("kv")
    n_x = lax.axis_size("tp")
    rows, feats = inputs.shape
    n_b = rows // BLOCK
    heads = log_sums.shape[0]
    n_list = chosen.shape[2]
    idx = index_table(chosen, n_b, n_dev)
    scratch = scratch_list(rows, n_dev, n_x, n_list, feats, heads)
    hbm = pl.BlockSpec(memory_space=pl.ANY)
    return pl.pallas_call(
        functools.partial(
            fused_kernel, [name for name, _ in scratch], n_dev // PLANE, n_x, n_list
        ),
        out_shape=(
            jax.ShapeDtypeStruct(queries.shape, F32),
            jax.ShapeDtypeStruct(key_heads.shape, F32),
            jax.ShapeDtypeStruct(values.shape, F32),
            jax.ShapeDtypeStruct((feats * n_x // n_dev, 128), F32),
        ),
        in_specs=[pl.BlockSpec(memory_space=pltpu.SMEM)] + [hbm] * 6,
        out_specs=(hbm,) * 4,
        scratch_shapes=[kind for _, kind in scratch],
        compiler_params=pltpu.CompilerParams(
            collective_id=0, has_side_effects=True, vmem_limit_bytes=60 * 1024 * 1024
        ),
        name="fused",
    )(
        idx,
        key_heads.reshape(n_b, BLOCK, -1),
        values.reshape(n_b, BLOCK, -1),
        queries,
        out_grad,
        log_sums,
        inputs,
    )


def solution(mesh):
    placed = (
        P("kv", "tp"),
        P("kv", "tp"),
        P("kv", "tp"),
        P("tp", "kv"),
        P("kv", "tp"),
        P("kv", "tp"),
        P("tp", None, None),
    )
    return jax.shard_map(
        local,
        mesh=mesh,
        in_specs=placed,
        out_specs=(P("kv", "tp"), P("kv", "tp"), P("kv", "tp"), P("kv", "tp")),
        check_vma=False,
    )
```

```python
import functools

import jax
import jax.numpy as jnp
from jax import lax
from jax.experimental import pallas as pl
from jax.experimental.pallas import tpu as pltpu
from jax.sharding import PartitionSpec as P

HD = 64
BLOCK = 64
NEG = -1e30
LOG2E = 1.4426950408889634
CHUNK = 4
N_Y = 4
N_C = 2
PLANE = N_Y * N_C
MESH = pl.DeviceIdType.MESH
RETURN_ORDER = (4, 5, 3, 6, 2, 7, 1, 0)
F32, BF16 = jnp.float32, jnp.bfloat16


def place():
    me = lax.axis_index("kv")
    return me // PLANE, me % PLANE


def scratch_list(rows, n_dev, n_x, n_list, feats, heads):
    n_b = rows // BLOCK
    tile = (BLOCK, 128)
    cols = heads // 2 * BLOCK
    dma = pltpu.SemaphoreType.DMA
    out = [
        ("kraw", pltpu.VMEM((n_b,) + tile, BF16)),
        ("vraw", pltpu.VMEM((n_b,) + tile, BF16)),
        ("qraw", pltpu.VMEM((rows, heads * HD), BF16)),
        ("graw", pltpu.VMEM((rows, heads * HD), BF16)),
        ("lraw", pltpu.VMEM((heads, rows), F32)),
        ("xraw", pltpu.VMEM((n_x, rows, feats), BF16)),
        ("lse", pltpu.VMEM((n_b * 2, 1, cols), F32)),
        ("bias", pltpu.VMEM((3,) + (BLOCK, cols), F32)),
        ("shift", pltpu.VMEM((3,) + (BLOCK, cols), F32)),
        ("qg", pltpu.VMEM((rows, heads * HD), F32)),
        ("picked", pltpu.VMEM((2, 8, PLANE) + tile, BF16)),
        ("qd", pltpu.VMEM((2 * cols, 128), BF16)),
        ("cat", pltpu.VMEM((n_list,) + tile, BF16)),
        ("sdp", pltpu.VMEM((n_list, BLOCK, 2 * cols), F32)),
        ("pd", pltpu.VMEM((n_list, BLOCK, 2 * cols), BF16)),
        ("terms", pltpu.VMEM((n_b, n_list + 1) + tile, F32)),
        ("ret", pltpu.VMEM((2, n_dev) + tile, BF16)),
        ("own_tot", pltpu.VMEM((2, n_b) + tile, F32)),
        ("back", pltpu.VMEM((2, 8, PLANE) + tile, BF16)),
        ("acc", pltpu.VMEM((2, n_b) + tile, F32)),
        ("zs", pltpu.VMEM((2, 8, 2, n_b, BLOCK // 2, 128), BF16)),
        ("zr_dn", pltpu.VMEM((2, 4, 2, n_b, BLOCK // 2, 128), BF16)),
        ("zr_up", pltpu.VMEM((2, 3, 2, n_b, BLOCK // 2, 128), BF16)),
        ("kg", pltpu.VMEM((rows, 128), BF16)),
        ("wpart", pltpu.VMEM((8, N_C, N_Y) + tile, BF16)),
        ("crecv", pltpu.VMEM((8, N_Y) + tile, BF16)),
        ("wy", pltpu.VMEM((4, N_Y, 2) + tile, BF16)),
        ("wy_own", pltpu.VMEM((8,) + tile, F32)),
        ("wyr", pltpu.VMEM((4, N_Y, 2) + tile, BF16)),
        ("wz", pltpu.VMEM((8,) + tile, BF16)),
        ("wz_own", pltpu.VMEM((8,) + tile, F32)),
        ("wzr", pltpu.VMEM((8,) + tile, BF16)),
        ("in_sem", dma((6,))),
        ("out_sem", dma((1,))),
        ("z_send", dma((2, 2, 5, 2))),
        ("z_recv", dma((2, 2, 5, 2))),
        ("y_send", dma((2, 8))),
        ("y_recv", dma((2, 8))),
        ("x_send", dma((2, 3, 2))),
        ("x_recv", dma((2, 3, 2))),
        ("b_send", dma((2, 8))),
        ("b_recv", dma((2, 8))),
        ("r_send", dma((2, 8, 2))),
        ("r_recv_dn", dma((2, 4, 2))),
        ("r_recv_up", dma((2, 3, 2))),
        ("c_send", dma((8,))),
        ("c_recv", dma((8,))),
        ("wy_send", dma((4, N_Y))),
        ("wy_recv", dma((4, N_Y))),
        ("wz_send", dma((8,))),
        ("wz_recv", dma((8,))),
    ]
    for g in range(2):
        out.append((f"own{g}", pltpu.VMEM((n_b,) + tile, BF16)))
        out.append((f"tab{g}", pltpu.VMEM((n_dev + n_b,) + tile, BF16)))
        for step in range(1, 5):
            out.append((f"held{g}0{step}", pltpu.VMEM((n_b,) + tile, BF16)))
        for step in range(1, 4):
            out.append((f"held{g}1{step}", pltpu.VMEM((n_b,) + tile, BF16)))
    return out


def fused_kernel(names, n_z, n_x, n_list, *refs):
    idx_picks, idx_slots, idx_kinds, idx_inv = refs[:4]
    keys, vals, queries, out_grad, log_sums, inputs = refs[4:10]
    query_grad, key_grad, value_grad, weight_grad = refs[10:14]
    m = dict(zip(names, refs[14:]))
    n_b = m["kraw"].shape[0]
    n_dev = n_z * PLANE
    heads = m["lraw"].shape[0]
    per_group = heads // 2
    cols = per_group * BLOCK
    z, q = place()
    y, c = q // N_C, q % N_C
    x = lax.axis_index("tp")

    barrier = pltpu.get_barrier_semaphore()
    partners = [{"kv": (z + r) % n_z * PLANE + q} for r in range(1, n_z)]
    partners += [{"kv": z * PLANE + (q + r) % PLANE} for r in range(1, PLANE)]
    right, left = {"tp": (x + 1) % n_x}, {"tp": (x + n_x - 1) % n_x}
    partners += [right, left]
    for who in partners:
        pl.semaphore_signal(barrier, inc=1, device_id=who, device_id_type=MESH)

    loads = [
        pltpu.make_async_copy(src, dst, m["in_sem"].at[i])
        for i, (src, dst) in enumerate(
            [
                (keys, m["kraw"]),
                (vals, m["vraw"]),
                (queries, m["qraw"]),
                (out_grad, m["graw"]),
                (log_sums, m["lraw"]),
                (inputs, m["xraw"].at[0]),
            ]
        )
    ]
    for copy in loads:
        copy.start()
    up_z = {"kv": (z + 1) % n_z * PLANE + q}
    dn_z = {"kv": (z + n_z - 1) % n_z * PLANE + q}
    lane = lax.broadcasted_iota(jnp.int32, (BLOCK, 128), 1)
    low = lane < HD
    loads[0].wait()
    loads[1].wait()
    for b in range(n_b):
        k = m["kraw"][b].astype(F32)
        v = m["vraw"][b].astype(F32)
        kv0 = jnp.where(low, k, pltpu.roll(v, HD, 1)).astype(BF16)
        kv1 = jnp.where(low, pltpu.roll(k, HD, 1), v).astype(BF16)
        m["own0"][b] = kv0
        m["own1"][b] = kv1
        m["tab0"][n_dev + b] = kv0
        m["tab1"][n_dev + b] = kv1
    pl.semaphore_wait(barrier, len(partners))

    def held(g, way, step):
        return m[f"own{g}"] if step == 0 else m[f"held{g}{way}{step}"]

    def z_copy(g, way, step, part):
        blocks = pl.ds(part * (n_b // 2), n_b // 2)
        return pltpu.make_async_remote_copy(
            src_ref=held(g, way, step - 1).at[blocks],
            dst_ref=held(g, way, step).at[blocks],
            send_sem=m["z_send"].at[g, way, step, part],
            recv_sem=m["z_recv"].at[g, way, step, part],
            device_id=dn_z if way else up_z,
            device_id_type=MESH,
        )

    def sends(way, step):
        if way:
            return (z + step - 1) % n_z < 3
        return (z < n_z - 1) & (z - step + 1 >= 0)

    def gets(way, step):
        if way:
            return (z + step) % n_z < 3
        return z - step >= 0

    def steps(way):
        return 3 if way else 4

    def x_copy(to_right, rel, part):
        half = inputs.shape[0] // 2
        rows = pl.ds(part * half, half)
        slot = rel if to_right else n_x - rel
        if rel == 1:
            src = inputs.at[rows]
        else:
            src = m["xraw"].at[1 if to_right else n_x - 1, rows]
        side = 0 if to_right else 1
        return pltpu.make_async_remote_copy(
            src_ref=src,
            dst_ref=m["xraw"].at[slot, rows],
            send_sem=m["x_send"].at[side, rel, part],
            recv_sem=m["x_recv"].at[side, rel, part],
            device_id=right if to_right else left,
            device_id_type=MESH,
        )

    def y_copy(g, order, z_from, r):
        to = (q + r) % PLANE
        return pltpu.make_async_remote_copy(
            src_ref=m["picked"].at[g, order, r],
            dst_ref=m[f"tab{g}"].at[z_from * PLANE + q],
            send_sem=m["y_send"].at[g, order],
            recv_sem=m["y_recv"].at[g, order],
            device_id={"kv": z * PLANE + to},
            device_id_type=MESH,
        )

    others = pl.ds(1, PLANE - 1)

    def wait_group(ref, sem):
        pltpu.make_async_copy(ref, ref, sem).wait()

    def pick(g, order, z_from, ref):
        def one(r, carry):
            to = (q + r) % PLANE
            m["picked"][g, order, r] = ref[idx_picks[(z_from * PLANE + to) * 2 + g]]

            @pl.when(r > 1)
            def _():
                y_copy(g, order, z_from, r - 1).start()

            return carry

        lax.fori_loop(1, PLANE, one, 0)
        m[f"tab{g}"][z_from * PLANE + q] = ref[idx_picks[(z_from * PLANE + q) * 2 + g]]
        y_copy(g, order, z_from, PLANE - 1).start()

    def each_piece(g, step, act):
        @pl.when(gets(0, step))
        def _():
            act(g, step, z - step, held(g, 0, step))

        if step < 4:
            @pl.when(gets(1, step) & (z + step >= n_z))
            def _():
                act(g, 4 + step, z + step - n_z, held(g, 1, step))

    def set_out(g):
        for part in range(2):
            for way in range(2):
                @pl.when(sends(way, 1))
                def _():
                    z_copy(g, way, 1, part).start()

    set_out(0)
    for part in range(2):
        x_copy(True, 1, part).start()
        x_copy(False, 1, 1 - part).start()
    pick(0, 0, z, m["own0"])
    pick(1, 0, z, m["own1"])

    def relay(g, step):
        for part in range(2):
            for way in range(2):
                if step <= steps(way):
                    @pl.when(gets(way, step))
                    def _():
                        z_copy(g, way, step, part).wait_recv()

                if step + 1 <= steps(way):
                    @pl.when(sends(way, step + 1))
                    def _():
                        z_copy(g, way, step + 1, part).start()

    key_at = lax.broadcasted_iota(jnp.int32, (BLOCK, cols), 0)
    tok_at = lax.broadcasted_iota(jnp.int32, (BLOCK, cols), 1) % BLOCK
    m["bias"][0] = jnp.zeros((BLOCK, cols), F32)
    m["bias"][1] = jnp.where(key_at <= tok_at, 0.0, NEG)
    m["bias"][2] = jnp.full((BLOCK, cols), NEG, F32)
    for p in range(n_b):
        m["terms"][p, n_list] = jnp.zeros((BLOCK, 128), F32)
    loads[4].wait()
    for p in range(n_b):
        for g in range(2):
            row = [
                m["lraw"][g * per_group + r : g * per_group + r + 1, p * BLOCK : (p + 1) * BLOCK]
                for r in range(per_group)
            ]
            m["lse"][p * 2 + g] = jnp.concatenate(row, axis=1)

    for step in range(1, 5):
        relay(0, step)
        if step == 3:
            set_out(1)
        each_piece(0, step, pick)

    def relay_and_pick(g, step):
        relay(g, step)
        each_piece(g, step, pick)

    def relay_x():
        x_copy(True, 1, 0).wait_recv()
        x_copy(True, 2, 0).start()
        x_copy(False, 1, 1).wait_recv()
        x_copy(False, 2, 1).start()

    def landed(g, order, z_from, ref):
        wait_group(m["picked"].at[g, order, others], m["y_recv"].at[g, order])

    def masked_rows(ref, row, g, factor, side):
        parts = []
        for r in range(per_group):
            col = (g * per_group + r) * HD
            part = ref[pl.ds(row, BLOCK), col // 128 * 128 : col // 128 * 128 + 128]
            part = part.astype(F32) * factor
            if r % 2 != side:
                part = pltpu.roll(part, HD, 1)
            parts.append(jnp.where(low != (side == 1), part, 0.0).astype(BF16))
        return parts

    def attention(g, between):
        tab = m[f"tab{g}"]
        sdp, pd, qd, cat, shift = m["sdp"], m["pd"], m["qd"], m["cat"], m["shift"]
        chunks = [slice(n, n + CHUNK) for n in range(0, n_list, CHUNK)]
        nt = (((1,), (1,)), ((), ()))
        nn = (((1,), (0,)), ((), ()))

        def one_position(p, carry):
            row = pl.multiple_of(p * BLOCK, BLOCK)
            unit = (p * 2 + g) * n_list
            for r, part in enumerate(masked_rows(m["qraw"], row, g, HD ** -0.5, 0)):
                qd[r * BLOCK : (r + 1) * BLOCK, :] = part
            for r, part in enumerate(masked_rows(m["graw"], row, g, 1.0, 1)):
                qd[cols + r * BLOCK : cols + (r + 1) * BLOCK, :] = part
            for n in range(n_list):
                cat[n] = tab[idx_slots[unit + n]]
            for kind in range(3):
                shift[kind] = m["bias"][kind] - m["lse"][p * 2 + g] * LOG2E

            acc = jnp.zeros((8, cols), F32)
            for ch in chunks:
                both = lax.dot_general(
                    cat[ch].reshape(CHUNK * BLOCK, 128), qd[...], nt, preferred_element_type=F32
                ).reshape(CHUNK, BLOCK, 2 * cols)
                for n in range(ch.start, ch.stop):
                    prod = both[n - ch.start]
                    pr = jnp.exp2(prod[:, :cols] * LOG2E + shift[idx_kinds[unit + n]])
                    sdp[n, :, :cols] = pr
                    sdp[n, :, cols:] = prod[:, cols:]
                    pd[n, :, cols:] = pr.astype(BF16)
                    pr = pr * prod[:, cols:]
                    acc = acc + pr.reshape(BLOCK // 8, 8, cols).sum(axis=0)
            delta = acc.sum(axis=0, keepdims=True)
            for ch in chunks:
                for n in range(ch.start, ch.stop):
                    ds = sdp[n, :, :cols] * (sdp[n, :, cols:] - delta)
                    pd[n, :, :cols] = ds.astype(BF16)
                m["terms"][p, ch] = lax.dot_general(
                    pd[ch].reshape(CHUNK * BLOCK, 2 * cols), qd[...], nn, preferred_element_type=F32
                ).reshape(CHUNK, BLOCK, 128)
            dq_t = lax.dot_general(
                cat[...].reshape(n_list * BLOCK, 128),
                pd[:, :, :cols].reshape(n_list * BLOCK, cols),
                (((0,), (0,)), ((), ())),
                preferred_element_type=F32,
            )
            dq = dq_t.T
            for pair in range(per_group // 2):
                even = dq[(2 * pair) * BLOCK : (2 * pair + 1) * BLOCK]
                odd = dq[(2 * pair + 1) * BLOCK : (2 * pair + 2) * BLOCK]
                col = g * per_group * HD + pair * 128
                m["qg"][pl.ds(row, BLOCK), col : col + 128] = jnp.where(
                    low, even, pltpu.roll(odd, HD, 1)
                )
            for at, act in between.items():
                @pl.when(p == at)
                def _():
                    act()

            return carry

        lax.fori_loop(0, n_b, one_position, 0)

    def summed_terms(g, j):
        at = (g * (n_dev + n_b) + j) * n_b
        total = m["terms"][0, idx_inv[at]]
        for p in range(1, n_b):
            total = total + m["terms"][p, idx_inv[at + p]]
        return total

    def b_copy(g, d, r):
        to = (q + r) % PLANE
        return pltpu.make_async_remote_copy(
            src_ref=m["ret"].at[g, (z - d) * PLANE + to],
            dst_ref=m["back"].at[g, d, q],
            send_sem=m["b_send"].at[g, d],
            recv_sem=m["b_recv"].at[g, d],
            device_id={"kv": z * PLANE + to},
            device_id_type=MESH,
        )

    def give_back(g):
        for d in RETURN_ORDER:
            @pl.when(z - d >= 0)
            def _():
                for r in list(range(1, PLANE)) + [0]:
                    j = (z - d) * PLANE + (q + r) % PLANE
                    m["ret"][g, j] = summed_terms(g, j).astype(BF16)
                for r in range(1, PLANE):
                    b_copy(g, d, r).start()

        def own(b, carry):
            m["own_tot"][g, b] = summed_terms(g, n_dev + b)
            return carry

        lax.fori_loop(0, n_b, own, 0)

    def accumulate(g, d, part):
        rows = slice(part * 32, part * 32 + 32)
        accs = [jnp.zeros((32, 128), F32) for _ in range(n_b)]
        for r in range(PLANE):
            frm = (q + r) % PLANE
            if r == 0:
                val = m["ret"][g, (z - d) * PLANE + q, rows, :]
            else:
                val = m["back"][g, d, frm, rows, :]
            val = val.astype(F32)
            block = idx_picks[((z - d) * PLANE + frm) * 2 + g]
            for b in range(n_b):
                accs[b] = accs[b] + jnp.where(block == b, val, 0.0)
        for b in range(n_b):
            m["acc"][g, b, rows, :] = accs[b]

    def dn_copy(g, d, part):
        return pltpu.make_async_remote_copy(
            src_ref=m["zs"].at[g, d, part],
            dst_ref=m["zr_dn"].at[g, d - 1, part],
            send_sem=m["r_send"].at[g, d, part],
            recv_sem=m["r_recv_dn"].at[g, d - 1, part],
            device_id=dn_z,
            device_id_type=MESH,
        )

    def up_copy(g, e, part, passing=False):
        return pltpu.make_async_remote_copy(
            src_ref=m["zr_up"].at[g, e, part] if passing else m["zs"].at[g, n_z - e, part],
            dst_ref=m["zr_up"].at[g, e - 1, part],
            send_sem=m["r_send"].at[g, n_z - e, part],
            recv_sem=m["r_recv_up"].at[g, e - 1, part],
            device_id=up_z,
            device_id_type=MESH,
        )

    def add_arrival(g, copy, ref, part):
        copy.wait_recv()
        rows = slice(part * 32, part * 32 + 32)
        for b in range(n_b):
            m["acc"][g, b, rows, :] += ref[b].astype(F32)

    def dn_arrival(g, d, part):
        add_arrival(g, dn_copy(g, d + 1, part), m["zr_dn"].at[g, d, part], part)

    def up_arrival(g, e, part):
        add_arrival(g, up_copy(g, e + 1, part), m["zr_up"].at[g, e, part], part)

    def store_out(g, d, part):
        rows = slice(part * 32, part * 32 + 32)
        for b in range(n_b):
            m["zs"][g, d, part, b] = m["acc"][g, b, rows, :].astype(BF16)

    def collect(g, d):
        e = n_z - d

        @pl.when(z - d >= 0)
        def _():
            wait_group(m["back"].at[g, d, others], m["b_recv"].at[g, d])
            for part in range(2):
                accumulate(g, d, part)
                if d > 4:
                    if e < 3:
                        up_arrival(g, e, part)
                    store_out(g, d, part)
                    up_copy(g, e, part).start()
                else:
                    if d < 4:
                        @pl.when(z < n_z - 1)
                        def _():
                            dn_arrival(g, d, part)
                    if d > 0:
                        store_out(g, d, part)
                        dn_copy(g, d, part).start()

        if d > 4 and e < 3:
            @pl.when(z < 3 - e)
            def _():
                for part in range(2):
                    up_copy(g, e + 1, part).wait_recv()
                    up_copy(g, e, part, passing=True).start()

        if d == 0:
            @pl.when(z < 3)
            def _():
                for part in range(2):
                    up_arrival(g, 0, part)

    def wait_fetch(g):
        landed(g, 0, z, None)
        for step in range(1, 5):
            each_piece(g, step, landed)

    relay_and_pick(1, 1)
    loads[2].wait()
    loads[3].wait()
    wait_fetch(0)
    attention(
        0,
        {
            0: functools.partial(relay_and_pick, 1, 2),
            2: functools.partial(relay_and_pick, 1, 3),
            3: functools.partial(relay_and_pick, 1, 4),
            4: relay_x,
        },
    )
    give_back(0)
    wait_fetch(1)
    attention(1, {2 + i: functools.partial(collect, 0, RETURN_ORDER[i]) for i in range(4)})
    give_back(1)
    out_q = pltpu.make_async_copy(m["qg"], query_grad, m["out_sem"].at[0])
    out_q.start()
    collect(0, 2)
    collect(0, 7)
    collect(1, 4)
    collect(0, 1)
    collect(1, 5)
    collect(1, 3)
    collect(0, 0)
    for d in RETURN_ORDER[3:]:
        collect(1, d)

    for b in range(n_b):
        rows = slice(b * BLOCK, (b + 1) * BLOCK)
        t0 = m["acc"][0, b] + m["own_tot"][0, b]
        t1 = m["acc"][1, b] + m["own_tot"][1, b]
        kg = jnp.where(low, t0, pltpu.roll(t1, HD, 1))
        key_grad[rows, :] = kg
        value_grad[rows, :] = jnp.where(low, pltpu.roll(t0, HD, 1), t1)
        m["kg"][rows, :] = kg.astype(BF16)

    def c_copy(i):
        return pltpu.make_async_remote_copy(
            src_ref=m["wpart"].at[i, 1 - c],
            dst_ref=m["crecv"].at[i],
            send_sem=m["c_send"].at[i],
            recv_sem=m["c_recv"].at[i],
            device_id={"kv": z * PLANE + y * N_C + (1 - c)},
            device_id_type=MESH,
        )

    x_copy(True, 1, 1).wait_recv()
    x_copy(False, 1, 0).wait_recv()
    x_copy(True, 2, 0).wait_recv()
    x_copy(False, 2, 1).wait_recv()
    loads[5].wait()
    kg_t = m["kg"][...].T
    half = inputs.shape[1] // 2
    n_i = 2 * n_x

    def wy_copy(part, r):
        to = (y + r) % N_Y
        return pltpu.make_async_remote_copy(
            src_ref=m["wy"].at[part, r],
            dst_ref=m["wyr"].at[part, r],
            send_sem=m["wy_send"].at[part, r],
            recv_sem=m["wy_recv"].at[part, r],
            device_id={"kv": z * PLANE + to * N_C + c},
            device_id_type=MESH,
        )

    def own_terms(i):
        rel, h = i // 2, i % 2
        w_t = lax.dot_general(
            kg_t, m["xraw"][rel, :, h * half : (h + 1) * half], (((1,), (0,)), ((), ())),
            preferred_element_type=F32,
        )
        w = w_t.T.astype(BF16)
        for yy in range(N_Y):
            for cc in range(N_C):
                first = (yy * N_C + cc) * BLOCK
                m["wpart"][i, cc, yy] = w[first : first + BLOCK]

    def core_sum(i):
        c_copy(i).wait_recv()
        for r in range(N_Y):
            yy = (y + r) % N_Y
            both = m["wpart"][i, c, yy].astype(F32) + m["crecv"][i, yy].astype(F32)
            if r:
                m["wy"][i // 2, r, i % 2] = both.astype(BF16)
            else:
                m["wy_own"][i] = both

    lag = 3
    for i in range(n_i + lag):
        if i < n_i:
            own_terms(i)
        if 0 < i <= n_i:
            c_copy(i - 1).start()
        if i >= lag:
            core_sum(i - lag)
            if (i - lag) % 2:
                for r in (2, 1, 3):
                    wy_copy((i - lag) // 2, r).start()

    def z_of(i):
        return 2 * ((x + n_x - i // 2) % n_x) + i % 2

    def wz_copy(i):
        return pltpu.make_async_remote_copy(
            src_ref=m["wz"].at[i],
            dst_ref=m["wzr"].at[z],
            send_sem=m["wz_send"].at[i],
            recv_sem=m["wz_recv"].at[z],
            device_id={"kv": z_of(i) * PLANE + q},
            device_id_type=MESH,
        )

    def sent(g, order, z_from, ref):
        wait_group(m["picked"].at[g, order, others], m["y_send"].at[g, order])

    for g in range(2):
        for way in range(2):
            for step in range(1, steps(way) + 1):
                @pl.when(sends(way, step))
                def _():
                    for part in range(2):
                        z_copy(g, way, step, part).wait_send()

        sent(g, 0, z, None)
        for step in range(1, 5):
            each_piece(g, step, sent)
        for d in range(8):
            @pl.when(z - d >= 0)
            def _():
                wait_group(m["back"].at[g, d, others], m["b_send"].at[g, d])

            for part in range(2):
                if 0 < d < 5:
                    @pl.when(z - d >= 0)
                    def _():
                        dn_copy(g, d, part).wait_send()
                elif d:
                    e = n_z - d
                    @pl.when((z - d >= 0) | (z < 3 - e))
                    def _():
                        up_copy(g, e, part).wait_send()

    for part in range(2):
        x_copy(True, 1, part).wait_send()
        x_copy(False, 1, part).wait_send()
    x_copy(True, 2, 0).wait_send()
    x_copy(False, 2, 1).wait_send()
    for i in range(n_i):
        c_copy(i).wait_send()
    out_q.wait()

    for part in range(n_x):
        for r in (1, 3, 2):
            wy_copy(part, r).wait_recv()
        for i in (2 * part, 2 * part + 1):
            total = m["wy_own"][i]
            for r in range(1, N_Y):
                total = total + m["wyr"][part, r, i % 2].astype(F32)
            m["wz_own"][i] = total
            m["wz"][i] = total.astype(BF16)
        for i in (2 * part, 2 * part + 1):
            @pl.when(z_of(i) != z)
            def _():
                wz_copy(i).start()
    for part in range(n_x):
        for r in range(1, N_Y):
            wy_copy(part, r).wait_send()
    mine = 2 * ((x + n_x - z // 2) % n_x) + z % 2
    total = m["wz_own"][mine]
    for r in range(1, n_z):
        frm = (z + r) % n_z
        pltpu.make_async_remote_copy(
            src_ref=m["wz"].at[0],
            dst_ref=m["wzr"].at[frm],
            send_sem=m["wz_send"].at[0],
            recv_sem=m["wz_recv"].at[frm],
            device_id={"kv": frm * PLANE + q},
            device_id_type=MESH,
        ).wait_recv()
        total = total + m["wzr"][frm].astype(F32)
    weight_grad[...] = total
    for i in range(n_i):
        @pl.when(z_of(i) != z)
        def _():
            wz_copy(i).wait_send()


def index_table(chosen, n_b, n_dev):
    groups, _, n_list = chosen.shape
    me = lax.axis_index("kv")
    z, q = place()
    plane = lax.dynamic_slice_in_dim(chosen, z * PLANE * n_b, PLANE * n_b, 1)
    column = (jnp.arange(n_dev // PLANE) * PLANE + q) * n_b
    offs = plane[..., None] - column
    offs = jnp.where((offs >= 0) & (offs < n_b), offs, 0)
    picks = jnp.max(offs.reshape(groups, PLANE, n_b * n_list, -1), axis=2)
    picks = picks.transpose(2, 1, 0).reshape(-1)
    lists = lax.dynamic_slice_in_dim(chosen, me * n_b, n_b, 1)
    owner = lists // n_b
    slot = jnp.where(owner == me, n_dev + lists % n_b, jnp.maximum(owner, 0))
    at_diag = lists == me * n_b + jnp.arange(n_b)[None, :, None]
    kind = jnp.where(lists < 0, 2, at_diag.astype(jnp.int32))
    listed = (slot[..., None] == jnp.arange(n_dev + n_b)) & (lists >= 0)[..., None]
    inverse = jnp.min(
        jnp.where(listed, jnp.arange(n_list)[:, None], n_list), axis=2
    )
    slots = slot.transpose(1, 0, 2).reshape(-1)
    kinds = kind.transpose(1, 0, 2).reshape(-1)
    inverse = inverse.transpose(0, 2, 1).reshape(-1)
    return picks, slots, kinds, inverse


def local(queries, key_heads, values, log_sums, out_grad, inputs, chosen):
    n_dev = lax.axis_size("kv")
    n_x = lax.axis_size("tp")
    rows, feats = inputs.shape
    n_b = rows // BLOCK
    heads = log_sums.shape[0]
    n_list = chosen.shape[2]
    idx = index_table(chosen, n_b, n_dev)
    scratch = scratch_list(rows, n_dev, n_x, n_list, feats, heads)
    hbm = pl.BlockSpec(memory_space=pltpu.HBM)
    vm = pl.BlockSpec(memory_space=pltpu.VMEM)
    query_sums, key_grad, value_grad, weight_grad = pl.pallas_call(
        functools.partial(
            fused_kernel, [name for name, _ in scratch], n_dev // PLANE, n_x, n_list
        ),
        out_shape=(
            jax.ShapeDtypeStruct(queries.shape, F32),
            jax.ShapeDtypeStruct(key_heads.shape, F32),
            jax.ShapeDtypeStruct(values.shape, F32),
            jax.ShapeDtypeStruct((feats * n_x // n_dev, 128), F32),
        ),
        in_specs=[pl.BlockSpec(memory_space=pltpu.SMEM)] * 4 + [hbm] * 6,
        out_specs=(hbm, vm, vm, vm),
        scratch_shapes=[kind for _, kind in scratch],
        compiler_params=pltpu.CompilerParams(
            collective_id=0, has_side_effects=True, vmem_limit_bytes=53 * 1024 * 1024
        ),
        name="fused",
    )(
        *idx,
        key_heads.reshape(n_b, BLOCK, -1),
        values.reshape(n_b, BLOCK, -1),
        queries,
        out_grad,
        log_sums,
        inputs,
    )
    return query_sums * (HD ** -0.5), key_grad, value_grad, weight_grad


def solution(mesh):
    placed = (
        P("kv", "tp"),
        P("kv", "tp"),
        P("kv", "tp"),
        P("tp", "kv"),
        P("kv", "tp"),
        P("kv", "tp"),
        P("tp", None, None),
    )
    return jax.shard_map(
        local,
        mesh=mesh,
        in_specs=placed,
        out_specs=(P("kv", "tp"), P("kv", "tp"), P("kv", "tp"), P("kv", "tp")),
        check_vma=False,
    )
```

```python
import functools

import jax
import jax.numpy as jnp
from jax import lax
from jax.experimental import pallas as pl
from jax.experimental.pallas import tpu as pltpu
from jax.sharding import PartitionSpec as P

HD = 64
BLOCK = 64
NEG = -1e30
LOG2E = 1.4426950408889634
CHUNK = 4
PARTS = 3
N_Y = 4
N_C = 2
PLANE = N_Y * N_C
MESH = pl.DeviceIdType.MESH
RETURN_ORDER = (4, 5, 3, 6, 2, 7, 1, 0)
F32, BF16 = jnp.float32, jnp.bfloat16


def place():
    me = lax.axis_index("kv")
    return me // PLANE, me % PLANE


def scratch_list(rows, n_dev, n_x, n_list, feats, heads):
    n_b = rows // BLOCK
    tile = (BLOCK, 128)
    cols = heads // 2 * BLOCK
    dma = pltpu.SemaphoreType.DMA
    out = [
        ("kraw", pltpu.VMEM((n_b,) + tile, BF16)),
        ("vraw", pltpu.VMEM((n_b,) + tile, BF16)),
        ("qraw", pltpu.VMEM((rows, heads * HD), BF16)),
        ("graw", pltpu.VMEM((rows, heads * HD), BF16)),
        ("lraw", pltpu.VMEM((heads, rows), F32)),
        ("xraw", pltpu.VMEM((n_x, rows, feats), BF16)),
        ("lse", pltpu.VMEM((n_b * 2, 1, cols), F32)),
        ("bias", pltpu.VMEM((3,) + (BLOCK, cols), F32)),
        ("shift", pltpu.VMEM((3,) + (BLOCK, cols), F32)),
        ("qg", pltpu.VMEM((rows, heads * HD), F32)),
        ("picked", pltpu.VMEM((2, 8, PLANE) + tile, BF16)),
        ("qd", pltpu.VMEM((2 * cols, 128), BF16)),
        ("cat", pltpu.VMEM((n_list,) + tile, BF16)),
        ("sdp", pltpu.VMEM((n_list, BLOCK, 2 * cols), F32)),
        ("pd", pltpu.VMEM((n_list, BLOCK, 2 * cols), BF16)),
        ("terms", pltpu.VMEM((n_b, n_list + 1) + tile, F32)),
        ("ret", pltpu.VMEM((2, n_dev) + tile, BF16)),
        ("own_tot", pltpu.VMEM((2, n_b) + tile, F32)),
        ("back", pltpu.VMEM((2, 8, PLANE) + tile, BF16)),
        ("acc", pltpu.VMEM((2, n_b) + tile, F32)),
        ("zs", pltpu.VMEM((2, 8, 2, n_b, BLOCK // 2, 128), BF16)),
        ("zr_dn", pltpu.VMEM((2, 4, 2, n_b, BLOCK // 2, 128), BF16)),
        ("zr_up", pltpu.VMEM((2, 3, 2, n_b, BLOCK // 2, 128), BF16)),
        ("kg", pltpu.VMEM((rows, 128), BF16)),
        ("wpart", pltpu.VMEM((8, N_C, N_Y) + tile, BF16)),
        ("crecv", pltpu.VMEM((8, N_Y) + tile, BF16)),
        ("wy", pltpu.VMEM((4, N_Y, 2) + tile, BF16)),
        ("wy_own", pltpu.VMEM((8,) + tile, F32)),
        ("wyr", pltpu.VMEM((4, N_Y, 2) + tile, BF16)),
        ("wz", pltpu.VMEM((8,) + tile, BF16)),
        ("wz_own", pltpu.VMEM((8,) + tile, F32)),
        ("wzr", pltpu.VMEM((8,) + tile, BF16)),
        ("in_sem", dma((6,))),
        ("out_sem", dma((1,))),
        ("z_send", dma((2, 2, 5, PARTS))),
        ("z_recv", dma((2, 2, 5, PARTS))),
        ("y_send", dma((2, 8))),
        ("y_recv", dma((2, 8))),
        ("x_send", dma((2, 3, 2))),
        ("x_recv", dma((2, 3, 2))),
        ("b_send", dma((2, 8))),
        ("b_recv", dma((2, 8))),
        ("r_send", dma((2, 8, 2))),
        ("r_recv_dn", dma((2, 4, 2))),
        ("r_recv_up", dma((2, 3, 2))),
        ("c_send", dma((8,))),
        ("c_recv", dma((8,))),
        ("wy_send", dma((4, N_Y))),
        ("wy_recv", dma((4, N_Y))),
        ("wz_send", dma((8,))),
        ("wz_recv", dma((8,))),
    ]
    for g in range(2):
        out.append((f"own{g}", pltpu.VMEM((n_b,) + tile, BF16)))
        out.append((f"tab{g}", pltpu.VMEM((n_dev + n_b,) + tile, BF16)))
        for step in range(1, 5):
            out.append((f"held{g}0{step}", pltpu.VMEM((n_b,) + tile, BF16)))
        for step in range(1, 4):
            out.append((f"held{g}1{step}", pltpu.VMEM((n_b,) + tile, BF16)))
    return out


def fused_kernel(names, n_z, n_x, n_list, *refs):
    idx_picks, idx_slots, idx_kinds, idx_inv = refs[:4]
    keys, vals, queries, out_grad, log_sums, inputs = refs[4:10]
    query_grad, key_grad, value_grad, weight_grad = refs[10:14]
    m = dict(zip(names, refs[14:]))
    n_b = m["kraw"].shape[0]
    n_dev = n_z * PLANE
    heads = m["lraw"].shape[0]
    per_group = heads // 2
    cols = per_group * BLOCK
    z, q = place()
    y, c = q // N_C, q % N_C
    x = lax.axis_index("tp")

    barrier = pltpu.get_barrier_semaphore()
    partners = [{"kv": (z + r) % n_z * PLANE + q} for r in range(1, n_z)]
    partners += [{"kv": z * PLANE + (q + r) % PLANE} for r in range(1, PLANE)]
    right, left = {"tp": (x + 1) % n_x}, {"tp": (x + n_x - 1) % n_x}
    partners += [right, left]
    for who in partners:
        pl.semaphore_signal(barrier, inc=1, device_id=who, device_id_type=MESH)

    loads = [
        pltpu.make_async_copy(src, dst, m["in_sem"].at[i])
        for i, (src, dst) in enumerate(
            [
                (keys, m["kraw"]),
                (vals, m["vraw"]),
                (queries, m["qraw"]),
                (out_grad, m["graw"]),
                (log_sums, m["lraw"]),
                (inputs, m["xraw"].at[0]),
            ]
        )
    ]
    for copy in loads:
        copy.start()
    up_z = {"kv": (z + 1) % n_z * PLANE + q}
    dn_z = {"kv": (z + n_z - 1) % n_z * PLANE + q}
    lane = lax.broadcasted_iota(jnp.int32, (BLOCK, 128), 1)
    low = lane < HD
    loads[0].wait()
    loads[1].wait()
    for b in range(n_b):
        k = m["kraw"][b].astype(F32)
        v = m["vraw"][b].astype(F32)
        kv0 = jnp.where(low, k, pltpu.roll(v, HD, 1)).astype(BF16)
        kv1 = jnp.where(low, pltpu.roll(k, HD, 1), v).astype(BF16)
        m["own0"][b] = kv0
        m["own1"][b] = kv1
        m["tab0"][n_dev + b] = kv0
        m["tab1"][n_dev + b] = kv1
    pl.semaphore_wait(barrier, len(partners))

    def held(g, way, step):
        return m[f"own{g}"] if step == 0 else m[f"held{g}{way}{step}"]

    def z_copy(g, way, step, part):
        blocks = pl.ds(part * (n_b // PARTS), n_b // PARTS)
        return pltpu.make_async_remote_copy(
            src_ref=held(g, way, step - 1).at[blocks],
            dst_ref=held(g, way, step).at[blocks],
            send_sem=m["z_send"].at[g, way, step, part],
            recv_sem=m["z_recv"].at[g, way, step, part],
            device_id=dn_z if way else up_z,
            device_id_type=MESH,
        )

    def sends(way, step):
        if way:
            return (z + step - 1) % n_z < 3
        return (z < n_z - 1) & (z - step + 1 >= 0)

    def gets(way, step):
        if way:
            return (z + step) % n_z < 3
        return z - step >= 0

    def steps(way):
        return 3 if way else 4

    def x_copy(to_right, rel, part):
        half = inputs.shape[0] // 2
        rows = pl.ds(part * half, half)
        slot = rel if to_right else n_x - rel
        if rel == 1:
            src = inputs.at[rows]
        else:
            src = m["xraw"].at[1 if to_right else n_x - 1, rows]
        side = 0 if to_right else 1
        return pltpu.make_async_remote_copy(
            src_ref=src,
            dst_ref=m["xraw"].at[slot, rows],
            send_sem=m["x_send"].at[side, rel, part],
            recv_sem=m["x_recv"].at[side, rel, part],
            device_id=right if to_right else left,
            device_id_type=MESH,
        )

    def y_copy(g, order, z_from, r):
        to = (q + r) % PLANE
        return pltpu.make_async_remote_copy(
            src_ref=m["picked"].at[g, order, r],
            dst_ref=m[f"tab{g}"].at[z_from * PLANE + q],
            send_sem=m["y_send"].at[g, order],
            recv_sem=m["y_recv"].at[g, order],
            device_id={"kv": z * PLANE + to},
            device_id_type=MESH,
        )

    others = pl.ds(1, PLANE - 1)

    def wait_group(ref, sem):
        pltpu.make_async_copy(ref, ref, sem).wait()

    def pick(g, order, z_from, ref):
        def one(r, carry):
            to = (q + r) % PLANE
            m["picked"][g, order, r] = ref[idx_picks[(z_from * PLANE + to) * 2 + g]]

            @pl.when(r > 1)
            def _():
                y_copy(g, order, z_from, r - 1).start()

            return carry

        lax.fori_loop(1, PLANE, one, 0)
        m[f"tab{g}"][z_from * PLANE + q] = ref[idx_picks[(z_from * PLANE + q) * 2 + g]]
        y_copy(g, order, z_from, PLANE - 1).start()

    def each_piece(g, step, act):
        @pl.when(gets(0, step))
        def _():
            act(g, step, z - step, held(g, 0, step))

        if step < 4:
            @pl.when(gets(1, step) & (z + step >= n_z))
            def _():
                act(g, 4 + step, z + step - n_z, held(g, 1, step))

    def set_out(g):
        for part in range(PARTS):
            for way in range(2):
                @pl.when(sends(way, 1))
                def _():
                    z_copy(g, way, 1, part).start()

    set_out(0)
    for part in range(2):
        x_copy(True, 1, part).start()
        x_copy(False, 1, 1 - part).start()
    pick(0, 0, z, m["own0"])
    pick(1, 0, z, m["own1"])

    def relay(g, step):
        for part in range(PARTS):
            for way in range(2):
                if step <= steps(way):
                    @pl.when(gets(way, step))
                    def _():
                        z_copy(g, way, step, part).wait_recv()

                if step + 1 <= steps(way):
                    @pl.when(sends(way, step + 1))
                    def _():
                        z_copy(g, way, step + 1, part).start()

    key_at = lax.broadcasted_iota(jnp.int32, (BLOCK, cols), 0)
    tok_at = lax.broadcasted_iota(jnp.int32, (BLOCK, cols), 1) % BLOCK
    m["bias"][0] = jnp.zeros((BLOCK, cols), F32)
    m["bias"][1] = jnp.where(key_at <= tok_at, 0.0, NEG)
    m["bias"][2] = jnp.full((BLOCK, cols), NEG, F32)
    for p in range(n_b):
        m["terms"][p, n_list] = jnp.zeros((BLOCK, 128), F32)
    loads[4].wait()
    for p in range(n_b):
        for g in range(2):
            row = [
                m["lraw"][g * per_group + r : g * per_group + r + 1, p * BLOCK : (p + 1) * BLOCK]
                for r in range(per_group)
            ]
            m["lse"][p * 2 + g] = jnp.concatenate(row, axis=1)

    for step in range(1, 5):
        relay(0, step)
        if step == 2:
            set_out(1)
        each_piece(0, step, pick)

    def relay_and_pick(g, step):
        relay(g, step)
        each_piece(g, step, pick)

    def relay_x():
        x_copy(True, 1, 0).wait_recv()
        x_copy(True, 2, 0).start()
        x_copy(False, 1, 1).wait_recv()
        x_copy(False, 2, 1).start()

    def landed(g, order, z_from, ref):
        wait_group(m["picked"].at[g, order, others], m["y_recv"].at[g, order])

    def masked_rows(ref, row, g, factor, side):
        parts = []
        for r in range(per_group):
            col = (g * per_group + r) * HD
            part = ref[pl.ds(row, BLOCK), col // 128 * 128 : col // 128 * 128 + 128]
            part = part.astype(F32) * factor
            if r % 2 != side:
                part = pltpu.roll(part, HD, 1)
            parts.append(jnp.where(low != (side == 1), part, 0.0).astype(BF16))
        return parts

    def attention(g, between):
        tab = m[f"tab{g}"]
        sdp, pd, qd, cat, shift = m["sdp"], m["pd"], m["qd"], m["cat"], m["shift"]
        chunks = [slice(n, n + CHUNK) for n in range(0, n_list, CHUNK)]
        nt = (((1,), (1,)), ((), ()))
        nn = (((1,), (0,)), ((), ()))

        def one_position(p, carry):
            row = pl.multiple_of(p * BLOCK, BLOCK)
            unit = (p * 2 + g) * n_list
            for r, part in enumerate(masked_rows(m["qraw"], row, g, HD ** -0.5, 0)):
                qd[r * BLOCK : (r + 1) * BLOCK, :] = part
            for r, part in enumerate(masked_rows(m["graw"], row, g, 1.0, 1)):
                qd[cols + r * BLOCK : cols + (r + 1) * BLOCK, :] = part
            for n in range(n_list):
                cat[n] = tab[idx_slots[unit + n]]
            for kind in range(3):
                shift[kind] = m["bias"][kind] - m["lse"][p * 2 + g] * LOG2E

            acc = jnp.zeros((8, cols), F32)
            for ch in chunks:
                both = lax.dot_general(
                    cat[ch].reshape(CHUNK * BLOCK, 128), qd[...], nt, preferred_element_type=F32
                ).reshape(CHUNK, BLOCK, 2 * cols)
                for n in range(ch.start, ch.stop):
                    prod = both[n - ch.start]
                    pr = jnp.exp2(prod[:, :cols] * LOG2E + shift[idx_kinds[unit + n]])
                    sdp[n, :, :cols] = pr
                    sdp[n, :, cols:] = prod[:, cols:]
                    pd[n, :, cols:] = pr.astype(BF16)
                    pr = pr * prod[:, cols:]
                    acc = acc + pr.reshape(BLOCK // 8, 8, cols).sum(axis=0)
            delta = acc.sum(axis=0, keepdims=True)
            for ch in chunks:
                for n in range(ch.start, ch.stop):
                    ds = sdp[n, :, :cols] * (sdp[n, :, cols:] - delta)
                    pd[n, :, :cols] = ds.astype(BF16)
                m["terms"][p, ch] = lax.dot_general(
                    pd[ch].reshape(CHUNK * BLOCK, 2 * cols), qd[...], nn, preferred_element_type=F32
                ).reshape(CHUNK, BLOCK, 128)
            dq_t = lax.dot_general(
                cat[...].reshape(n_list * BLOCK, 128),
                pd[:, :, :cols].reshape(n_list * BLOCK, cols),
                (((0,), (0,)), ((), ())),
                preferred_element_type=F32,
            )
            dq = dq_t.T * (HD ** -0.5)
            for pair in range(per_group // 2):
                even = dq[(2 * pair) * BLOCK : (2 * pair + 1) * BLOCK]
                odd = dq[(2 * pair + 1) * BLOCK : (2 * pair + 2) * BLOCK]
                col = g * per_group * HD + pair * 128
                m["qg"][pl.ds(row, BLOCK), col : col + 128] = jnp.where(
                    low, even, pltpu.roll(odd, HD, 1)
                )
            for at, act in between.items():
                @pl.when(p == at)
                def _():
                    act()

            return carry

        lax.fori_loop(0, n_b, one_position, 0)

    def summed_terms(g, j):
        at = (g * (n_dev + n_b) + j) * n_b
        total = m["terms"][0, idx_inv[at]]
        for p in range(1, n_b):
            total = total + m["terms"][p, idx_inv[at + p]]
        return total

    def b_copy(g, d, r):
        to = (q + r) % PLANE
        return pltpu.make_async_remote_copy(
            src_ref=m["ret"].at[g, (z - d) * PLANE + to],
            dst_ref=m["back"].at[g, d, q],
            send_sem=m["b_send"].at[g, d],
            recv_sem=m["b_recv"].at[g, d],
            device_id={"kv": z * PLANE + to},
            device_id_type=MESH,
        )

    def give_back(g):
        for d in RETURN_ORDER:
            @pl.when(z - d >= 0)
            def _():
                for r in list(range(1, PLANE)) + [0]:
                    j = (z - d) * PLANE + (q + r) % PLANE
                    m["ret"][g, j] = summed_terms(g, j).astype(BF16)
                for r in range(1, PLANE):
                    b_copy(g, d, r).start()

        def own(b, carry):
            m["own_tot"][g, b] = summed_terms(g, n_dev + b)
            return carry

        lax.fori_loop(0, n_b, own, 0)

    def accumulate(g, d, part):
        rows = slice(part * 32, part * 32 + 32)
        accs = [jnp.zeros((32, 128), F32) for _ in range(n_b)]
        for r in range(PLANE):
            frm = (q + r) % PLANE
            if r == 0:
                val = m["ret"][g, (z - d) * PLANE + q, rows, :]
            else:
                val = m["back"][g, d, frm, rows, :]
            val = val.astype(F32)
            block = idx_picks[((z - d) * PLANE + frm) * 2 + g]
            for b in range(n_b):
                accs[b] = accs[b] + jnp.where(block == b, val, 0.0)
        for b in range(n_b):
            m["acc"][g, b, rows, :] = accs[b]

    def dn_copy(g, d, part):
        return pltpu.make_async_remote_copy(
            src_ref=m["zs"].at[g, d, part],
            dst_ref=m["zr_dn"].at[g, d - 1, part],
            send_sem=m["r_send"].at[g, d, part],
            recv_sem=m["r_recv_dn"].at[g, d - 1, part],
            device_id=dn_z,
            device_id_type=MESH,
        )

    def up_copy(g, e, part, passing=False):
        return pltpu.make_async_remote_copy(
            src_ref=m["zr_up"].at[g, e, part] if passing else m["zs"].at[g, n_z - e, part],
            dst_ref=m["zr_up"].at[g, e - 1, part],
            send_sem=m["r_send"].at[g, n_z - e, part],
            recv_sem=m["r_recv_up"].at[g, e - 1, part],
            device_id=up_z,
            device_id_type=MESH,
        )

    def add_arrival(g, copy, ref, part):
        copy.wait_recv()
        rows = slice(part * 32, part * 32 + 32)
        for b in range(n_b):
            m["acc"][g, b, rows, :] += ref[b].astype(F32)

    def dn_arrival(g, d, part):
        add_arrival(g, dn_copy(g, d + 1, part), m["zr_dn"].at[g, d, part], part)

    def up_arrival(g, e, part):
        add_arrival(g, up_copy(g, e + 1, part), m["zr_up"].at[g, e, part], part)

    def store_out(g, d, part):
        rows = slice(part * 32, part * 32 + 32)
        for b in range(n_b):
            m["zs"][g, d, part, b] = m["acc"][g, b, rows, :].astype(BF16)

    def collect(g, d):
        e = n_z - d

        @pl.when(z - d >= 0)
        def _():
            wait_group(m["back"].at[g, d, others], m["b_recv"].at[g, d])
            for part in range(2):
                accumulate(g, d, part)
                if d > 4:
                    if e < 3:
                        up_arrival(g, e, part)
                    store_out(g, d, part)
                    up_copy(g, e, part).start()
                else:
                    if d < 4:
                        @pl.when(z < n_z - 1)
                        def _():
                            dn_arrival(g, d, part)
                    if d > 0:
                        store_out(g, d, part)
                        dn_copy(g, d, part).start()

        if d > 4 and e < 3:
            @pl.when(z < 3 - e)
            def _():
                for part in range(2):
                    up_copy(g, e + 1, part).wait_recv()
                    up_copy(g, e, part, passing=True).start()

        if d == 0:
            @pl.when(z < 3)
            def _():
                for part in range(2):
                    up_arrival(g, 0, part)

    def wait_fetch(g):
        landed(g, 0, z, None)
        for step in range(1, 5):
            each_piece(g, step, landed)

    relay_and_pick(1, 1)
    loads[2].wait()
    loads[3].wait()
    wait_fetch(0)
    attention(
        0,
        {
            0: functools.partial(relay_and_pick, 1, 2),
            1: functools.partial(relay_and_pick, 1, 3),
            3: functools.partial(relay_and_pick, 1, 4),
            4: relay_x,
        },
    )
    give_back(0)
    wait_fetch(1)
    attention(1, {2 + i: functools.partial(collect, 0, RETURN_ORDER[i]) for i in range(4)})
    give_back(1)
    out_q = pltpu.make_async_copy(m["qg"], query_grad, m["out_sem"].at[0])
    out_q.start()
    collect(0, 2)
    collect(1, 4)
    collect(0, 7)
    collect(1, 5)
    collect(0, 1)
    collect(1, 3)
    collect(0, 0)
    for d in RETURN_ORDER[3:]:
        collect(1, d)

    for b in range(n_b):
        rows = slice(b * BLOCK, (b + 1) * BLOCK)
        t0 = m["acc"][0, b] + m["own_tot"][0, b]
        t1 = m["acc"][1, b] + m["own_tot"][1, b]
        kg = jnp.where(low, t0, pltpu.roll(t1, HD, 1))
        key_grad[rows, :] = kg
        value_grad[rows, :] = jnp.where(low, pltpu.roll(t0, HD, 1), t1)
        m["kg"][rows, :] = kg.astype(BF16)

    def c_copy(i):
        return pltpu.make_async_remote_copy(
            src_ref=m["wpart"].at[i, 1 - c],
            dst_ref=m["crecv"].at[i],
            send_sem=m["c_send"].at[i],
            recv_sem=m["c_recv"].at[i],
            device_id={"kv": z * PLANE + y * N_C + (1 - c)},
            device_id_type=MESH,
        )

    x_copy(True, 1, 1).wait_recv()
    x_copy(False, 1, 0).wait_recv()
    x_copy(True, 2, 0).wait_recv()
    x_copy(False, 2, 1).wait_recv()
    loads[5].wait()
    kg_t = m["kg"][...].T
    half = inputs.shape[1] // 2
    n_i = 2 * n_x

    def wy_copy(part, r):
        to = (y + r) % N_Y
        return pltpu.make_async_remote_copy(
            src_ref=m["wy"].at[part, r],
            dst_ref=m["wyr"].at[part, r],
            send_sem=m["wy_send"].at[part, r],
            recv_sem=m["wy_recv"].at[part, r],
            device_id={"kv": z * PLANE + to * N_C + c},
            device_id_type=MESH,
        )

    def own_terms(i):
        rel, h = i // 2, i % 2
        w_t = lax.dot_general(
            kg_t, m["xraw"][rel, :, h * half : (h + 1) * half], (((1,), (0,)), ((), ())),
            preferred_element_type=F32,
        )
        w = w_t.T.astype(BF16)
        for yy in range(N_Y):
            for cc in range(N_C):
                first = (yy * N_C + cc) * BLOCK
                m["wpart"][i, cc, yy] = w[first : first + BLOCK]

    def core_sum(i):
        c_copy(i).wait_recv()
        for r in range(N_Y):
            yy = (y + r) % N_Y
            both = m["wpart"][i, c, yy].astype(F32) + m["crecv"][i, yy].astype(F32)
            if r:
                m["wy"][i // 2, r, i % 2] = both.astype(BF16)
            else:
                m["wy_own"][i] = both

    lag = 3
    for i in range(n_i + lag):
        if i < n_i:
            own_terms(i)
        if 0 < i <= n_i:
            c_copy(i - 1).start()
        if i >= lag:
            core_sum(i - lag)
            if (i - lag) % 2:
                for r in (2, 1, 3):
                    wy_copy((i - lag) // 2, r).start()

    def z_of(i):
        return 2 * ((x + n_x - i // 2) % n_x) + i % 2

    def wz_copy(i):
        return pltpu.make_async_remote_copy(
            src_ref=m["wz"].at[i],
            dst_ref=m["wzr"].at[z],
            send_sem=m["wz_send"].at[i],
            recv_sem=m["wz_recv"].at[z],
            device_id={"kv": z_of(i) * PLANE + q},
            device_id_type=MESH,
        )

    def sent(g, order, z_from, ref):
        wait_group(m["picked"].at[g, order, others], m["y_send"].at[g, order])

    for g in range(2):
        for way in range(2):
            for step in range(1, steps(way) + 1):
                @pl.when(sends(way, step))
                def _():
                    for part in range(PARTS):
                        z_copy(g, way, step, part).wait_send()

        sent(g, 0, z, None)
        for step in range(1, 5):
            each_piece(g, step, sent)
        for d in range(8):
            @pl.when(z - d >= 0)
            def _():
                wait_group(m["back"].at[g, d, others], m["b_send"].at[g, d])

            for part in range(2):
                if 0 < d < 5:
                    @pl.when(z - d >= 0)
                    def _():
                        dn_copy(g, d, part).wait_send()
                elif d:
                    e = n_z - d
                    @pl.when((z - d >= 0) | (z < 3 - e))
                    def _():
                        up_copy(g, e, part).wait_send()

    for part in range(2):
        x_copy(True, 1, part).wait_send()
        x_copy(False, 1, part).wait_send()
    x_copy(True, 2, 0).wait_send()
    x_copy(False, 2, 1).wait_send()
    for i in range(n_i):
        c_copy(i).wait_send()
    out_q.wait()

    for part in range(n_x):
        for r in (1, 3, 2):
            wy_copy(part, r).wait_recv()
        for i in (2 * part, 2 * part + 1):
            total = m["wy_own"][i]
            for r in range(1, N_Y):
                total = total + m["wyr"][part, r, i % 2].astype(F32)
            m["wz_own"][i] = total
            m["wz"][i] = total.astype(BF16)
        for i in (2 * part, 2 * part + 1):
            @pl.when(z_of(i) != z)
            def _():
                wz_copy(i).start()
    for part in range(n_x):
        for r in range(1, N_Y):
            wy_copy(part, r).wait_send()
    mine = 2 * ((x + n_x - z // 2) % n_x) + z % 2
    total = m["wz_own"][mine]
    for r in range(1, n_z):
        frm = (z + r) % n_z
        pltpu.make_async_remote_copy(
            src_ref=m["wz"].at[0],
            dst_ref=m["wzr"].at[frm],
            send_sem=m["wz_send"].at[0],
            recv_sem=m["wz_recv"].at[frm],
            device_id={"kv": frm * PLANE + q},
            device_id_type=MESH,
        ).wait_recv()
        total = total + m["wzr"][frm].astype(F32)
    weight_grad[...] = total
    for i in range(n_i):
        @pl.when(z_of(i) != z)
        def _():
            wz_copy(i).wait_send()


def put_kernel(q_src, k_src, v_src, w_src, q_dst, k_dst, v_dst, w_dst, q_mid, sem):
    rows = q_mid.shape[0] // 3
    part = [pl.ds(i * rows, rows) for i in range(3)]
    into = [
        pltpu.make_async_copy(q_src.at[part[i]], q_mid.at[part[i]], sem.at[i]) for i in range(3)
    ]
    rest = [
        pltpu.make_async_copy(src, dst, sem.at[3 + i])
        for i, (src, dst) in enumerate([(k_src, k_dst), (v_src, v_dst), (w_src, w_dst)])
    ]
    out = [
        pltpu.make_async_copy(q_mid.at[part[i]], q_dst.at[part[i]], sem.at[6 + i]) for i in range(3)
    ]
    for copy in into + rest:
        copy.start()
    for i in range(3):
        into[i].wait()
        out[i].start()
    for copy in rest + out:
        copy.wait()


def put_out(query_grad, key_grad, value_grad, weight_grad):
    hbm = pl.BlockSpec(memory_space=pltpu.HBM)
    vm = pl.BlockSpec(memory_space=pltpu.VMEM)
    arrays = (query_grad, key_grad, value_grad, weight_grad)
    return pl.pallas_call(
        put_kernel,
        out_shape=tuple(jax.ShapeDtypeStruct(a.shape, a.dtype) for a in arrays),
        in_specs=[hbm, vm, vm, vm],
        out_specs=(hbm,) * 4,
        scratch_shapes=[pltpu.VMEM(query_grad.shape, F32), pltpu.SemaphoreType.DMA((9,))],
        compiler_params=pltpu.CompilerParams(vmem_limit_bytes=int(53.4 * 1024 * 1024)),
        name="put_out",
    )(*arrays)


def index_table(chosen, n_b, n_dev):
    groups, _, n_list = chosen.shape
    me = lax.axis_index("kv")
    z, q = place()
    plane = lax.dynamic_slice_in_dim(chosen, z * PLANE * n_b, PLANE * n_b, 1)
    column = (jnp.arange(n_dev // PLANE) * PLANE + q) * n_b
    offs = plane[..., None] - column
    offs = jnp.where((offs >= 0) & (offs < n_b), offs, 0)
    picks = jnp.max(offs.reshape(groups, PLANE, n_b * n_list, -1), axis=2)
    picks = picks.transpose(2, 1, 0).reshape(-1)
    lists = lax.dynamic_slice_in_dim(chosen, me * n_b, n_b, 1)
    owner = lists // n_b
    slot = jnp.where(owner == me, n_dev + lists % n_b, jnp.maximum(owner, 0))
    at_diag = lists == me * n_b + jnp.arange(n_b)[None, :, None]
    kind = jnp.where(lists < 0, 2, at_diag.astype(jnp.int32))
    listed = (slot[..., None] == jnp.arange(n_dev + n_b)) & (lists >= 0)[..., None]
    inverse = jnp.min(
        jnp.where(listed, jnp.arange(n_list)[:, None], n_list), axis=2
    )
    slots = slot.transpose(1, 0, 2).reshape(-1)
    kinds = kind.transpose(1, 0, 2).reshape(-1)
    inverse = inverse.transpose(0, 2, 1).reshape(-1)
    return picks, slots, kinds, inverse


def local(queries, key_heads, values, log_sums, out_grad, inputs, chosen):
    n_dev = lax.axis_size("kv")
    n_x = lax.axis_size("tp")
    rows, feats = inputs.shape
    n_b = rows // BLOCK
    heads = log_sums.shape[0]
    n_list = chosen.shape[2]
    idx = index_table(chosen, n_b, n_dev)
    scratch = scratch_list(rows, n_dev, n_x, n_list, feats, heads)
    hbm = pl.BlockSpec(memory_space=pltpu.HBM)
    vm = pl.BlockSpec(memory_space=pltpu.VMEM)
    results = pl.pallas_call(
        functools.partial(
            fused_kernel, [name for name, _ in scratch], n_dev // PLANE, n_x, n_list
        ),
        out_shape=(
            jax.ShapeDtypeStruct(queries.shape, F32),
            jax.ShapeDtypeStruct(key_heads.shape, F32),
            jax.ShapeDtypeStruct(values.shape, F32),
            jax.ShapeDtypeStruct((feats * n_x // n_dev, 128), F32),
        ),
        in_specs=[pl.BlockSpec(memory_space=pltpu.SMEM)] * 4 + [hbm] * 6,
        out_specs=(hbm, vm, vm, vm),
        scratch_shapes=[kind for _, kind in scratch],
        compiler_params=pltpu.CompilerParams(
            collective_id=0, has_side_effects=True, vmem_limit_bytes=53 * 1024 * 1024
        ),
        name="fused",
    )(
        *idx,
        key_heads.reshape(n_b, BLOCK, -1),
        values.reshape(n_b, BLOCK, -1),
        queries,
        out_grad,
        log_sums,
        inputs,
    )
    return put_out(*results)


def solution(mesh):
    placed = (
        P("kv", "tp"),
        P("kv", "tp"),
        P("kv", "tp"),
        P("tp", "kv"),
        P("kv", "tp"),
        P("kv", "tp"),
        P("tp", None, None),
    )
    return jax.shard_map(
        local,
        mesh=mesh,
        in_specs=placed,
        out_specs=(P("kv", "tp"), P("kv", "tp"), P("kv", "tp"), P("kv", "tp")),
        check_vma=False,
    )
```

```python
import functools

import jax
import jax.numpy as jnp
from jax import lax
from jax.experimental import pallas as pl
from jax.experimental.pallas import tpu as pltpu
from jax.sharding import PartitionSpec as P

HD = 64
BLOCK = 64
NEG = -1e30
LOG2E = 1.4426950408889634
CHUNK = 4
PARTS = 3
N_Y = 4
N_C = 2
PLANE = N_Y * N_C
MESH = pl.DeviceIdType.MESH
RETURN_ORDER = (4, 5, 3, 6, 2, 7, 1, 0)
F32, BF16 = jnp.float32, jnp.bfloat16


def place():
    me = lax.axis_index("kv")
    return me // PLANE, me % PLANE


def scratch_list(rows, n_dev, n_x, n_list, feats, heads):
    n_b = rows // BLOCK
    tile = (BLOCK, 128)
    cols = heads // 2 * BLOCK
    dma = pltpu.SemaphoreType.DMA
    out = [
        ("kraw", pltpu.VMEM((n_b,) + tile, BF16)),
        ("vraw", pltpu.VMEM((n_b,) + tile, BF16)),
        ("qraw", pltpu.VMEM((rows, heads * HD), BF16)),
        ("graw", pltpu.VMEM((rows, heads * HD), BF16)),
        ("lraw", pltpu.VMEM((heads, rows), F32)),
        ("xraw", pltpu.VMEM((n_x, rows, feats), BF16)),
        ("lse", pltpu.VMEM((n_b * 2, 1, cols), F32)),
        ("bias", pltpu.VMEM((3,) + (BLOCK, cols), F32)),
        ("shift", pltpu.VMEM((3,) + (BLOCK, cols), F32)),
        ("qg", pltpu.VMEM((rows, heads * HD), F32)),
        ("picked", pltpu.VMEM((2, 8, PLANE) + tile, BF16)),
        ("qd", pltpu.VMEM((2 * cols, 128), BF16)),
        ("cat", pltpu.VMEM((n_list,) + tile, BF16)),
        ("sdp", pltpu.VMEM((n_list, BLOCK, 2 * cols), F32)),
        ("pd", pltpu.VMEM((n_list, BLOCK, 2 * cols), BF16)),
        ("terms", pltpu.VMEM((n_b, n_list + 1) + tile, F32)),
        ("ret", pltpu.VMEM((2, n_dev) + tile, BF16)),
        ("own_tot", pltpu.VMEM((2, n_b) + tile, F32)),
        ("back", pltpu.VMEM((2, 8, PLANE) + tile, BF16)),
        ("acc", pltpu.VMEM((2, n_b) + tile, F32)),
        ("zs", pltpu.VMEM((2, 8, 2, n_b, BLOCK // 2, 128), BF16)),
        ("zr_dn", pltpu.VMEM((2, 4, 2, n_b, BLOCK // 2, 128), BF16)),
        ("zr_up", pltpu.VMEM((2, 3, 2, n_b, BLOCK // 2, 128), BF16)),
        ("kg", pltpu.VMEM((rows, 128), BF16)),
        ("wpart", pltpu.VMEM((8, N_C, N_Y) + tile, BF16)),
        ("crecv", pltpu.VMEM((8, N_Y) + tile, BF16)),
        ("wy", pltpu.VMEM((4, N_Y, 2) + tile, BF16)),
        ("wy_own", pltpu.VMEM((8,) + tile, F32)),
        ("wyr", pltpu.VMEM((4, N_Y, 2) + tile, BF16)),
        ("wz", pltpu.VMEM((8,) + tile, BF16)),
        ("wz_own", pltpu.VMEM((8,) + tile, F32)),
        ("wzr", pltpu.VMEM((8,) + tile, BF16)),
        ("in_sem", dma((6,))),
        ("out_sem", dma((1,))),
        ("z_send", dma((2, 2, 5, PARTS))),
        ("z_recv", dma((2, 2, 5, PARTS))),
        ("y_send", dma((2, 8))),
        ("y_recv", dma((2, 8))),
        ("x_send", dma((2, 3, 2))),
        ("x_recv", dma((2, 3, 2))),
        ("b_send", dma((2, 8))),
        ("b_recv", dma((2, 8))),
        ("r_send", dma((2, 8, 2))),
        ("r_recv_dn", dma((2, 4, 2))),
        ("r_recv_up", dma((2, 3, 2))),
        ("c_send", dma((8,))),
        ("c_recv", dma((8,))),
        ("wy_send", dma((4, N_Y))),
        ("wy_recv", dma((4, N_Y))),
        ("wz_send", dma((8,))),
        ("wz_recv", dma((8,))),
    ]
    for g in range(2):
        out.append((f"own{g}", pltpu.VMEM((n_b,) + tile, BF16)))
        out.append((f"tab{g}", pltpu.VMEM((n_dev + n_b,) + tile, BF16)))
        for step in range(1, 5):
            out.append((f"held{g}0{step}", pltpu.VMEM((n_b,) + tile, BF16)))
        for step in range(1, 4):
            out.append((f"held{g}1{step}", pltpu.VMEM((n_b,) + tile, BF16)))
    return out


def fused_kernel(names, n_z, n_x, n_list, *refs):
    idx_picks, idx_slots, idx_kinds, idx_inv = refs[:4]
    keys, vals, queries, out_grad, log_sums, inputs = refs[4:10]
    query_grad, key_grad, value_grad, weight_grad = refs[10:14]
    m = dict(zip(names, refs[14:]))
    n_b = m["kraw"].shape[0]
    n_dev = n_z * PLANE
    heads = m["lraw"].shape[0]
    per_group = heads // 2
    cols = per_group * BLOCK
    z, q = place()
    y, c = q // N_C, q % N_C
    x = lax.axis_index("tp")

    barrier = pltpu.get_barrier_semaphore()
    partners = [{"kv": (z + r) % n_z * PLANE + q} for r in range(1, n_z)]
    partners += [{"kv": z * PLANE + (q + r) % PLANE} for r in range(1, PLANE)]
    right, left = {"tp": (x + 1) % n_x}, {"tp": (x + n_x - 1) % n_x}
    partners += [right, left]
    for who in partners:
        pl.semaphore_signal(barrier, inc=1, device_id=who, device_id_type=MESH)

    loads = [
        pltpu.make_async_copy(src, dst, m["in_sem"].at[i])
        for i, (src, dst) in enumerate(
            [
                (keys, m["kraw"]),
                (vals, m["vraw"]),
                (queries, m["qraw"]),
                (out_grad, m["graw"]),
                (log_sums, m["lraw"]),
                (inputs, m["xraw"].at[0]),
            ]
        )
    ]
    for copy in loads:
        copy.start()
    up_z = {"kv": (z + 1) % n_z * PLANE + q}
    dn_z = {"kv": (z + n_z - 1) % n_z * PLANE + q}
    lane = lax.broadcasted_iota(jnp.int32, (BLOCK, 128), 1)
    low = lane < HD
    loads[0].wait()
    loads[1].wait()
    for b in range(n_b):
        k = m["kraw"][b].astype(F32)
        v = m["vraw"][b].astype(F32)
        kv0 = jnp.where(low, k, pltpu.roll(v, HD, 1)).astype(BF16)
        kv1 = jnp.where(low, pltpu.roll(k, HD, 1), v).astype(BF16)
        m["own0"][b] = kv0
        m["own1"][b] = kv1
        m["tab0"][n_dev + b] = kv0
        m["tab1"][n_dev + b] = kv1
    pl.semaphore_wait(barrier, len(partners))

    def held(g, way, step):
        return m[f"own{g}"] if step == 0 else m[f"held{g}{way}{step}"]

    def z_copy(g, way, step, part):
        blocks = pl.ds(part * (n_b // PARTS), n_b // PARTS)
        return pltpu.make_async_remote_copy(
            src_ref=held(g, way, step - 1).at[blocks],
            dst_ref=held(g, way, step).at[blocks],
            send_sem=m["z_send"].at[g, way, step, part],
            recv_sem=m["z_recv"].at[g, way, step, part],
            device_id=dn_z if way else up_z,
            device_id_type=MESH,
        )

    def sends(way, step):
        if way:
            return gets(1, step - 1) & (z > n_z - 3)
        return (z < n_z - 1) & (z - step + 1 >= 0)

    def gets(way, step):
        if way:
            return (z + step >= n_z) & (z + step < n_z + 3)
        return z - step >= 0

    def top_copy(g, part):
        blocks = pl.ds(part * (n_b // PARTS), n_b // PARTS)
        out = []
        for step in range(1, 4):
            out.append(
                pltpu.make_async_remote_copy(
                    src_ref=m[f"own{g}"].at[blocks],
                    dst_ref=held(g, 1, step).at[blocks],
                    send_sem=m["z_send"].at[g, 1, 0, part],
                    recv_sem=m["z_recv"].at[g, 1, step, part],
                    device_id={"kv": (n_z - 1) * PLANE + q},
                    device_id_type=MESH,
                )
            )
        return out

    def steps(way):
        return 3 if way else 4

    def x_copy(to_right, rel, part):
        half = inputs.shape[0] // 2
        rows = pl.ds(part * half, half)
        slot = rel if to_right else n_x - rel
        if rel == 1:
            src = inputs.at[rows]
        else:
            src = m["xraw"].at[1 if to_right else n_x - 1, rows]
        side = 0 if to_right else 1
        return pltpu.make_async_remote_copy(
            src_ref=src,
            dst_ref=m["xraw"].at[slot, rows],
            send_sem=m["x_send"].at[side, rel, part],
            recv_sem=m["x_recv"].at[side, rel, part],
            device_id=right if to_right else left,
            device_id_type=MESH,
        )

    def y_copy(g, order, z_from, r):
        to = (q + r) % PLANE
        return pltpu.make_async_remote_copy(
            src_ref=m["picked"].at[g, order, r],
            dst_ref=m[f"tab{g}"].at[z_from * PLANE + q],
            send_sem=m["y_send"].at[g, order],
            recv_sem=m["y_recv"].at[g, order],
            device_id={"kv": z * PLANE + to},
            device_id_type=MESH,
        )

    others = pl.ds(1, PLANE - 1)

    def wait_group(ref, sem):
        pltpu.make_async_copy(ref, ref, sem).wait()

    def pick(g, order, z_from, ref):
        def one(r, carry):
            to = (q + r) % PLANE
            m["picked"][g, order, r] = ref[idx_picks[(z_from * PLANE + to) * 2 + g]]

            @pl.when(r > 1)
            def _():
                y_copy(g, order, z_from, r - 1).start()

            return carry

        lax.fori_loop(1, PLANE, one, 0)
        m[f"tab{g}"][z_from * PLANE + q] = ref[idx_picks[(z_from * PLANE + q) * 2 + g]]
        y_copy(g, order, z_from, PLANE - 1).start()

    def each_piece(g, step, act):
        @pl.when(gets(0, step))
        def _():
            act(g, step, z - step, held(g, 0, step))

        if step < 4:
            @pl.when(gets(1, step))
            def _():
                act(g, 4 + step, z + step - n_z, held(g, 1, step))

    def set_out(g):
        for part in range(PARTS):
            @pl.when(sends(0, 1))
            def _():
                z_copy(g, 0, 1, part).start()

            for step, copy in enumerate(top_copy(g, part), 1):
                @pl.when(z == step - 1)
                def _():
                    copy.start()

    set_out(0)
    for part in range(2):
        x_copy(True, 1, part).start()
        x_copy(False, 1, 1 - part).start()
    pick(0, 0, z, m["own0"])
    pick(1, 0, z, m["own1"])

    def relay(g, step):
        for part in range(PARTS):
            for way in range(2):
                if step <= steps(way):
                    @pl.when(gets(way, step))
                    def _():
                        z_copy(g, way, step, part).wait_recv()

                if step + 1 <= steps(way):
                    @pl.when(sends(way, step + 1))
                    def _():
                        z_copy(g, way, step + 1, part).start()

    key_at = lax.broadcasted_iota(jnp.int32, (BLOCK, cols), 0)
    tok_at = lax.broadcasted_iota(jnp.int32, (BLOCK, cols), 1) % BLOCK
    m["bias"][0] = jnp.zeros((BLOCK, cols), F32)
    m["bias"][1] = jnp.where(key_at <= tok_at, 0.0, NEG)
    m["bias"][2] = jnp.full((BLOCK, cols), NEG, F32)
    for p in range(n_b):
        m["terms"][p, n_list] = jnp.zeros((BLOCK, 128), F32)
    loads[4].wait()
    for p in range(n_b):
        for g in range(2):
            row = [
                m["lraw"][g * per_group + r : g * per_group + r + 1, p * BLOCK : (p + 1) * BLOCK]
                for r in range(per_group)
            ]
            m["lse"][p * 2 + g] = jnp.concatenate(row, axis=1)

    for step in range(1, 5):
        relay(0, step)
        if step == 2:
            set_out(1)
        each_piece(0, step, pick)

    def relay_and_pick(g, step):
        relay(g, step)
        each_piece(g, step, pick)

    def relay_x():
        x_copy(True, 1, 0).wait_recv()
        x_copy(True, 2, 0).start()
        x_copy(False, 1, 1).wait_recv()
        x_copy(False, 2, 1).start()

    def landed(g, order, z_from, ref):
        wait_group(m["picked"].at[g, order, others], m["y_recv"].at[g, order])

    def masked_rows(ref, row, g, factor, side):
        parts = []
        for r in range(per_group):
            col = (g * per_group + r) * HD
            part = ref[pl.ds(row, BLOCK), col // 128 * 128 : col // 128 * 128 + 128]
            part = part.astype(F32) * factor
            if r % 2 != side:
                part = pltpu.roll(part, HD, 1)
            parts.append(jnp.where(low != (side == 1), part, 0.0).astype(BF16))
        return parts

    def attention(g, between):
        tab = m[f"tab{g}"]
        sdp, pd, qd, cat, shift = m["sdp"], m["pd"], m["qd"], m["cat"], m["shift"]
        chunks = [slice(n, n + CHUNK) for n in range(0, n_list, CHUNK)]
        nt = (((1,), (1,)), ((), ()))
        nn = (((1,), (0,)), ((), ()))

        def one_position(p, carry):
            row = pl.multiple_of(p * BLOCK, BLOCK)
            unit = (p * 2 + g) * n_list
            for r, part in enumerate(masked_rows(m["qraw"], row, g, HD ** -0.5, 0)):
                qd[r * BLOCK : (r + 1) * BLOCK, :] = part
            for r, part in enumerate(masked_rows(m["graw"], row, g, 1.0, 1)):
                qd[cols + r * BLOCK : cols + (r + 1) * BLOCK, :] = part
            for n in range(n_list):
                cat[n] = tab[idx_slots[unit + n]]
            for kind in range(3):
                shift[kind] = m["bias"][kind] - m["lse"][p * 2 + g] * LOG2E

            acc = jnp.zeros((8, cols), F32)
            for ch in chunks:
                both = lax.dot_general(
                    cat[ch].reshape(CHUNK * BLOCK, 128), qd[...], nt, preferred_element_type=F32
                ).reshape(CHUNK, BLOCK, 2 * cols)
                for n in range(ch.start, ch.stop):
                    prod = both[n - ch.start]
                    pr = jnp.exp2(prod[:, :cols] * LOG2E + shift[idx_kinds[unit + n]])
                    sdp[n, :, :cols] = pr
                    sdp[n, :, cols:] = prod[:, cols:]
                    pd[n, :, cols:] = pr.astype(BF16)
                    pr = pr * prod[:, cols:]
                    acc = acc + pr.reshape(BLOCK // 8, 8, cols).sum(axis=0)
            delta = acc.sum(axis=0, keepdims=True)
            for ch in chunks:
                for n in range(ch.start, ch.stop):
                    ds = sdp[n, :, :cols] * (sdp[n, :, cols:] - delta)
                    pd[n, :, :cols] = ds.astype(BF16)
                m["terms"][p, ch] = lax.dot_general(
                    pd[ch].reshape(CHUNK * BLOCK, 2 * cols), qd[...], nn, preferred_element_type=F32
                ).reshape(CHUNK, BLOCK, 128)
            dq_t = lax.dot_general(
                cat[...].reshape(n_list * BLOCK, 128),
                pd[:, :, :cols].reshape(n_list * BLOCK, cols),
                (((0,), (0,)), ((), ())),
                preferred_element_type=F32,
            )
            dq = dq_t.T * (HD ** -0.5)
            for pair in range(per_group // 2):
                even = dq[(2 * pair) * BLOCK : (2 * pair + 1) * BLOCK]
                odd = dq[(2 * pair + 1) * BLOCK : (2 * pair + 2) * BLOCK]
                col = g * per_group * HD + pair * 128
                m["qg"][pl.ds(row, BLOCK), col : col + 128] = jnp.where(
                    low, even, pltpu.roll(odd, HD, 1)
                )
            for at, act in between.items():
                @pl.when(p == at)
                def _():
                    act()

            return carry

        lax.fori_loop(0, n_b, one_position, 0)

    def summed_terms(g, j):
        at = (g * (n_dev + n_b) + j) * n_b
        total = m["terms"][0, idx_inv[at]]
        for p in range(1, n_b):
            total = total + m["terms"][p, idx_inv[at + p]]
        return total

    def b_copy(g, d, r):
        to = (q + r) % PLANE
        return pltpu.make_async_remote_copy(
            src_ref=m["ret"].at[g, (z - d) * PLANE + to],
            dst_ref=m["back"].at[g, d, q],
            send_sem=m["b_send"].at[g, d],
            recv_sem=m["b_recv"].at[g, d],
            device_id={"kv": z * PLANE + to},
            device_id_type=MESH,
        )

    def give_back(g):
        for d in RETURN_ORDER:
            @pl.when(z - d >= 0)
            def _():
                for r in list(range(1, PLANE)) + [0]:
                    j = (z - d) * PLANE + (q + r) % PLANE
                    m["ret"][g, j] = summed_terms(g, j).astype(BF16)
                for r in range(1, PLANE):
                    b_copy(g, d, r).start()

        def own(b, carry):
            m["own_tot"][g, b] = summed_terms(g, n_dev + b)
            return carry

        lax.fori_loop(0, n_b, own, 0)

    def accumulate(g, d, part):
        rows = slice(part * 32, part * 32 + 32)
        accs = [jnp.zeros((32, 128), F32) for _ in range(n_b)]
        for r in range(PLANE):
            frm = (q + r) % PLANE
            if r == 0:
                val = m["ret"][g, (z - d) * PLANE + q, rows, :]
            else:
                val = m["back"][g, d, frm, rows, :]
            val = val.astype(F32)
            block = idx_picks[((z - d) * PLANE + frm) * 2 + g]
            for b in range(n_b):
                accs[b] = accs[b] + jnp.where(block == b, val, 0.0)
        for b in range(n_b):
            m["acc"][g, b, rows, :] = accs[b]

    def dn_copy(g, d, part):
        return pltpu.make_async_remote_copy(
            src_ref=m["zs"].at[g, d, part],
            dst_ref=m["zr_dn"].at[g, d - 1, part],
            send_sem=m["r_send"].at[g, d, part],
            recv_sem=m["r_recv_dn"].at[g, d - 1, part],
            device_id=dn_z,
            device_id_type=MESH,
        )

    def up_copy(g, e, part, last=False):
        d = n_z - e
        at = 0 if last else e - 1
        return pltpu.make_async_remote_copy(
            src_ref=m["zs"].at[g, d, part],
            dst_ref=m["zr_up"].at[g, at, part],
            send_sem=m["r_send"].at[g, d, part],
            recv_sem=m["r_recv_up"].at[g, at, part],
            device_id={"kv": (n_z - 1 - d) * PLANE + q} if last else up_z,
            device_id_type=MESH,
        )

    def add_arrival(g, copy, ref, part):
        copy.wait_recv()
        rows = slice(part * 32, part * 32 + 32)
        for b in range(n_b):
            m["acc"][g, b, rows, :] += ref[b].astype(F32)

    def dn_arrival(g, d, part):
        add_arrival(g, dn_copy(g, d + 1, part), m["zr_dn"].at[g, d, part], part)

    def up_arrival(g, e, part):
        add_arrival(g, up_copy(g, e + 1, part), m["zr_up"].at[g, e, part], part)

    def store_out(g, d, part):
        rows = slice(part * 32, part * 32 + 32)
        for b in range(n_b):
            m["zs"][g, d, part, b] = m["acc"][g, b, rows, :].astype(BF16)

    def collect(g, d):
        e = n_z - d

        @pl.when(z - d >= 0)
        def _():
            wait_group(m["back"].at[g, d, others], m["b_recv"].at[g, d])
            for part in range(2):
                accumulate(g, d, part)
                if d > 4:
                    if e < 3:
                        up_arrival(g, e, part)
                    store_out(g, d, part)

                    @pl.when(z == n_z - 1)
                    def _():
                        up_copy(g, e, part, last=True).start()

                    if e > 1:
                        @pl.when(z < n_z - 1)
                        def _():
                            up_copy(g, e, part).start()
                else:
                    if d < 4:
                        @pl.when(z < n_z - 1)
                        def _():
                            dn_arrival(g, d, part)
                    if d > 0:
                        store_out(g, d, part)
                        dn_copy(g, d, part).start()

        if d == 0:
            @pl.when(z < 3)
            def _():
                for part in range(2):
                    up_arrival(g, 0, part)

    def wait_fetch(g):
        landed(g, 0, z, None)
        for step in range(1, 5):
            each_piece(g, step, landed)

    relay_and_pick(1, 1)
    relay_and_pick(1, 2)
    loads[2].wait()
    loads[3].wait()
    wait_fetch(0)
    attention(
        0,
        {
            0: functools.partial(relay_and_pick, 1, 3),
            2: functools.partial(relay_and_pick, 1, 4),
            4: relay_x,
        },
    )
    give_back(0)
    wait_fetch(1)
    attention(1, {2 + i: functools.partial(collect, 0, RETURN_ORDER[i]) for i in range(4)})
    give_back(1)
    out_q = pltpu.make_async_copy(m["qg"], query_grad, m["out_sem"].at[0])
    out_q.start()
    collect(0, 2)
    collect(1, 4)
    collect(0, 7)
    collect(1, 5)
    collect(0, 1)
    collect(1, 3)
    collect(0, 0)
    for d in RETURN_ORDER[3:]:
        collect(1, d)

    for b in range(n_b):
        rows = slice(b * BLOCK, (b + 1) * BLOCK)
        t0 = m["acc"][0, b] + m["own_tot"][0, b]
        t1 = m["acc"][1, b] + m["own_tot"][1, b]
        kg = jnp.where(low, t0, pltpu.roll(t1, HD, 1))
        key_grad[rows, :] = kg
        value_grad[rows, :] = jnp.where(low, pltpu.roll(t0, HD, 1), t1)
        m["kg"][rows, :] = kg.astype(BF16)

    def c_copy(i):
        return pltpu.make_async_remote_copy(
            src_ref=m["wpart"].at[i, 1 - c],
            dst_ref=m["crecv"].at[i],
            send_sem=m["c_send"].at[i],
            recv_sem=m["c_recv"].at[i],
            device_id={"kv": z * PLANE + y * N_C + (1 - c)},
            device_id_type=MESH,
        )

    x_copy(True, 1, 1).wait_recv()
    x_copy(False, 1, 0).wait_recv()
    x_copy(True, 2, 0).wait_recv()
    x_copy(False, 2, 1).wait_recv()
    loads[5].wait()
    kg_t = m["kg"][...].T
    half = inputs.shape[1] // 2
    n_i = 2 * n_x

    def wy_copy(part, r):
        to = (y + r) % N_Y
        return pltpu.make_async_remote_copy(
            src_ref=m["wy"].at[part, r],
            dst_ref=m["wyr"].at[part, r],
            send_sem=m["wy_send"].at[part, r],
            recv_sem=m["wy_recv"].at[part, r],
            device_id={"kv": z * PLANE + to * N_C + c},
            device_id_type=MESH,
        )

    def own_terms(i):
        rel, h = i // 2, i % 2
        w_t = lax.dot_general(
            kg_t, m["xraw"][rel, :, h * half : (h + 1) * half], (((1,), (0,)), ((), ())),
            preferred_element_type=F32,
        )
        w = w_t.T.astype(BF16)
        for yy in range(N_Y):
            for cc in range(N_C):
                first = (yy * N_C + cc) * BLOCK
                m["wpart"][i, cc, yy] = w[first : first + BLOCK]

    def core_sum(i):
        c_copy(i).wait_recv()
        for r in range(N_Y):
            yy = (y + r) % N_Y
            both = m["wpart"][i, c, yy].astype(F32) + m["crecv"][i, yy].astype(F32)
            if r:
                m["wy"][i // 2, r, i % 2] = both.astype(BF16)
            else:
                m["wy_own"][i] = both

    lag = 3
    for i in range(n_i + lag):
        if i < n_i:
            own_terms(i)
        if 0 < i <= n_i:
            c_copy(i - 1).start()
        if i >= lag:
            core_sum(i - lag)
            if (i - lag) % 2:
                for r in (2, 1, 3):
                    wy_copy((i - lag) // 2, r).start()

    def z_of(i):
        return 2 * ((x + n_x - i // 2) % n_x) + i % 2

    def wz_copy(i):
        return pltpu.make_async_remote_copy(
            src_ref=m["wz"].at[i],
            dst_ref=m["wzr"].at[z],
            send_sem=m["wz_send"].at[i],
            recv_sem=m["wz_recv"].at[z],
            device_id={"kv": z_of(i) * PLANE + q},
            device_id_type=MESH,
        )

    def sent(g, order, z_from, ref):
        wait_group(m["picked"].at[g, order, others], m["y_send"].at[g, order])

    for g in range(2):
        for part in range(PARTS):
            @pl.when(z < 3)
            def _():
                top_copy(g, part)[0].wait_send()

        for way in range(2):
            for step in range(1 + way, steps(way) + 1):
                @pl.when(sends(way, step))
                def _():
                    for part in range(PARTS):
                        z_copy(g, way, step, part).wait_send()

        sent(g, 0, z, None)
        for step in range(1, 5):
            each_piece(g, step, sent)
        for d in range(8):
            @pl.when(z - d >= 0)
            def _():
                wait_group(m["back"].at[g, d, others], m["b_send"].at[g, d])

            for part in range(2):
                if 0 < d < 5:
                    @pl.when(z - d >= 0)
                    def _():
                        dn_copy(g, d, part).wait_send()
                elif d:
                    e = n_z - d
                    @pl.when(z - d >= 0)
                    def _():
                        up_copy(g, e, part, last=True).wait_send()

    for part in range(2):
        x_copy(True, 1, part).wait_send()
        x_copy(False, 1, part).wait_send()
    x_copy(True, 2, 0).wait_send()
    x_copy(False, 2, 1).wait_send()
    for i in range(n_i):
        c_copy(i).wait_send()
    out_q.wait()

    for part in range(n_x):
        for r in (1, 3, 2):
            wy_copy(part, r).wait_recv()
        for i in (2 * part, 2 * part + 1):
            total = m["wy_own"][i]
            for r in range(1, N_Y):
                total = total + m["wyr"][part, r, i % 2].astype(F32)
            m["wz_own"][i] = total
            m["wz"][i] = total.astype(BF16)
        for i in (2 * part, 2 * part + 1):
            @pl.when(z_of(i) != z)
            def _():
                wz_copy(i).start()
    for part in range(n_x):
        for r in range(1, N_Y):
            wy_copy(part, r).wait_send()
    mine = 2 * ((x + n_x - z // 2) % n_x) + z % 2
    total = m["wz_own"][mine]
    for r in range(1, n_z):
        frm = (z + r) % n_z
        pltpu.make_async_remote_copy(
            src_ref=m["wz"].at[0],
            dst_ref=m["wzr"].at[frm],
            send_sem=m["wz_send"].at[0],
            recv_sem=m["wz_recv"].at[frm],
            device_id={"kv": frm * PLANE + q},
            device_id_type=MESH,
        ).wait_recv()
        total = total + m["wzr"][frm].astype(F32)
    weight_grad[...] = total
    for i in range(n_i):
        @pl.when(z_of(i) != z)
        def _():
            wz_copy(i).wait_send()


def put_kernel(q_src, k_src, v_src, w_src, q_dst, k_dst, v_dst, w_dst, q_mid, sem):
    rows = q_mid.shape[0] // 3
    part = [pl.ds(i * rows, rows) for i in range(3)]
    into = [
        pltpu.make_async_copy(q_src.at[part[i]], q_mid.at[part[i]], sem.at[i]) for i in range(3)
    ]
    rest = [
        pltpu.make_async_copy(src, dst, sem.at[3 + i])
        for i, (src, dst) in enumerate([(k_src, k_dst), (v_src, v_dst), (w_src, w_dst)])
    ]
    out = [
        pltpu.make_async_copy(q_mid.at[part[i]], q_dst.at[part[i]], sem.at[6 + i]) for i in range(3)
    ]
    for copy in into + rest:
        copy.start()
    for i in range(3):
        into[i].wait()
        out[i].start()
    for copy in rest + out:
        copy.wait()


def put_out(query_grad, key_grad, value_grad, weight_grad):
    hbm = pl.BlockSpec(memory_space=pltpu.HBM)
    vm = pl.BlockSpec(memory_space=pltpu.VMEM)
    arrays = (query_grad, key_grad, value_grad, weight_grad)
    return pl.pallas_call(
        put_kernel,
        out_shape=tuple(jax.ShapeDtypeStruct(a.shape, a.dtype) for a in arrays),
        in_specs=[hbm, vm, vm, vm],
        out_specs=(hbm,) * 4,
        scratch_shapes=[pltpu.VMEM(query_grad.shape, F32), pltpu.SemaphoreType.DMA((9,))],
        compiler_params=pltpu.CompilerParams(vmem_limit_bytes=int(53.4 * 1024 * 1024)),
        name="put_out",
    )(*arrays)


def index_table(chosen, n_b, n_dev):
    groups, _, n_list = chosen.shape
    me = lax.axis_index("kv")
    z, q = place()
    plane = lax.dynamic_slice_in_dim(chosen, z * PLANE * n_b, PLANE * n_b, 1)
    column = (jnp.arange(n_dev // PLANE) * PLANE + q) * n_b
    offs = plane[..., None] - column
    offs = jnp.where((offs >= 0) & (offs < n_b), offs, 0)
    picks = jnp.max(offs.reshape(groups, PLANE, n_b * n_list, -1), axis=2)
    picks = picks.transpose(2, 1, 0).reshape(-1)
    lists = lax.dynamic_slice_in_dim(chosen, me * n_b, n_b, 1)
    owner = lists // n_b
    slot = jnp.where(owner == me, n_dev + lists % n_b, jnp.maximum(owner, 0))
    at_diag = lists == me * n_b + jnp.arange(n_b)[None, :, None]
    kind = jnp.where(lists < 0, 2, at_diag.astype(jnp.int32))
    listed = (slot[..., None] == jnp.arange(n_dev + n_b)) & (lists >= 0)[..., None]
    inverse = jnp.min(
        jnp.where(listed, jnp.arange(n_list)[:, None], n_list), axis=2
    )
    slots = slot.transpose(1, 0, 2).reshape(-1)
    kinds = kind.transpose(1, 0, 2).reshape(-1)
    inverse = inverse.transpose(0, 2, 1).reshape(-1)
    return picks, slots, kinds, inverse


def local(queries, key_heads, values, log_sums, out_grad, inputs, chosen):
    n_dev = lax.axis_size("kv")
    n_x = lax.axis_size("tp")
    rows, feats = inputs.shape
    n_b = rows // BLOCK
    heads = log_sums.shape[0]
    n_list = chosen.shape[2]
    idx = index_table(chosen, n_b, n_dev)
    scratch = scratch_list(rows, n_dev, n_x, n_list, feats, heads)
    hbm = pl.BlockSpec(memory_space=pltpu.HBM)
    vm = pl.BlockSpec(memory_space=pltpu.VMEM)
    results = pl.pallas_call(
        functools.partial(
            fused_kernel, [name for name, _ in scratch], n_dev // PLANE, n_x, n_list
        ),
        out_shape=(
            jax.ShapeDtypeStruct(queries.shape, F32),
            jax.ShapeDtypeStruct(key_heads.shape, F32),
            jax.ShapeDtypeStruct(values.shape, F32),
            jax.ShapeDtypeStruct((feats * n_x // n_dev, 128), F32),
        ),
        in_specs=[pl.BlockSpec(memory_space=pltpu.SMEM)] * 4 + [hbm] * 6,
        out_specs=(hbm, vm, vm, vm),
        scratch_shapes=[kind for _, kind in scratch],
        compiler_params=pltpu.CompilerParams(
            collective_id=0, has_side_effects=True, vmem_limit_bytes=53 * 1024 * 1024
        ),
        name="fused",
    )(
        *idx,
        key_heads.reshape(n_b, BLOCK, -1),
        values.reshape(n_b, BLOCK, -1),
        queries,
        out_grad,
        log_sums,
        inputs,
    )
    return put_out(*results)


def solution(mesh):
    placed = (
        P("kv", "tp"),
        P("kv", "tp"),
        P("kv", "tp"),
        P("tp", "kv"),
        P("kv", "tp"),
        P("kv", "tp"),
        P("tp", None, None),
    )
    return jax.shard_map(
        local,
        mesh=mesh,
        in_specs=placed,
        out_specs=(P("kv", "tp"), P("kv", "tp"), P("kv", "tp"), P("kv", "tp")),
        check_vma=False,
    )
```

```python
import functools

import jax
import jax.numpy as jnp
from jax import lax
from jax.experimental import pallas as pl
from jax.experimental.pallas import tpu as pltpu
from jax.sharding import PartitionSpec as P

HD = 64
BLOCK = 64
NEG = -1e30
LOG2E = 1.4426950408889634
CHUNK = 4
PARTS = 3
N_Y = 4
N_C = 2
PLANE = N_Y * N_C
MESH = pl.DeviceIdType.MESH
RETURN_ORDER = (4, 3, 5, 6, 2, 1, 7, 0)
F32, BF16 = jnp.float32, jnp.bfloat16


def place():
    me = lax.axis_index("kv")
    return me // PLANE, me % PLANE


def scratch_list(rows, n_dev, n_x, n_list, feats, heads):
    n_b = rows // BLOCK
    tile = (BLOCK, 128)
    cols = heads // 2 * BLOCK
    dma = pltpu.SemaphoreType.DMA
    out = [
        ("kraw", pltpu.VMEM((n_b,) + tile, BF16)),
        ("vraw", pltpu.VMEM((n_b,) + tile, BF16)),
        ("qraw", pltpu.VMEM((rows, heads * HD), BF16)),
        ("graw", pltpu.VMEM((rows, heads * HD), BF16)),
        ("lraw", pltpu.VMEM((heads, rows), F32)),
        ("xraw", pltpu.VMEM((n_x, rows, feats), BF16)),
        ("lse", pltpu.VMEM((n_b * 2, 1, cols), F32)),
        ("bias", pltpu.VMEM((3,) + (BLOCK, cols), F32)),
        ("shift", pltpu.VMEM((3,) + (BLOCK, cols), F32)),
        ("qg", pltpu.VMEM((rows, heads * HD), F32)),
        ("picked", pltpu.VMEM((2, 8, PLANE) + tile, BF16)),
        ("qd", pltpu.VMEM((2 * cols, 128), BF16)),
        ("cat", pltpu.VMEM((n_list,) + tile, BF16)),
        ("sdp", pltpu.VMEM((n_list, BLOCK, 2 * cols), F32)),
        ("pd", pltpu.VMEM((n_list, BLOCK, 2 * cols), BF16)),
        ("terms", pltpu.VMEM((n_b, n_list + 1) + tile, F32)),
        ("ret", pltpu.VMEM((2, n_dev) + tile, BF16)),
        ("own_tot", pltpu.VMEM((2, n_b) + tile, F32)),
        ("back", pltpu.VMEM((2, 8, PLANE) + tile, BF16)),
        ("acc", pltpu.VMEM((2, n_b) + tile, F32)),
        ("zs", pltpu.VMEM((2, 8, 2, n_b, BLOCK // 2, 128), BF16)),
        ("zr_dn", pltpu.VMEM((2, 4, 2, n_b, BLOCK // 2, 128), BF16)),
        ("zr_up", pltpu.VMEM((2, 4, 2, n_b, BLOCK // 2, 128), BF16)),
        ("kg", pltpu.VMEM((rows, 128), BF16)),
        ("wpart", pltpu.VMEM((8, N_C, N_Y) + tile, BF16)),
        ("crecv", pltpu.VMEM((8, N_Y) + tile, BF16)),
        ("wy", pltpu.VMEM((4, N_Y, 2) + tile, BF16)),
        ("wy_own", pltpu.VMEM((8,) + tile, F32)),
        ("wyr", pltpu.VMEM((4, N_Y, 2) + tile, BF16)),
        ("wz", pltpu.VMEM((8,) + tile, BF16)),
        ("wz_own", pltpu.VMEM((8,) + tile, F32)),
        ("wzr", pltpu.VMEM((8,) + tile, BF16)),
        ("in_sem", dma((6,))),
        ("out_sem", dma((1,))),
        ("z_send", dma((2, 2, 5, PARTS))),
        ("z_recv", dma((2, 2, 5, PARTS))),
        ("y_send", dma((2, 8))),
        ("y_recv", dma((2, 8))),
        ("x_send", dma((2, 3, 2))),
        ("x_recv", dma((2, 3, 2))),
        ("b_send", dma((2, 8))),
        ("b_recv", dma((2, 8))),
        ("r_send", dma((2, 8, 2))),
        ("r_recv_dn", dma((2, 4, 2))),
        ("r_recv_up", dma((2, 4, 2))),
        ("c_send", dma((8,))),
        ("c_recv", dma((8,))),
        ("wy_send", dma((4, N_Y))),
        ("wy_recv", dma((4, N_Y))),
        ("wz_send", dma((8,))),
        ("wz_recv", dma((8,))),
    ]
    for g in range(2):
        out.append((f"own{g}", pltpu.VMEM((n_b,) + tile, BF16)))
        out.append((f"tab{g}", pltpu.VMEM((n_dev + n_b,) + tile, BF16)))
        for step in range(1, 5):
            out.append((f"held{g}0{step}", pltpu.VMEM((n_b,) + tile, BF16)))
        for step in range(1, 4):
            out.append((f"held{g}1{step}", pltpu.VMEM((n_b,) + tile, BF16)))
    return out


def fused_kernel(names, n_z, n_x, n_list, *refs):
    idx_picks, idx_slots, idx_kinds, idx_inv = refs[:4]
    keys, vals, queries, out_grad, log_sums, inputs = refs[4:10]
    query_grad, key_grad, value_grad, weight_grad = refs[10:14]
    m = dict(zip(names, refs[14:]))
    n_b = m["kraw"].shape[0]
    n_dev = n_z * PLANE
    heads = m["lraw"].shape[0]
    per_group = heads // 2
    cols = per_group * BLOCK
    z, q = place()
    y, c = q // N_C, q % N_C
    x = lax.axis_index("tp")

    barrier = pltpu.get_barrier_semaphore()
    partners = [{"kv": (z + r) % n_z * PLANE + q} for r in range(1, n_z)]
    partners += [{"kv": z * PLANE + (q + r) % PLANE} for r in range(1, PLANE)]
    right, left = {"tp": (x + 1) % n_x}, {"tp": (x + n_x - 1) % n_x}
    partners += [right, left]
    for who in partners:
        pl.semaphore_signal(barrier, inc=1, device_id=who, device_id_type=MESH)

    loads = [
        pltpu.make_async_copy(src, dst, m["in_sem"].at[i])
        for i, (src, dst) in enumerate(
            [
                (keys, m["kraw"]),
                (vals, m["vraw"]),
                (queries, m["qraw"]),
                (out_grad, m["graw"]),
                (log_sums, m["lraw"]),
                (inputs, m["xraw"].at[0]),
            ]
        )
    ]
    for copy in loads:
        copy.start()
    up_z = {"kv": (z + 1) % n_z * PLANE + q}
    dn_z = {"kv": (z + n_z - 1) % n_z * PLANE + q}
    lane = lax.broadcasted_iota(jnp.int32, (BLOCK, 128), 1)
    low = lane < HD
    loads[0].wait()
    loads[1].wait()
    for b in range(n_b):
        k = m["kraw"][b].astype(F32)
        v = m["vraw"][b].astype(F32)
        kv0 = jnp.where(low, k, pltpu.roll(v, HD, 1)).astype(BF16)
        kv1 = jnp.where(low, pltpu.roll(k, HD, 1), v).astype(BF16)
        m["own0"][b] = kv0
        m["own1"][b] = kv1
        m["tab0"][n_dev + b] = kv0
        m["tab1"][n_dev + b] = kv1
    pl.semaphore_wait(barrier, len(partners))

    def held(g, way, step):
        return m[f"own{g}"] if step == 0 else m[f"held{g}{way}{step}"]

    def z_copy(g, way, step, part):
        blocks = pl.ds(part * (n_b // PARTS), n_b // PARTS)
        return pltpu.make_async_remote_copy(
            src_ref=held(g, way, step - 1).at[blocks],
            dst_ref=held(g, way, step).at[blocks],
            send_sem=m["z_send"].at[g, way, step, part],
            recv_sem=m["z_recv"].at[g, way, step, part],
            device_id=dn_z if way else up_z,
            device_id_type=MESH,
        )

    def sends(way, step):
        if way:
            return (z + step - 1) % n_z < 3
        return (z < n_z - 1) & (z - step + 1 >= 0)

    def gets(way, step):
        if way:
            return (z + step) % n_z < 3
        return z - step >= 0

    def steps(way):
        return 3 if way else 4

    def x_copy(to_right, rel, part):
        half = inputs.shape[0] // 2
        rows = pl.ds(part * half, half)
        slot = rel if to_right else n_x - rel
        if rel == 1:
            src = inputs.at[rows]
        else:
            src = m["xraw"].at[1 if to_right else n_x - 1, rows]
        side = 0 if to_right else 1
        return pltpu.make_async_remote_copy(
            src_ref=src,
            dst_ref=m["xraw"].at[slot, rows],
            send_sem=m["x_send"].at[side, rel, part],
            recv_sem=m["x_recv"].at[side, rel, part],
            device_id=right if to_right else left,
            device_id_type=MESH,
        )

    def y_copy(g, order, z_from, r):
        to = (q + r) % PLANE
        return pltpu.make_async_remote_copy(
            src_ref=m["picked"].at[g, order, r],
            dst_ref=m[f"tab{g}"].at[z_from * PLANE + q],
            send_sem=m["y_send"].at[g, order],
            recv_sem=m["y_recv"].at[g, order],
            device_id={"kv": z * PLANE + to},
            device_id_type=MESH,
        )

    others = pl.ds(1, PLANE - 1)

    def wait_group(ref, sem):
        pltpu.make_async_copy(ref, ref, sem).wait()

    def pick(g, order, z_from, ref):
        def one(r, carry):
            to = (q + r) % PLANE
            m["picked"][g, order, r] = ref[idx_picks[(z_from * PLANE + to) * 2 + g]]

            @pl.when(r > 1)
            def _():
                y_copy(g, order, z_from, r - 1).start()

            return carry

        lax.fori_loop(1, PLANE, one, 0)
        m[f"tab{g}"][z_from * PLANE + q] = ref[idx_picks[(z_from * PLANE + q) * 2 + g]]
        y_copy(g, order, z_from, PLANE - 1).start()

    def each_piece(g, step, act):
        @pl.when(gets(0, step))
        def _():
            act(g, step, z - step, held(g, 0, step))

        if step < 4:
            @pl.when(gets(1, step) & (z + step >= n_z))
            def _():
                act(g, 4 + step, z + step - n_z, held(g, 1, step))

    def set_out(g):
        for part in range(PARTS):
            for way in range(2):
                @pl.when(sends(way, 1))
                def _():
                    z_copy(g, way, 1, part).start()

    set_out(0)
    for part in range(2):
        x_copy(True, 1, part).start()
        x_copy(False, 1, 1 - part).start()
    pick(0, 0, z, m["own0"])
    pick(1, 0, z, m["own1"])

    def relay(g, step):
        for part in range(PARTS):
            for way in range(2):
                if step <= steps(way):
                    @pl.when(gets(way, step))
                    def _():
                        z_copy(g, way, step, part).wait_recv()

                if step + 1 <= steps(way):
                    @pl.when(sends(way, step + 1))
                    def _():
                        z_copy(g, way, step + 1, part).start()

    key_at = lax.broadcasted_iota(jnp.int32, (BLOCK, cols), 0)
    tok_at = lax.broadcasted_iota(jnp.int32, (BLOCK, cols), 1) % BLOCK
    m["bias"][0] = jnp.zeros((BLOCK, cols), F32)
    m["bias"][1] = jnp.where(key_at <= tok_at, 0.0, NEG)
    m["bias"][2] = jnp.full((BLOCK, cols), NEG, F32)
    for p in range(n_b):
        m["terms"][p, n_list] = jnp.zeros((BLOCK, 128), F32)
    loads[4].wait()
    for p in range(n_b):
        for g in range(2):
            row = [
                m["lraw"][g * per_group + r : g * per_group + r + 1, p * BLOCK : (p + 1) * BLOCK]
                for r in range(per_group)
            ]
            m["lse"][p * 2 + g] = jnp.concatenate(row, axis=1)

    for step in range(1, 5):
        relay(0, step)
        if step == 2:
            set_out(1)
        each_piece(0, step, pick)

    def relay_and_pick(g, step):
        relay(g, step)
        each_piece(g, step, pick)

    def relay_x():
        x_copy(True, 1, 0).wait_recv()
        x_copy(True, 2, 0).start()
        x_copy(False, 1, 1).wait_recv()
        x_copy(False, 2, 1).start()

    def landed(g, order, z_from, ref):
        wait_group(m["picked"].at[g, order, others], m["y_recv"].at[g, order])

    def masked_rows(ref, row, g, factor, side):
        parts = []
        for r in range(per_group):
            col = (g * per_group + r) * HD
            part = ref[pl.ds(row, BLOCK), col // 128 * 128 : col // 128 * 128 + 128]
            part = part.astype(F32) * factor
            if r % 2 != side:
                part = pltpu.roll(part, HD, 1)
            parts.append(jnp.where(low != (side == 1), part, 0.0).astype(BF16))
        return parts

    def attention(g, between):
        tab = m[f"tab{g}"]
        sdp, pd, qd, cat, shift = m["sdp"], m["pd"], m["qd"], m["cat"], m["shift"]
        chunks = [slice(n, n + CHUNK) for n in range(0, n_list, CHUNK)]
        nt = (((1,), (1,)), ((), ()))
        nn = (((1,), (0,)), ((), ()))

        def one_position(p, carry):
            row = pl.multiple_of(p * BLOCK, BLOCK)
            unit = (p * 2 + g) * n_list
            for r, part in enumerate(masked_rows(m["qraw"], row, g, HD ** -0.5, 0)):
                qd[r * BLOCK : (r + 1) * BLOCK, :] = part
            for r, part in enumerate(masked_rows(m["graw"], row, g, 1.0, 1)):
                qd[cols + r * BLOCK : cols + (r + 1) * BLOCK, :] = part
            for n in range(n_list):
                cat[n] = tab[idx_slots[unit + n]]
            for kind in range(3):
                shift[kind] = m["bias"][kind] - m["lse"][p * 2 + g] * LOG2E

            acc = jnp.zeros((8, cols), F32)
            for ch in chunks:
                both = lax.dot_general(
                    cat[ch].reshape(CHUNK * BLOCK, 128), qd[...], nt, preferred_element_type=F32
                ).reshape(CHUNK, BLOCK, 2 * cols)
                for n in range(ch.start, ch.stop):
                    prod = both[n - ch.start]
                    pr = jnp.exp2(prod[:, :cols] * LOG2E + shift[idx_kinds[unit + n]])
                    sdp[n, :, :cols] = pr
                    sdp[n, :, cols:] = prod[:, cols:]
                    pd[n, :, cols:] = pr.astype(BF16)
                    pr = pr * prod[:, cols:]
                    acc = acc + pr.reshape(BLOCK // 8, 8, cols).sum(axis=0)
            delta = acc.sum(axis=0, keepdims=True)
            for ch in chunks:
                for n in range(ch.start, ch.stop):
                    ds = sdp[n, :, :cols] * (sdp[n, :, cols:] - delta)
                    pd[n, :, :cols] = ds.astype(BF16)
                m["terms"][p, ch] = lax.dot_general(
                    pd[ch].reshape(CHUNK * BLOCK, 2 * cols), qd[...], nn, preferred_element_type=F32
                ).reshape(CHUNK, BLOCK, 128)
            dq_t = lax.dot_general(
                cat[...].reshape(n_list * BLOCK, 128),
                pd[:, :, :cols].reshape(n_list * BLOCK, cols),
                (((0,), (0,)), ((), ())),
                preferred_element_type=F32,
            )
            dq = dq_t.T * (HD ** -0.5)
            for pair in range(per_group // 2):
                even = dq[(2 * pair) * BLOCK : (2 * pair + 1) * BLOCK]
                odd = dq[(2 * pair + 1) * BLOCK : (2 * pair + 2) * BLOCK]
                col = g * per_group * HD + pair * 128
                m["qg"][pl.ds(row, BLOCK), col : col + 128] = jnp.where(
                    low, even, pltpu.roll(odd, HD, 1)
                )
            for at, act in between.items():
                @pl.when(p == at)
                def _():
                    act()

            return carry

        lax.fori_loop(0, n_b, one_position, 0)

    def summed_terms(g, j):
        at = (g * (n_dev + n_b) + j) * n_b
        total = m["terms"][0, idx_inv[at]]
        for p in range(1, n_b):
            total = total + m["terms"][p, idx_inv[at + p]]
        return total

    def b_copy(g, d, r):
        to = (q + r) % PLANE
        return pltpu.make_async_remote_copy(
            src_ref=m["ret"].at[g, (z - d) * PLANE + to],
            dst_ref=m["back"].at[g, d, q],
            send_sem=m["b_send"].at[g, d],
            recv_sem=m["b_recv"].at[g, d],
            device_id={"kv": z * PLANE + to},
            device_id_type=MESH,
        )

    def give_back(g):
        for d in RETURN_ORDER:
            @pl.when(z - d >= 0)
            def _():
                for r in list(range(1, PLANE)) + [0]:
                    j = (z - d) * PLANE + (q + r) % PLANE
                    m["ret"][g, j] = summed_terms(g, j).astype(BF16)
                for r in range(1, PLANE):
                    b_copy(g, d, r).start()

        def own(b, carry):
            m["own_tot"][g, b] = summed_terms(g, n_dev + b)
            return carry

        lax.fori_loop(0, n_b, own, 0)

    def accumulate(g, d, part):
        rows = slice(part * 32, part * 32 + 32)
        accs = [jnp.zeros((32, 128), F32) for _ in range(n_b)]
        for r in range(PLANE):
            frm = (q + r) % PLANE
            if r == 0:
                val = m["ret"][g, (z - d) * PLANE + q, rows, :]
            else:
                val = m["back"][g, d, frm, rows, :]
            val = val.astype(F32)
            block = idx_picks[((z - d) * PLANE + frm) * 2 + g]
            for b in range(n_b):
                accs[b] = accs[b] + jnp.where(block == b, val, 0.0)
        for b in range(n_b):
            m["acc"][g, b, rows, :] = accs[b]

    def dn_copy(g, d, part):
        return pltpu.make_async_remote_copy(
            src_ref=m["zs"].at[g, d, part],
            dst_ref=m["zr_dn"].at[g, d - 1, part],
            send_sem=m["r_send"].at[g, d, part],
            recv_sem=m["r_recv_dn"].at[g, d - 1, part],
            device_id={"kv": (z + n_z - (2 - d % 2)) % n_z * PLANE + q},
            device_id_type=MESH,
        )

    def up_copy(g, d, at, part):
        to = n_z - 1 if at else n_z - 1 - d
        return pltpu.make_async_remote_copy(
            src_ref=m["zs"].at[g, d, part],
            dst_ref=m["zr_up"].at[g, at, part],
            send_sem=m["r_send"].at[g, d, part],
            recv_sem=m["r_recv_up"].at[g, at, part],
            device_id={"kv": to * PLANE + q},
            device_id_type=MESH,
        )

    def add_arrival(g, copy, ref, part):
        copy.wait_recv()
        rows = slice(part * 32, part * 32 + 32)
        for b in range(n_b):
            m["acc"][g, b, rows, :] += ref[b].astype(F32)

    def dn_arrival(g, d, part):
        @pl.when(z < n_z - (2 - d % 2))
        def _():
            add_arrival(g, dn_copy(g, d, part), m["zr_dn"].at[g, d - 1, part], part)

    def up_arrival(g, at, part):
        add_arrival(g, up_copy(g, 5, at, part), m["zr_up"].at[g, at, part], part)

    def store_out(g, d, part):
        rows = slice(part * 32, part * 32 + 32)
        for b in range(n_b):
            m["zs"][g, d, part, b] = m["acc"][g, b, rows, :].astype(BF16)

    def collect(g, d):
        @pl.when(z - d >= 0)
        def _():
            wait_group(m["back"].at[g, d, others], m["b_recv"].at[g, d])
            for part in range(2):
                accumulate(g, d, part)
                if d in (0, 2):
                    dn_arrival(g, d + 1, part)
                    dn_arrival(g, d + 2, part)
                if d in (6, 7):
                    @pl.when(z == n_z - 1)
                    def _():
                        for at in {6: (2,), 7: (1, 3)}[d]:
                            up_arrival(g, at, part)

                if d == 0:
                    @pl.when(z < 3)
                    def _():
                        up_arrival(g, 0, part)
                    continue
                store_out(g, d, part)
                if d < 5:
                    dn_copy(g, d, part).start()
                else:
                    @pl.when(z == n_z - 1)
                    def _():
                        up_copy(g, d, 0, part).start()

                    for plane, at in {5: ((5, 1), (6, 2)), 6: ((6, 3),), 7: ()}[d]:
                        @pl.when(z == plane)
                        def _():
                            up_copy(g, d, at, part).start()

    def wait_fetch(g):
        landed(g, 0, z, None)
        for step in range(1, 5):
            each_piece(g, step, landed)

    relay_and_pick(1, 1)
    relay_and_pick(1, 2)
    loads[2].wait()
    loads[3].wait()
    wait_fetch(0)
    attention(
        0,
        {
            0: functools.partial(relay_and_pick, 1, 3),
            2: functools.partial(relay_and_pick, 1, 4),
            4: relay_x,
        },
    )
    give_back(0)
    wait_fetch(1)
    attention(1, {2 + i: functools.partial(collect, 0, RETURN_ORDER[i]) for i in range(4)})
    give_back(1)
    out_q = pltpu.make_async_copy(m["qg"], query_grad, m["out_sem"].at[0])
    out_q.start()
    for g, d in [
        (0, 2), (1, 4), (0, 1), (1, 3), (0, 7), (1, 5), (1, 6), (1, 2), (1, 1), (1, 7), (1, 0), (0, 0)
    ]:
        collect(g, d)

    for b in range(n_b):
        rows = slice(b * BLOCK, (b + 1) * BLOCK)
        t0 = m["acc"][0, b] + m["own_tot"][0, b]
        t1 = m["acc"][1, b] + m["own_tot"][1, b]
        kg = jnp.where(low, t0, pltpu.roll(t1, HD, 1))
        key_grad[rows, :] = kg
        value_grad[rows, :] = jnp.where(low, pltpu.roll(t0, HD, 1), t1)
        m["kg"][rows, :] = kg.astype(BF16)

    def c_copy(i):
        return pltpu.make_async_remote_copy(
            src_ref=m["wpart"].at[i, 1 - c],
            dst_ref=m["crecv"].at[i],
            send_sem=m["c_send"].at[i],
            recv_sem=m["c_recv"].at[i],
            device_id={"kv": z * PLANE + y * N_C + (1 - c)},
            device_id_type=MESH,
        )

    x_copy(True, 1, 1).wait_recv()
    x_copy(False, 1, 0).wait_recv()
    x_copy(True, 2, 0).wait_recv()
    x_copy(False, 2, 1).wait_recv()
    loads[5].wait()
    kg_t = m["kg"][...].T
    half = inputs.shape[1] // 2
    n_i = 2 * n_x

    def wy_copy(part, r):
        to = (y + r) % N_Y
        return pltpu.make_async_remote_copy(
            src_ref=m["wy"].at[part, r],
            dst_ref=m["wyr"].at[part, r],
            send_sem=m["wy_send"].at[part, r],
            recv_sem=m["wy_recv"].at[part, r],
            device_id={"kv": z * PLANE + to * N_C + c},
            device_id_type=MESH,
        )

    def own_terms(i):
        rel, h = i // 2, i % 2
        w_t = lax.dot_general(
            kg_t, m["xraw"][rel, :, h * half : (h + 1) * half], (((1,), (0,)), ((), ())),
            preferred_element_type=F32,
        )
        w = w_t.T.astype(BF16)
        for yy in range(N_Y):
            for cc in range(N_C):
                first = (yy * N_C + cc) * BLOCK
                m["wpart"][i, cc, yy] = w[first : first + BLOCK]

    def core_sum(i):
        c_copy(i).wait_recv()
        for r in range(N_Y):
            yy = (y + r) % N_Y
            both = m["wpart"][i, c, yy].astype(F32) + m["crecv"][i, yy].astype(F32)
            if r:
                m["wy"][i // 2, r, i % 2] = both.astype(BF16)
            else:
                m["wy_own"][i] = both

    lag = 3
    for i in range(n_i + lag):
        if i < n_i:
            own_terms(i)
        if 0 < i <= n_i:
            c_copy(i - 1).start()
        if i >= lag:
            core_sum(i - lag)
            if (i - lag) % 2:
                for r in (2, 1, 3):
                    wy_copy((i - lag) // 2, r).start()

    def z_of(i):
        return 2 * ((x + n_x - i // 2) % n_x) + i % 2

    def wz_copy(i):
        return pltpu.make_async_remote_copy(
            src_ref=m["wz"].at[i],
            dst_ref=m["wzr"].at[z],
            send_sem=m["wz_send"].at[i],
            recv_sem=m["wz_recv"].at[z],
            device_id={"kv": z_of(i) * PLANE + q},
            device_id_type=MESH,
        )

    def sent(g, order, z_from, ref):
        wait_group(m["picked"].at[g, order, others], m["y_send"].at[g, order])

    for g in range(2):
        for way in range(2):
            for step in range(1, steps(way) + 1):
                @pl.when(sends(way, step))
                def _():
                    for part in range(PARTS):
                        z_copy(g, way, step, part).wait_send()

        sent(g, 0, z, None)
        for step in range(1, 5):
            each_piece(g, step, sent)
        for d in range(8):
            @pl.when(z - d >= 0)
            def _():
                wait_group(m["back"].at[g, d, others], m["b_send"].at[g, d])

            for part in range(2):
                if 0 < d < 5:
                    @pl.when(z - d >= 0)
                    def _():
                        dn_copy(g, d, part).wait_send()
                elif d:
                    @pl.when(z - d >= 0)
                    def _():
                        up_copy(g, d, 0, part).wait_send()

    for part in range(2):
        x_copy(True, 1, part).wait_send()
        x_copy(False, 1, part).wait_send()
    x_copy(True, 2, 0).wait_send()
    x_copy(False, 2, 1).wait_send()
    for i in range(n_i):
        c_copy(i).wait_send()
    out_q.wait()

    for part in range(n_x):
        for r in (1, 3, 2):
            wy_copy(part, r).wait_recv()
        for i in (2 * part, 2 * part + 1):
            total = m["wy_own"][i]
            for r in range(1, N_Y):
                total = total + m["wyr"][part, r, i % 2].astype(F32)
            m["wz_own"][i] = total
            m["wz"][i] = total.astype(BF16)
        for i in (2 * part, 2 * part + 1):
            @pl.when(z_of(i) != z)
            def _():
                wz_copy(i).start()
    for part in range(n_x):
        for r in range(1, N_Y):
            wy_copy(part, r).wait_send()
    mine = 2 * ((x + n_x - z // 2) % n_x) + z % 2
    total = m["wz_own"][mine]
    for r in range(1, n_z):
        frm = (z + r) % n_z
        pltpu.make_async_remote_copy(
            src_ref=m["wz"].at[0],
            dst_ref=m["wzr"].at[frm],
            send_sem=m["wz_send"].at[0],
            recv_sem=m["wz_recv"].at[frm],
            device_id={"kv": frm * PLANE + q},
            device_id_type=MESH,
        ).wait_recv()
        total = total + m["wzr"][frm].astype(F32)
    weight_grad[...] = total
    for i in range(n_i):
        @pl.when(z_of(i) != z)
        def _():
            wz_copy(i).wait_send()


def put_kernel(q_src, k_src, v_src, w_src, q_dst, k_dst, v_dst, w_dst, q_mid, sem):
    rows = q_mid.shape[0] // 3
    part = [pl.ds(i * rows, rows) for i in range(3)]
    into = [
        pltpu.make_async_copy(q_src.at[part[i]], q_mid.at[part[i]], sem.at[i]) for i in range(3)
    ]
    rest = [
        pltpu.make_async_copy(src, dst, sem.at[3 + i])
        for i, (src, dst) in enumerate([(k_src, k_dst), (v_src, v_dst), (w_src, w_dst)])
    ]
    out = [
        pltpu.make_async_copy(q_mid.at[part[i]], q_dst.at[part[i]], sem.at[6 + i]) for i in range(3)
    ]
    for copy in into + rest:
        copy.start()
    for i in range(3):
        into[i].wait()
        out[i].start()
    for copy in rest + out:
        copy.wait()


def put_out(query_grad, key_grad, value_grad, weight_grad):
    hbm = pl.BlockSpec(memory_space=pltpu.HBM)
    vm = pl.BlockSpec(memory_space=pltpu.VMEM)
    arrays = (query_grad, key_grad, value_grad, weight_grad)
    return pl.pallas_call(
        put_kernel,
        out_shape=tuple(jax.ShapeDtypeStruct(a.shape, a.dtype) for a in arrays),
        in_specs=[hbm, vm, vm, vm],
        out_specs=(hbm,) * 4,
        scratch_shapes=[pltpu.VMEM(query_grad.shape, F32), pltpu.SemaphoreType.DMA((9,))],
        compiler_params=pltpu.CompilerParams(vmem_limit_bytes=int(53.4 * 1024 * 1024)),
        name="put_out",
    )(*arrays)


def index_table(chosen, n_b, n_dev):
    groups, _, n_list = chosen.shape
    me = lax.axis_index("kv")
    z, q = place()
    plane = lax.dynamic_slice_in_dim(chosen, z * PLANE * n_b, PLANE * n_b, 1)
    column = (jnp.arange(n_dev // PLANE) * PLANE + q) * n_b
    offs = plane[..., None] - column
    offs = jnp.where((offs >= 0) & (offs < n_b), offs, 0)
    picks = jnp.max(offs.reshape(groups, PLANE, n_b * n_list, -1), axis=2)
    picks = picks.transpose(2, 1, 0).reshape(-1)
    lists = lax.dynamic_slice_in_dim(chosen, me * n_b, n_b, 1)
    owner = lists // n_b
    slot = jnp.where(owner == me, n_dev + lists % n_b, jnp.maximum(owner, 0))
    at_diag = lists == me * n_b + jnp.arange(n_b)[None, :, None]
    kind = jnp.where(lists < 0, 2, at_diag.astype(jnp.int32))
    listed = (slot[..., None] == jnp.arange(n_dev + n_b)) & (lists >= 0)[..., None]
    inverse = jnp.min(
        jnp.where(listed, jnp.arange(n_list)[:, None], n_list), axis=2
    )
    slots = slot.transpose(1, 0, 2).reshape(-1)
    kinds = kind.transpose(1, 0, 2).reshape(-1)
    inverse = inverse.transpose(0, 2, 1).reshape(-1)
    return picks, slots, kinds, inverse


def local(queries, key_heads, values, log_sums, out_grad, inputs, chosen):
    n_dev = lax.axis_size("kv")
    n_x = lax.axis_size("tp")
    rows, feats = inputs.shape
    n_b = rows // BLOCK
    heads = log_sums.shape[0]
    n_list = chosen.shape[2]
    idx = index_table(chosen, n_b, n_dev)
    scratch = scratch_list(rows, n_dev, n_x, n_list, feats, heads)
    hbm = pl.BlockSpec(memory_space=pltpu.HBM)
    vm = pl.BlockSpec(memory_space=pltpu.VMEM)
    results = pl.pallas_call(
        functools.partial(
            fused_kernel, [name for name, _ in scratch], n_dev // PLANE, n_x, n_list
        ),
        out_shape=(
            jax.ShapeDtypeStruct(queries.shape, F32),
            jax.ShapeDtypeStruct(key_heads.shape, F32),
            jax.ShapeDtypeStruct(values.shape, F32),
            jax.ShapeDtypeStruct((feats * n_x // n_dev, 128), F32),
        ),
        in_specs=[pl.BlockSpec(memory_space=pltpu.SMEM)] * 4 + [hbm] * 6,
        out_specs=(hbm, vm, vm, vm),
        scratch_shapes=[kind for _, kind in scratch],
        compiler_params=pltpu.CompilerParams(
            collective_id=0, has_side_effects=True, vmem_limit_bytes=53 * 1024 * 1024
        ),
        name="fused",
    )(
        *idx,
        key_heads.reshape(n_b, BLOCK, -1),
        values.reshape(n_b, BLOCK, -1),
        queries,
        out_grad,
        log_sums,
        inputs,
    )
    return put_out(*results)


def solution(mesh):
    placed = (
        P("kv", "tp"),
        P("kv", "tp"),
        P("kv", "tp"),
        P("tp", "kv"),
        P("kv", "tp"),
        P("kv", "tp"),
        P("tp", None, None),
    )
    return jax.shard_map(
        local,
        mesh=mesh,
        in_specs=placed,
        out_specs=(P("kv", "tp"), P("kv", "tp"), P("kv", "tp"), P("kv", "tp")),
        check_vma=False,
    )
```

```python
import functools

import jax
import jax.numpy as jnp
from jax import lax
from jax.experimental import pallas as pl
from jax.experimental.pallas import tpu as pltpu
from jax.sharding import PartitionSpec as P

HD = 64
BLOCK = 64
NEG = -1e30
LOG2E = 1.4426950408889634
CHUNK = 4
PARTS = 3
ROW_PARTS = 4
PART_ROWS = BLOCK // ROW_PARTS
N_Y = 4
N_C = 2
PLANE = N_Y * N_C
MESH = pl.DeviceIdType.MESH
RETURN_ORDER = (4, 5, 3, 6, 2, 7, 1, 0)
F32, BF16 = jnp.float32, jnp.bfloat16


def place():
    me = lax.axis_index("kv")
    return me // PLANE, me % PLANE


def scratch_list(rows, n_dev, n_x, n_list, feats, heads):
    n_b = rows // BLOCK
    tile = (BLOCK, 128)
    cols = heads // 2 * BLOCK
    dma = pltpu.SemaphoreType.DMA
    out = [
        ("kraw", pltpu.VMEM((n_b,) + tile, BF16)),
        ("vraw", pltpu.VMEM((n_b,) + tile, BF16)),
        ("qraw", pltpu.VMEM((rows, heads * HD), BF16)),
        ("graw", pltpu.VMEM((rows, heads * HD), BF16)),
        ("lraw", pltpu.VMEM((heads, rows), F32)),
        ("xraw", pltpu.VMEM((n_x, rows, feats), BF16)),
        ("lse", pltpu.VMEM((n_b * 2, 1, cols), F32)),
        ("bias", pltpu.VMEM((3,) + (BLOCK, cols), F32)),
        ("shift", pltpu.VMEM((3,) + (BLOCK, cols), F32)),
        ("qg", pltpu.VMEM((rows, heads * HD), F32)),
        ("picked", pltpu.VMEM((2, 8, PLANE) + tile, BF16)),
        ("qd", pltpu.VMEM((2 * cols, 128), BF16)),
        ("cat", pltpu.VMEM((n_list,) + tile, BF16)),
        ("sdp", pltpu.VMEM((n_list, BLOCK, 2 * cols), F32)),
        ("pd", pltpu.VMEM((n_list, BLOCK, 2 * cols), BF16)),
        ("terms", pltpu.VMEM((n_b, n_list + 1) + tile, F32)),
        ("ret", pltpu.VMEM((2, n_dev) + tile, BF16)),
        ("own_tot", pltpu.VMEM((2, n_b) + tile, F32)),
        ("back", pltpu.VMEM((2, 8, PLANE) + tile, BF16)),
        ("acc", pltpu.VMEM((2, n_b) + tile, F32)),
        ("zs", pltpu.VMEM((2, 8, ROW_PARTS, n_b, PART_ROWS, 128), BF16)),
        ("zr_dn", pltpu.VMEM((2, 4, ROW_PARTS, n_b, PART_ROWS, 128), BF16)),
        ("zr_up", pltpu.VMEM((2, 4, ROW_PARTS, n_b, PART_ROWS, 128), BF16)),
        ("kg", pltpu.VMEM((rows, 128), BF16)),
        ("kg_t", pltpu.VMEM((128, rows), BF16)),
        ("wpart", pltpu.VMEM((2, n_x, N_C, N_Y) + tile, BF16)),
        ("crecv", pltpu.VMEM((2, n_x, N_Y) + tile, BF16)),
        ("wy", pltpu.VMEM((2, 2, N_Y, n_x // 2) + tile, BF16)),
        ("wy_own", pltpu.VMEM((2, n_x) + tile, F32)),
        ("wyr", pltpu.VMEM((2, 2, N_Y, n_x // 2) + tile, BF16)),
        ("wz", pltpu.VMEM((8,) + tile, BF16)),
        ("wz_own", pltpu.VMEM((8,) + tile, F32)),
        ("wzr", pltpu.VMEM((8,) + tile, BF16)),
        ("in_sem", dma((6,))),
        ("out_sem", dma((1,))),
        ("sent", dma((8,))),
        ("z_recv", dma((2, 7, PARTS))),
        ("y_recv", dma((2, 8))),
        ("x_recv", dma((2, 3))),
        ("b_recv", dma((2, 8))),
        ("r_recv_dn", dma((2, 4, ROW_PARTS))),
        ("r_recv_up", dma((2, 4, ROW_PARTS))),
        ("c_recv", dma((2, n_x))),
        ("wy_recv", dma((2, 2, N_Y - 1))),
        ("wz_recv", dma((8,))),
    ]
    for g in range(2):
        out.append((f"own{g}", pltpu.VMEM((n_b,) + tile, BF16)))
        out.append((f"tab{g}", pltpu.VMEM((n_dev + n_b,) + tile, BF16)))
        for step in range(1, 5):
            out.append((f"held{g}0{step}", pltpu.VMEM((n_b,) + tile, BF16)))
        for step in range(1, 4):
            out.append((f"held{g}1{step}", pltpu.VMEM((n_b,) + tile, BF16)))
    return out


def fused_kernel(names, n_z, n_x, n_list, *refs):
    idx_picks, idx_slots, idx_kinds, idx_inv = refs[:4]
    keys, vals, queries, out_grad, log_sums, inputs = refs[4:10]
    query_grad, key_grad, value_grad, weight_grad = refs[10:14]
    m = dict(zip(names, refs[14:]))
    n_b = m["kraw"].shape[0]
    n_dev = n_z * PLANE
    heads = m["lraw"].shape[0]
    per_group = heads // 2
    cols = per_group * BLOCK
    z, q = place()
    y, c = q // N_C, q % N_C
    x = lax.axis_index("tp")

    barrier = pltpu.get_barrier_semaphore()
    partners = [{"kv": (z + r) % n_z * PLANE + q} for r in range(1, n_z)]
    partners += [{"kv": z * PLANE + (q + r) % PLANE} for r in range(1, PLANE)]
    right, left = {"tp": (x + 1) % n_x}, {"tp": (x + n_x - 1) % n_x}
    partners += [right, left]
    for who in partners:
        pl.semaphore_signal(barrier, inc=1, device_id=who, device_id_type=MESH)

    loads = [
        pltpu.make_async_copy(src, dst, m["in_sem"].at[i])
        for i, (src, dst) in enumerate(
            [
                (keys, m["kraw"]),
                (vals, m["vraw"]),
                (queries, m["qraw"]),
                (out_grad, m["graw"]),
                (log_sums, m["lraw"]),
                (inputs, m["xraw"].at[0]),
            ]
        )
    ]
    for copy in loads:
        copy.start()
    up_z = {"kv": (z + 1) % n_z * PLANE + q}
    dn_z = {"kv": (z + n_z - 1) % n_z * PLANE + q}
    lane = lax.broadcasted_iota(jnp.int32, (BLOCK, 128), 1)
    low = lane < HD
    loads[0].wait()
    loads[1].wait()
    for b in range(n_b):
        k = m["kraw"][b].astype(F32)
        v = m["vraw"][b].astype(F32)
        kv0 = jnp.where(low, k, pltpu.roll(v, HD, 1)).astype(BF16)
        kv1 = jnp.where(low, pltpu.roll(k, HD, 1), v).astype(BF16)
        m["own0"][b] = kv0
        m["own1"][b] = kv1
        m["tab0"][n_dev + b] = kv0
        m["tab1"][n_dev + b] = kv1
    pl.semaphore_wait(barrier, len(partners))

    def held(g, way, step):
        return m[f"own{g}"] if step == 0 else m[f"held{g}{way}{step}"]

    def z_copy(g, way, step, part):
        blocks = pl.ds(part * (n_b // PARTS), n_b // PARTS)
        return pltpu.make_async_remote_copy(
            src_ref=held(g, way, step - 1).at[blocks],
            dst_ref=held(g, way, step).at[blocks],
            send_sem=m["sent"].at[0],
            recv_sem=m["z_recv"].at[g, way * 4 + step - 1, part],
            device_id=dn_z if way else up_z,
            device_id_type=MESH,
        )

    def sends(way, step):
        if way:
            return (z + step - 1) % n_z < 3
        return (z < n_z - 1) & (z - step + 1 >= 0)

    def gets(way, step):
        if way:
            return (z + step) % n_z < 3
        return z - step >= 0

    def steps(way):
        return 3 if way else 4

    def x_copy(to_right, rel, part):
        half = inputs.shape[0] // 2
        rows = pl.ds(part * half, half)
        slot = rel if to_right else n_x - rel
        if rel == 1:
            src = inputs.at[rows]
        else:
            src = m["xraw"].at[1 if to_right else n_x - 1, rows]
        side = 0 if to_right else 1
        return pltpu.make_async_remote_copy(
            src_ref=src,
            dst_ref=m["xraw"].at[slot, rows],
            send_sem=m["sent"].at[1],
            recv_sem=m["x_recv"].at[side, 2 if rel == 2 else part],
            device_id=right if to_right else left,
            device_id_type=MESH,
        )

    def y_copy(g, order, z_from, r):
        to = (q + r) % PLANE
        return pltpu.make_async_remote_copy(
            src_ref=m["picked"].at[g, order, r],
            dst_ref=m[f"tab{g}"].at[z_from * PLANE + q],
            send_sem=m["sent"].at[2],
            recv_sem=m["y_recv"].at[g, order],
            device_id={"kv": z * PLANE + to},
            device_id_type=MESH,
        )

    others = pl.ds(1, PLANE - 1)

    def wait_group(ref, sem):
        pltpu.make_async_copy(ref, ref, sem).wait()

    def pick(g, order, z_from, ref):
        def one(r, carry):
            to = (q + r) % PLANE
            m["picked"][g, order, r] = ref[idx_picks[(z_from * PLANE + to) * 2 + g]]

            @pl.when(r > 1)
            def _():
                y_copy(g, order, z_from, r - 1).start()

            return carry

        lax.fori_loop(1, PLANE, one, 0)
        m[f"tab{g}"][z_from * PLANE + q] = ref[idx_picks[(z_from * PLANE + q) * 2 + g]]
        y_copy(g, order, z_from, PLANE - 1).start()

    def each_piece(g, step, act):
        @pl.when(gets(0, step))
        def _():
            act(g, step, z - step, held(g, 0, step))

        if step < 4:
            @pl.when(gets(1, step) & (z + step >= n_z))
            def _():
                act(g, 4 + step, z + step - n_z, held(g, 1, step))

    def set_out(g):
        for part in range(PARTS):
            for way in range(2):
                @pl.when(sends(way, 1))
                def _():
                    z_copy(g, way, 1, part).start()

    set_out(0)
    for part in range(2):
        x_copy(True, 1, part).start()
        x_copy(False, 1, 1 - part).start()
    pick(0, 0, z, m["own0"])
    pick(1, 0, z, m["own1"])

    def relay(g, step):
        for part in range(PARTS):
            for way in range(2):
                if step <= steps(way):
                    @pl.when(gets(way, step))
                    def _():
                        z_copy(g, way, step, part).wait_recv()

                if step + 1 <= steps(way):
                    @pl.when(sends(way, step + 1))
                    def _():
                        z_copy(g, way, step + 1, part).start()

    key_at = lax.broadcasted_iota(jnp.int32, (BLOCK, cols), 0)
    tok_at = lax.broadcasted_iota(jnp.int32, (BLOCK, cols), 1) % BLOCK
    m["bias"][0] = jnp.zeros((BLOCK, cols), F32)
    m["bias"][1] = jnp.where(key_at <= tok_at, 0.0, NEG)
    m["bias"][2] = jnp.full((BLOCK, cols), NEG, F32)
    for p in range(n_b):
        m["terms"][p, n_list] = jnp.zeros((BLOCK, 128), F32)
    loads[4].wait()
    for p in range(n_b):
        for g in range(2):
            row = [
                m["lraw"][g * per_group + r : g * per_group + r + 1, p * BLOCK : (p + 1) * BLOCK]
                for r in range(per_group)
            ]
            m["lse"][p * 2 + g] = jnp.concatenate(row, axis=1)

    for step in range(1, 5):
        relay(0, step)
        if step == 2:
            set_out(1)
        each_piece(0, step, pick)

    def relay_and_pick(g, step):
        relay(g, step)
        each_piece(g, step, pick)

    def relay_x():
        x_copy(True, 1, 0).wait_recv()
        x_copy(True, 2, 0).start()
        x_copy(False, 1, 1).wait_recv()
        x_copy(False, 2, 1).start()

    def landed(g, order, z_from, ref):
        wait_group(m["picked"].at[g, order, others], m["y_recv"].at[g, order])

    def masked_rows(ref, row, g, factor, side):
        parts = []
        for r in range(per_group):
            col = (g * per_group + r) * HD
            part = ref[pl.ds(row, BLOCK), col // 128 * 128 : col // 128 * 128 + 128]
            part = part.astype(F32) * factor
            if r % 2 != side:
                part = pltpu.roll(part, HD, 1)
            parts.append(jnp.where(low != (side == 1), part, 0.0).astype(BF16))
        return parts

    def attention(g, between):
        tab = m[f"tab{g}"]
        sdp, pd, qd, cat, shift = m["sdp"], m["pd"], m["qd"], m["cat"], m["shift"]
        chunks = [slice(n, n + CHUNK) for n in range(0, n_list, CHUNK)]
        nt = (((1,), (1,)), ((), ()))
        nn = (((1,), (0,)), ((), ()))

        def one_position(p, carry):
            row = pl.multiple_of(p * BLOCK, BLOCK)
            unit = (p * 2 + g) * n_list
            for r, part in enumerate(masked_rows(m["qraw"], row, g, HD ** -0.5, 0)):
                qd[r * BLOCK : (r + 1) * BLOCK, :] = part
            for r, part in enumerate(masked_rows(m["graw"], row, g, 1.0, 1)):
                qd[cols + r * BLOCK : cols + (r + 1) * BLOCK, :] = part
            for n in range(n_list):
                cat[n] = tab[idx_slots[unit + n]]
            for kind in range(3):
                shift[kind] = m["bias"][kind] - m["lse"][p * 2 + g] * LOG2E

            acc = jnp.zeros((8, cols), F32)
            for ch in chunks:
                both = lax.dot_general(
                    cat[ch].reshape(CHUNK * BLOCK, 128), qd[...], nt, preferred_element_type=F32
                ).reshape(CHUNK, BLOCK, 2 * cols)
                for n in range(ch.start, ch.stop):
                    prod = both[n - ch.start]
                    pr = jnp.exp2(prod[:, :cols] * LOG2E + shift[idx_kinds[unit + n]])
                    sdp[n, :, :cols] = pr
                    sdp[n, :, cols:] = prod[:, cols:]
                    pd[n, :, cols:] = pr.astype(BF16)
                    pr = pr * prod[:, cols:]
                    acc = acc + pr.reshape(BLOCK // 8, 8, cols).sum(axis=0)
            delta = acc.sum(axis=0, keepdims=True)
            for ch in chunks:
                for n in range(ch.start, ch.stop):
                    ds = sdp[n, :, :cols] * (sdp[n, :, cols:] - delta)
                    pd[n, :, :cols] = ds.astype(BF16)
                m["terms"][p, ch] = lax.dot_general(
                    pd[ch].reshape(CHUNK * BLOCK, 2 * cols), qd[...], nn, preferred_element_type=F32
                ).reshape(CHUNK, BLOCK, 128)
            dq_t = lax.dot_general(
                cat[...].reshape(n_list * BLOCK, 128),
                pd[:, :, :cols].reshape(n_list * BLOCK, cols),
                (((0,), (0,)), ((), ())),
                preferred_element_type=F32,
            )
            dq = dq_t.T * (HD ** -0.5)
            for pair in range(per_group // 2):
                even = dq[(2 * pair) * BLOCK : (2 * pair + 1) * BLOCK]
                odd = dq[(2 * pair + 1) * BLOCK : (2 * pair + 2) * BLOCK]
                col = g * per_group * HD + pair * 128
                m["qg"][pl.ds(row, BLOCK), col : col + 128] = jnp.where(
                    low, even, pltpu.roll(odd, HD, 1)
                )
            for at, act in between.items():
                @pl.when(p == at)
                def _():
                    act()

            return carry

        lax.fori_loop(0, n_b, one_position, 0)

    def summed_terms(g, j):
        at = (g * (n_dev + n_b) + j) * n_b
        total = m["terms"][0, idx_inv[at]]
        for p in range(1, n_b):
            total = total + m["terms"][p, idx_inv[at + p]]
        return total

    def b_copy(g, d, r):
        to = (q + r) % PLANE
        return pltpu.make_async_remote_copy(
            src_ref=m["ret"].at[g, (z - d) * PLANE + to],
            dst_ref=m["back"].at[g, d, q],
            send_sem=m["sent"].at[3],
            recv_sem=m["b_recv"].at[g, d],
            device_id={"kv": z * PLANE + to},
            device_id_type=MESH,
        )

    def give_back(g):
        for d in RETURN_ORDER:
            @pl.when(z - d >= 0)
            def _():
                for r in list(range(1, PLANE)) + [0]:
                    j = (z - d) * PLANE + (q + r) % PLANE
                    m["ret"][g, j] = summed_terms(g, j).astype(BF16)
                for r in range(1, PLANE):
                    b_copy(g, d, r).start()

        def own(b, carry):
            m["own_tot"][g, b] = summed_terms(g, n_dev + b)
            return carry

        lax.fori_loop(0, n_b, own, 0)

    def accumulate(g, d, part):
        rows = slice(part * PART_ROWS, (part + 1) * PART_ROWS)
        accs = [jnp.zeros((PART_ROWS, 128), F32) for _ in range(n_b)]
        for r in range(PLANE):
            frm = (q + r) % PLANE
            if r == 0:
                val = m["ret"][g, (z - d) * PLANE + q, rows, :]
            else:
                val = m["back"][g, d, frm, rows, :]
            val = val.astype(F32)
            block = idx_picks[((z - d) * PLANE + frm) * 2 + g]
            for b in range(n_b):
                accs[b] = accs[b] + jnp.where(block == b, val, 0.0)
        for b in range(n_b):
            m["acc"][g, b, rows, :] = accs[b]

    def dn_copy(g, d, part):
        return pltpu.make_async_remote_copy(
            src_ref=m["zs"].at[g, d, part],
            dst_ref=m["zr_dn"].at[g, d - 1, part],
            send_sem=m["sent"].at[4],
            recv_sem=m["r_recv_dn"].at[g, d - 1, part],
            device_id=dn_z,
            device_id_type=MESH,
        )

    def up_copy(g, d, at, part):
        to = n_z - 1 if at else n_z - 1 - d
        return pltpu.make_async_remote_copy(
            src_ref=m["zs"].at[g, d, part],
            dst_ref=m["zr_up"].at[g, at, part],
            send_sem=m["sent"].at[4],
            recv_sem=m["r_recv_up"].at[g, at, part],
            device_id={"kv": to * PLANE + q},
            device_id_type=MESH,
        )

    def add_arrival(g, copy, ref, part):
        copy.wait_recv()
        rows = slice(part * PART_ROWS, (part + 1) * PART_ROWS)
        for b in range(n_b):
            m["acc"][g, b, rows, :] += ref[b].astype(F32)

    def dn_arrival(g, d, part):
        @pl.when(z < n_z - 1)
        def _():
            add_arrival(g, dn_copy(g, d, part), m["zr_dn"].at[g, d - 1, part], part)

    def up_arrival(g, at, part):
        add_arrival(g, up_copy(g, 5, at, part), m["zr_up"].at[g, at, part], part)

    def store_out(g, d, part):
        rows = slice(part * PART_ROWS, (part + 1) * PART_ROWS)
        for b in range(n_b):
            m["zs"][g, d, part, b] = m["acc"][g, b, rows, :].astype(BF16)

    def collect(g, d):
        @pl.when(z - d >= 0)
        def _():
            wait_group(m["back"].at[g, d, others], m["b_recv"].at[g, d])
            for part in range(ROW_PARTS):
                accumulate(g, d, part)
                if d < 4:
                    dn_arrival(g, d + 1, part)
                if d in (6, 7):
                    @pl.when(z == n_z - 1)
                    def _():
                        for at in {6: (2,), 7: (1, 3)}[d]:
                            up_arrival(g, at, part)

                if d == 0:
                    @pl.when(z < 3)
                    def _():
                        up_arrival(g, 0, part)
                    continue
                store_out(g, d, part)
                if d < 5:
                    dn_copy(g, d, part).start()
                else:
                    @pl.when(z == n_z - 1)
                    def _():
                        up_copy(g, d, 0, part).start()

                    for plane, at in {5: ((5, 1), (6, 2)), 6: ((6, 3),), 7: ()}[d]:
                        @pl.when(z == plane)
                        def _():
                            up_copy(g, d, at, part).start()

    def wait_fetch(g):
        landed(g, 0, z, None)
        for step in range(1, 5):
            each_piece(g, step, landed)

    relay_and_pick(1, 1)
    relay_and_pick(1, 2)
    loads[2].wait()
    loads[3].wait()
    wait_fetch(0)
    attention(
        0,
        {
            0: functools.partial(relay_and_pick, 1, 3),
            2: functools.partial(relay_and_pick, 1, 4),
            4: relay_x,
        },
    )
    give_back(0)
    wait_fetch(1)
    attention(1, {2 + i: functools.partial(collect, 0, RETURN_ORDER[i]) for i in range(3)})
    give_back(1)
    out_q = pltpu.make_async_copy(m["qg"], query_grad, m["out_sem"].at[0])
    out_q.start()
    def c_copy(g, i):
        return pltpu.make_async_remote_copy(
            src_ref=m["wpart"].at[g, i, 1 - c],
            dst_ref=m["crecv"].at[g, i],
            send_sem=m["sent"].at[5],
            recv_sem=m["c_recv"].at[g, i],
            device_id={"kv": z * PLANE + y * N_C + (1 - c)},
            device_id_type=MESH,
        )

    def wy_copy(g, part, r):
        to = (y + r) % N_Y
        return pltpu.make_async_remote_copy(
            src_ref=m["wy"].at[g, part, r],
            dst_ref=m["wyr"].at[g, part, r],
            send_sem=m["sent"].at[6],
            recv_sem=m["wy_recv"].at[g, part, r - 1],
            device_id={"kv": z * PLANE + to * N_C + c},
            device_id_type=MESH,
        )

    half = inputs.shape[1] // 2

    def combine(g):
        for b in range(n_b):
            total = m["acc"][g, b] + m["own_tot"][g, b]
            m["acc"][g, b] = total
            m["kg"][b * BLOCK : (b + 1) * BLOCK, :] = total.astype(BF16)
        m["kg_t"][...] = m["kg"][...].T

    def own_terms(g, i):
        w_t = [
            lax.dot_general(
                m["kg_t"][:HD, :], m["xraw"][i, :, h * half : (h + 1) * half],
                (((1,), (0,)), ((), ())), preferred_element_type=F32,
            )
            for h in range(2)
        ]
        w = jnp.concatenate(w_t, axis=0).T.astype(BF16)
        for yy in range(N_Y):
            for cc in range(N_C):
                first = (yy * N_C + cc) * BLOCK
                m["wpart"][g, i, cc, yy] = w[first : first + BLOCK]

    def core_sum(g, i):
        c_copy(g, i).wait_recv()
        for r in range(N_Y):
            yy = (y + r) % N_Y
            both = m["wpart"][g, i, c, yy].astype(F32) + m["crecv"][g, i, yy].astype(F32)
            if r:
                m["wy"][g, i // 2, r, i % 2] = both.astype(BF16)
            else:
                m["wy_own"][g, i] = both
        if i % 2:
            for r in (2, 1, 3):
                wy_copy(g, i // 2, r).start()

    def terms_out(g):
        combine(g)
        for i in range(n_x):
            own_terms(g, i)
            if i:
                c_copy(g, i - 1).start()
        c_copy(g, n_x - 1).start()

    for g, d in [
        (0, 2), (1, 4), (0, 6), (1, 5), (0, 1), (1, 3), (0, 7), (1, 6), (1, 2), (0, 0)
    ]:
        collect(g, d)
    x_copy(True, 1, 1).wait_recv()
    x_copy(False, 1, 0).wait_recv()
    x_copy(True, 2, 0).wait_recv()
    x_copy(False, 2, 1).wait_recv()
    loads[5].wait()
    terms_out(0)
    collect(1, 7)
    for i in range(n_x):
        core_sum(0, i)
    collect(1, 1)
    collect(1, 0)
    combine(1)
    lag = 2
    for i in range(n_x + lag):
        if i < n_x:
            own_terms(1, i)
        if 0 < i <= n_x:
            c_copy(1, i - 1).start()
        if i >= lag:
            core_sum(1, i - lag)
    for b in range(n_b):
        rows = slice(b * BLOCK, (b + 1) * BLOCK)
        t0, t1 = m["acc"][0, b], m["acc"][1, b]
        key_grad[rows, :] = jnp.where(low, t0, pltpu.roll(t1, HD, 1))
        value_grad[rows, :] = jnp.where(low, pltpu.roll(t0, HD, 1), t1)

    def z_of(i):
        return 2 * ((x + n_x - i // 2) % n_x) + i % 2

    def wz_copy(i):
        return pltpu.make_async_remote_copy(
            src_ref=m["wz"].at[i],
            dst_ref=m["wzr"].at[z],
            send_sem=m["sent"].at[7],
            recv_sem=m["wz_recv"].at[z],
            device_id={"kv": z_of(i) * PLANE + q},
            device_id_type=MESH,
        )

    def sent(g, order, z_from, ref):
        wait_group(m["picked"].at[g, order, others], m["sent"].at[2])

    for g in range(2):
        for way in range(2):
            for step in range(1, steps(way) + 1):
                @pl.when(sends(way, step))
                def _():
                    for part in range(PARTS):
                        z_copy(g, way, step, part).wait_send()

        sent(g, 0, z, None)
        for step in range(1, 5):
            each_piece(g, step, sent)
        for d in range(8):
            @pl.when(z - d >= 0)
            def _():
                wait_group(m["back"].at[g, d, others], m["sent"].at[3])

            for part in range(ROW_PARTS):
                if 0 < d < 5:
                    @pl.when(z - d >= 0)
                    def _():
                        dn_copy(g, d, part).wait_send()
                elif d:
                    @pl.when(z - d >= 0)
                    def _():
                        up_copy(g, d, 0, part).wait_send()

    for part in range(2):
        x_copy(True, 1, part).wait_send()
        x_copy(False, 1, part).wait_send()
    x_copy(True, 2, 0).wait_send()
    x_copy(False, 2, 1).wait_send()
    for g in range(2):
        for i in range(n_x):
            c_copy(g, i).wait_send()
    out_q.wait()

    for g, part in ((0, 0), (0, 1), (1, 0), (1, 1)):
        for r in (1, 3, 2):
            wy_copy(g, part, r).wait_recv()
        if g == 0:
            continue
        for i in (2 * part, 2 * part + 1):
            total = []
            for h in range(2):
                total.append(m["wy_own"][h, i])
                for r in range(1, N_Y):
                    total[h] = total[h] + m["wyr"][h, part, r, i % 2].astype(F32)
            tiles = [
                jnp.where(low, total[0], pltpu.roll(total[1], HD, 1)),
                jnp.where(low, pltpu.roll(total[0], HD, 1), total[1]),
            ]
            for h in range(2):
                m["wz_own"][2 * i + h] = tiles[h]
                m["wz"][2 * i + h] = tiles[h].astype(BF16)
        for i in range(4 * part, 4 * part + 4):
            @pl.when(z_of(i) != z)
            def _():
                wz_copy(i).start()
    for g in range(2):
        for part in range(2):
            for r in range(1, N_Y):
                wy_copy(g, part, r).wait_send()
    mine = 2 * ((x + n_x - z // 2) % n_x) + z % 2
    total = m["wz_own"][mine]
    for r in range(1, n_z):
        frm = (z + r) % n_z
        pltpu.make_async_remote_copy(
            src_ref=m["wz"].at[0],
            dst_ref=m["wzr"].at[frm],
            send_sem=m["sent"].at[7],
            recv_sem=m["wz_recv"].at[frm],
            device_id={"kv": frm * PLANE + q},
            device_id_type=MESH,
        ).wait_recv()
        total = total + m["wzr"][frm].astype(F32)
    weight_grad[...] = total
    for i in range(n_z):
        @pl.when(z_of(i) != z)
        def _():
            wz_copy(i).wait_send()


def put_kernel(q_src, k_src, v_src, w_src, q_dst, k_dst, v_dst, w_dst, q_mid, sem):
    rows = q_mid.shape[0] // 3
    part = [pl.ds(i * rows, rows) for i in range(3)]
    into = [
        pltpu.make_async_copy(q_src.at[part[i]], q_mid.at[part[i]], sem.at[i]) for i in range(3)
    ]
    rest = [
        pltpu.make_async_copy(src, dst, sem.at[3 + i])
        for i, (src, dst) in enumerate([(k_src, k_dst), (v_src, v_dst), (w_src, w_dst)])
    ]
    out = [
        pltpu.make_async_copy(q_mid.at[part[i]], q_dst.at[part[i]], sem.at[6 + i]) for i in range(3)
    ]
    for copy in into + rest:
        copy.start()
    for i in range(3):
        into[i].wait()
        out[i].start()
    for copy in rest + out:
        copy.wait()


def put_out(query_grad, key_grad, value_grad, weight_grad):
    hbm = pl.BlockSpec(memory_space=pltpu.HBM)
    vm = pl.BlockSpec(memory_space=pltpu.VMEM)
    arrays = (query_grad, key_grad, value_grad, weight_grad)
    return pl.pallas_call(
        put_kernel,
        out_shape=tuple(jax.ShapeDtypeStruct(a.shape, a.dtype) for a in arrays),
        in_specs=[hbm, vm, vm, vm],
        out_specs=(hbm,) * 4,
        scratch_shapes=[pltpu.VMEM(query_grad.shape, F32), pltpu.SemaphoreType.DMA((9,))],
        compiler_params=pltpu.CompilerParams(vmem_limit_bytes=int(53.4 * 1024 * 1024)),
        name="put_out",
    )(*arrays)


def index_table(chosen, n_b, n_dev):
    groups, _, n_list = chosen.shape
    me = lax.axis_index("kv")
    z, q = place()
    plane = lax.dynamic_slice_in_dim(chosen, z * PLANE * n_b, PLANE * n_b, 1)
    column = (jnp.arange(n_dev // PLANE) * PLANE + q) * n_b
    offs = plane[..., None] - column
    offs = jnp.where((offs >= 0) & (offs < n_b), offs, 0)
    picks = jnp.max(offs.reshape(groups, PLANE, n_b * n_list, -1), axis=2)
    picks = picks.transpose(2, 1, 0).reshape(-1)
    lists = lax.dynamic_slice_in_dim(chosen, me * n_b, n_b, 1)
    owner = lists // n_b
    slot = jnp.where(owner == me, n_dev + lists % n_b, jnp.maximum(owner, 0))
    at_diag = lists == me * n_b + jnp.arange(n_b)[None, :, None]
    kind = jnp.where(lists < 0, 2, at_diag.astype(jnp.int32))
    listed = (slot[..., None] == jnp.arange(n_dev + n_b)) & (lists >= 0)[..., None]
    inverse = jnp.min(
        jnp.where(listed, jnp.arange(n_list)[:, None], n_list), axis=2
    )
    slots = slot.transpose(1, 0, 2).reshape(-1)
    kinds = kind.transpose(1, 0, 2).reshape(-1)
    inverse = inverse.transpose(0, 2, 1).reshape(-1)
    return picks, slots, kinds, inverse


def local(queries, key_heads, values, log_sums, out_grad, inputs, chosen):
    n_dev = lax.axis_size("kv")
    n_x = lax.axis_size("tp")
    rows, feats = inputs.shape
    n_b = rows // BLOCK
    heads = log_sums.shape[0]
    n_list = chosen.shape[2]
    idx = index_table(chosen, n_b, n_dev)
    scratch = scratch_list(rows, n_dev, n_x, n_list, feats, heads)
    hbm = pl.BlockSpec(memory_space=pltpu.HBM)
    vm = pl.BlockSpec(memory_space=pltpu.VMEM)
    results = pl.pallas_call(
        functools.partial(
            fused_kernel, [name for name, _ in scratch], n_dev // PLANE, n_x, n_list
        ),
        out_shape=(
            jax.ShapeDtypeStruct(queries.shape, F32),
            jax.ShapeDtypeStruct(key_heads.shape, F32),
            jax.ShapeDtypeStruct(values.shape, F32),
            jax.ShapeDtypeStruct((feats * n_x // n_dev, 128), F32),
        ),
        in_specs=[pl.BlockSpec(memory_space=pltpu.SMEM)] * 4 + [hbm] * 6,
        out_specs=(hbm, vm, vm, vm),
        scratch_shapes=[kind for _, kind in scratch],
        compiler_params=pltpu.CompilerParams(
            collective_id=0, has_side_effects=True, vmem_limit_bytes=53 * 1024 * 1024
        ),
        name="fused",
    )(
        *idx,
        key_heads.reshape(n_b, BLOCK, -1),
        values.reshape(n_b, BLOCK, -1),
        queries,
        out_grad,
        log_sums,
        inputs,
    )
    return put_out(*results)


def solution(mesh):
    placed = (
        P("kv", "tp"),
        P("kv", "tp"),
        P("kv", "tp"),
        P("tp", "kv"),
        P("kv", "tp"),
        P("kv", "tp"),
        P("tp", None, None),
    )
    return jax.shard_map(
        local,
        mesh=mesh,
        in_specs=placed,
        out_specs=(P("kv", "tp"), P("kv", "tp"), P("kv", "tp"), P("kv", "tp")),
        check_vma=False,
    )
```

```python
import functools

import jax
import jax.numpy as jnp
from jax import lax
from jax.experimental import pallas as pl
from jax.experimental.pallas import tpu as pltpu
from jax.sharding import PartitionSpec as P

HD = 64
BLOCK = 64
NEG = -1e30
LOG2E = 1.4426950408889634
CHUNK = 8
PARTS = 3
ROW_PARTS = 4
PART_ROWS = BLOCK // ROW_PARTS
N_Y = 4
N_C = 2
PLANE = N_Y * N_C
MESH = pl.DeviceIdType.MESH
RETURN_ORDER = (4, 5, 3, 6, 2, 7, 1, 0)
F32, BF16 = jnp.float32, jnp.bfloat16


def place():
    me = lax.axis_index("kv")
    return me // PLANE, me % PLANE


def scratch_list(rows, n_dev, n_x, n_list, feats, heads):
    n_b = rows // BLOCK
    tile = (BLOCK, 128)
    cols = heads // 2 * BLOCK
    dma = pltpu.SemaphoreType.DMA
    out = [
        ("kraw", pltpu.VMEM((n_b,) + tile, BF16)),
        ("vraw", pltpu.VMEM((n_b,) + tile, BF16)),
        ("qraw", pltpu.VMEM((rows, heads * HD), BF16)),
        ("graw", pltpu.VMEM((rows, heads * HD), BF16)),
        ("lraw", pltpu.VMEM((heads, rows), F32)),
        ("xraw", pltpu.VMEM((n_x, rows, feats), BF16)),
        ("lse", pltpu.VMEM((n_b * 2, 1, cols), F32)),
        ("bias", pltpu.VMEM((3,) + (BLOCK, cols), F32)),
        ("shift", pltpu.VMEM((3,) + (BLOCK, cols), F32)),
        ("qg", pltpu.VMEM((rows, heads * HD), F32)),
        ("picked", pltpu.VMEM((2, 8, PLANE) + tile, BF16)),
        ("qd", pltpu.VMEM((2 * cols, 128), BF16)),
        ("cat", pltpu.VMEM((n_list,) + tile, BF16)),
        ("sdp", pltpu.VMEM((n_list, BLOCK, 2 * cols), F32)),
        ("pd", pltpu.VMEM((n_list, BLOCK, 2 * cols), BF16)),
        ("terms", pltpu.VMEM((n_b, n_list + 1) + tile, F32)),
        ("ret", pltpu.VMEM((2, n_dev) + tile, BF16)),
        ("own_tot", pltpu.VMEM((2, n_b) + tile, F32)),
        ("back", pltpu.VMEM((2, 8, PLANE) + tile, BF16)),
        ("acc", pltpu.VMEM((2, n_b) + tile, F32)),
        ("zs", pltpu.VMEM((2, 8, ROW_PARTS, n_b, PART_ROWS, 128), BF16)),
        ("zr_dn", pltpu.VMEM((2, 4, ROW_PARTS, n_b, PART_ROWS, 128), BF16)),
        ("zr_up", pltpu.VMEM((2, 4, ROW_PARTS, n_b, PART_ROWS, 128), BF16)),
        ("kg", pltpu.VMEM((rows, 128), BF16)),
        ("kg_t", pltpu.VMEM((128, rows), BF16)),
        ("wpart", pltpu.VMEM((2, n_x, N_C, N_Y) + tile, BF16)),
        ("crecv", pltpu.VMEM((2, n_x, N_Y) + tile, BF16)),
        ("wy", pltpu.VMEM((2, 2, N_Y, n_x // 2) + tile, BF16)),
        ("wy_own", pltpu.VMEM((2, n_x) + tile, F32)),
        ("wyr", pltpu.VMEM((2, 2, N_Y, n_x // 2) + tile, BF16)),
        ("wz", pltpu.VMEM((8,) + tile, BF16)),
        ("wz_own", pltpu.VMEM((8,) + tile, F32)),
        ("wzr", pltpu.VMEM((8,) + tile, BF16)),
        ("in_sem", dma((6,))),
        ("out_sem", dma((1,))),
        ("sent", dma((8,))),
        ("z_recv", dma((2, 7, PARTS))),
        ("y_recv", dma((2, 8))),
        ("x_recv", dma((2, 3))),
        ("b_recv", dma((2, 8))),
        ("r_recv_dn", dma((2, 4, ROW_PARTS))),
        ("r_recv_up", dma((2, 4, ROW_PARTS))),
        ("c_recv", dma((2, n_x))),
        ("wy_recv", dma((2, 2, N_Y - 1))),
        ("wz_recv", dma((8,))),
    ]
    for g in range(2):
        out.append((f"own{g}", pltpu.VMEM((n_b,) + tile, BF16)))
        out.append((f"tab{g}", pltpu.VMEM((n_dev + n_b,) + tile, BF16)))
        for step in range(1, 5):
            out.append((f"held{g}0{step}", pltpu.VMEM((n_b,) + tile, BF16)))
        for step in range(1, 4):
            out.append((f"held{g}1{step}", pltpu.VMEM((n_b,) + tile, BF16)))
    return out


def fused_kernel(names, n_z, n_x, n_list, *refs):
    idx, keys, vals, queries, out_grad, log_sums, inputs = refs[:7]
    query_grad, key_grad, value_grad, weight_grad = refs[7:11]
    m = dict(zip(names, refs[11:]))
    n_b = m["kraw"].shape[0]
    n_dev = n_z * PLANE
    heads = m["lraw"].shape[0]
    per_group = heads // 2
    cols = per_group * BLOCK
    z, q = place()
    y, c = q // N_C, q % N_C
    x = lax.axis_index("tp")

    barrier = pltpu.get_barrier_semaphore()
    partners = [{"kv": (z + r) % n_z * PLANE + q} for r in range(1, n_z)]
    partners += [{"kv": z * PLANE + (q + r) % PLANE} for r in range(1, PLANE)]
    right, left = {"tp": (x + 1) % n_x}, {"tp": (x + n_x - 1) % n_x}
    partners += [right, left]
    for who in partners:
        pl.semaphore_signal(barrier, inc=1, device_id=who, device_id_type=MESH)

    loads = [
        pltpu.make_async_copy(src, dst, m["in_sem"].at[i])
        for i, (src, dst) in enumerate(
            [
                (keys, m["kraw"]),
                (vals, m["vraw"]),
                (queries, m["qraw"]),
                (out_grad, m["graw"]),
                (log_sums, m["lraw"]),
                (inputs, m["xraw"].at[0]),
            ]
        )
    ]
    for copy in loads:
        copy.start()
    up_z = {"kv": (z + 1) % n_z * PLANE + q}
    dn_z = {"kv": (z + n_z - 1) % n_z * PLANE + q}
    lane = lax.broadcasted_iota(jnp.int32, (BLOCK, 128), 1)
    low = lane < HD
    loads[0].wait()
    loads[1].wait()
    for b in range(n_b):
        k = m["kraw"][b].astype(F32)
        v = m["vraw"][b].astype(F32)
        kv0 = jnp.where(low, k, pltpu.roll(v, HD, 1)).astype(BF16)
        kv1 = jnp.where(low, pltpu.roll(k, HD, 1), v).astype(BF16)
        m["own0"][b] = kv0
        m["own1"][b] = kv1
        m["tab0"][n_dev + b] = kv0
        m["tab1"][n_dev + b] = kv1
    pl.semaphore_wait(barrier, len(partners))

    def held(g, way, step):
        return m[f"own{g}"] if step == 0 else m[f"held{g}{way}{step}"]

    def z_copy(g, way, step, part):
        blocks = pl.ds(part * (n_b // PARTS), n_b // PARTS)
        return pltpu.make_async_remote_copy(
            src_ref=held(g, way, step - 1).at[blocks],
            dst_ref=held(g, way, step).at[blocks],
            send_sem=m["sent"].at[0],
            recv_sem=m["z_recv"].at[g, way * 4 + step - 1, part],
            device_id=dn_z if way else up_z,
            device_id_type=MESH,
        )

    def sends(way, step):
        if way:
            return (z + step - 1) % n_z < 3
        return (z < n_z - 1) & (z - step + 1 >= 0)

    def gets(way, step):
        if way:
            return (z + step) % n_z < 3
        return z - step >= 0

    def steps(way):
        return 3 if way else 4

    def x_copy(to_right, rel, part):
        half = inputs.shape[0] // 2
        rows = pl.ds(part * half, half)
        slot = rel if to_right else n_x - rel
        if rel == 1:
            src = inputs.at[rows]
        else:
            src = m["xraw"].at[1 if to_right else n_x - 1, rows]
        side = 0 if to_right else 1
        return pltpu.make_async_remote_copy(
            src_ref=src,
            dst_ref=m["xraw"].at[slot, rows],
            send_sem=m["sent"].at[1],
            recv_sem=m["x_recv"].at[side, 2 if rel == 2 else part],
            device_id=right if to_right else left,
            device_id_type=MESH,
        )

    def y_copy(g, order, z_from, r):
        to = (q + r) % PLANE
        return pltpu.make_async_remote_copy(
            src_ref=m["picked"].at[g, order, r],
            dst_ref=m[f"tab{g}"].at[z_from * PLANE + q],
            send_sem=m["sent"].at[2],
            recv_sem=m["y_recv"].at[g, order],
            device_id={"kv": z * PLANE + to},
            device_id_type=MESH,
        )

    others = pl.ds(1, PLANE - 1)

    def wait_group(ref, sem):
        pltpu.make_async_copy(ref, ref, sem).wait()

    def pick(g, order, z_from, ref):
        def one(r, carry):
            to = (q + r) % PLANE
            m["picked"][g, order, r] = ref[idx[24 + g * n_z + z_from, to * n_b]]

            @pl.when(r > 1)
            def _():
                y_copy(g, order, z_from, r - 1).start()

            return carry

        lax.fori_loop(1, PLANE, one, 0)
        m[f"tab{g}"][z_from * PLANE + q] = ref[idx[24 + g * n_z + z_from, q * n_b]]
        y_copy(g, order, z_from, PLANE - 1).start()

    def each_piece(g, step, act):
        @pl.when(gets(0, step))
        def _():
            act(g, step, z - step, held(g, 0, step))

        if step < 4:
            @pl.when(gets(1, step) & (z + step >= n_z))
            def _():
                act(g, 4 + step, z + step - n_z, held(g, 1, step))

    def set_out(g):
        for part in range(PARTS):
            for way in range(2):
                @pl.when(sends(way, 1))
                def _():
                    z_copy(g, way, 1, part).start()

    set_out(0)
    for part in range(2):
        x_copy(True, 1, part).start()
        x_copy(False, 1, 1 - part).start()
    pick(0, 0, z, m["own0"])
    pick(1, 0, z, m["own1"])

    def relay(g, step):
        for part in range(PARTS):
            for way in range(2):
                if step <= steps(way):
                    @pl.when(gets(way, step))
                    def _():
                        z_copy(g, way, step, part).wait_recv()

                if step + 1 <= steps(way):
                    @pl.when(sends(way, step + 1))
                    def _():
                        z_copy(g, way, step + 1, part).start()

    key_at = lax.broadcasted_iota(jnp.int32, (BLOCK, cols), 0)
    tok_at = lax.broadcasted_iota(jnp.int32, (BLOCK, cols), 1) % BLOCK
    m["bias"][0] = jnp.zeros((BLOCK, cols), F32)
    m["bias"][1] = jnp.where(key_at <= tok_at, 0.0, NEG)
    m["bias"][2] = jnp.full((BLOCK, cols), NEG, F32)
    for p in range(n_b):
        m["terms"][p, n_list] = jnp.zeros((BLOCK, 128), F32)
    loads[4].wait()
    for p in range(n_b):
        for g in range(2):
            row = [
                m["lraw"][g * per_group + r : g * per_group + r + 1, p * BLOCK : (p + 1) * BLOCK]
                for r in range(per_group)
            ]
            m["lse"][p * 2 + g] = jnp.concatenate(row, axis=1)

    for step in range(1, 5):
        relay(0, step)
        if step == 2:
            set_out(1)
        each_piece(0, step, pick)

    def relay_and_pick(g, step):
        relay(g, step)
        each_piece(g, step, pick)

    def relay_x():
        x_copy(True, 1, 0).wait_recv()
        x_copy(True, 2, 0).start()
        x_copy(False, 1, 1).wait_recv()
        x_copy(False, 2, 1).start()

    def landed(g, order, z_from, ref):
        wait_group(m["picked"].at[g, order, others], m["y_recv"].at[g, order])

    def masked_rows(ref, row, g, factor, side):
        parts = []
        for r in range(per_group):
            col = (g * per_group + r) * HD
            part = ref[pl.ds(row, BLOCK), col // 128 * 128 : col // 128 * 128 + 128]
            part = part.astype(F32) * factor
            if r % 2 != side:
                part = pltpu.roll(part, HD, 1)
            parts.append(jnp.where(low != (side == 1), part, 0.0).astype(BF16))
        return parts

    def attention(g, between):
        tab = m[f"tab{g}"]
        sdp, pd, qd, cat, shift = m["sdp"], m["pd"], m["qd"], m["cat"], m["shift"]
        chunks = [slice(n, n + CHUNK) for n in range(0, n_list, CHUNK)]
        nt = (((1,), (1,)), ((), ()))
        nn = (((1,), (0,)), ((), ()))

        def one_position(p, carry):
            row = pl.multiple_of(p * BLOCK, BLOCK)
            for r, part in enumerate(masked_rows(m["qraw"], row, g, HD ** -0.5, 0)):
                qd[r * BLOCK : (r + 1) * BLOCK, :] = part
            for r, part in enumerate(masked_rows(m["graw"], row, g, 1.0, 1)):
                qd[cols + r * BLOCK : cols + (r + 1) * BLOCK, :] = part
            for n in range(n_list):
                cat[n] = tab[idx[p, g * n_list + n]]
            for kind in range(3):
                shift[kind] = m["bias"][kind] - m["lse"][p * 2 + g] * LOG2E

            acc = jnp.zeros((8, cols), F32)
            for ch in chunks:
                both = lax.dot_general(
                    cat[ch].reshape(CHUNK * BLOCK, 128), qd[...], nt, preferred_element_type=F32
                ).reshape(CHUNK, BLOCK, 2 * cols)
                for n in range(ch.start, ch.stop):
                    prod = both[n - ch.start]
                    pr = jnp.exp2(prod[:, :cols] * LOG2E + shift[idx[p, (2 + g) * n_list + n]])
                    sdp[n, :, :cols] = pr
                    sdp[n, :, cols:] = prod[:, cols:]
                    pd[n, :, cols:] = pr.astype(BF16)
                    pr = pr * prod[:, cols:]
                    acc = acc + pr.reshape(BLOCK // 8, 8, cols).sum(axis=0)
            delta = acc.sum(axis=0, keepdims=True)
            for ch in chunks:
                for n in range(ch.start, ch.stop):
                    ds = sdp[n, :, :cols] * (sdp[n, :, cols:] - delta)
                    pd[n, :, :cols] = ds.astype(BF16)
                m["terms"][p, ch] = lax.dot_general(
                    pd[ch].reshape(CHUNK * BLOCK, 2 * cols), qd[...], nn, preferred_element_type=F32
                ).reshape(CHUNK, BLOCK, 128)
            dq_t = lax.dot_general(
                cat[...].reshape(n_list * BLOCK, 128),
                pd[:, :, :cols].reshape(n_list * BLOCK, cols),
                (((0,), (0,)), ((), ())),
                preferred_element_type=F32,
            )
            dq = dq_t.T * (HD ** -0.5)
            for pair in range(per_group // 2):
                even = dq[(2 * pair) * BLOCK : (2 * pair + 1) * BLOCK]
                odd = dq[(2 * pair + 1) * BLOCK : (2 * pair + 2) * BLOCK]
                col = g * per_group * HD + pair * 128
                m["qg"][pl.ds(row, BLOCK), col : col + 128] = jnp.where(
                    low, even, pltpu.roll(odd, HD, 1)
                )
            for at, act in between.items():
                @pl.when(p == at)
                def _():
                    act()

            return carry

        lax.fori_loop(0, n_b, one_position, 0)

    def summed_terms(g, j):
        total = m["terms"][0, idx[8 + 8 * g, j]]
        for p in range(1, n_b):
            total = total + m["terms"][p, idx[8 + 8 * g + p, j]]
        return total

    def b_copy(g, d, r):
        to = (q + r) % PLANE
        return pltpu.make_async_remote_copy(
            src_ref=m["ret"].at[g, (z - d) * PLANE + to],
            dst_ref=m["back"].at[g, d, q],
            send_sem=m["sent"].at[3],
            recv_sem=m["b_recv"].at[g, d],
            device_id={"kv": z * PLANE + to},
            device_id_type=MESH,
        )

    def give_back(g):
        for d in RETURN_ORDER:
            @pl.when(z - d >= 0)
            def _():
                for r in list(range(1, PLANE)) + [0]:
                    j = (z - d) * PLANE + (q + r) % PLANE
                    m["ret"][g, j] = summed_terms(g, j).astype(BF16)
                for r in range(1, PLANE):
                    b_copy(g, d, r).start()

        def own(b, carry):
            m["own_tot"][g, b] = summed_terms(g, n_dev + b)
            return carry

        lax.fori_loop(0, n_b, own, 0)

    def accumulate(g, d, part):
        rows = slice(part * PART_ROWS, (part + 1) * PART_ROWS)
        accs = [jnp.zeros((PART_ROWS, 128), F32) for _ in range(n_b)]
        for r in range(PLANE):
            frm = (q + r) % PLANE
            if r == 0:
                val = m["ret"][g, (z - d) * PLANE + q, rows, :]
            else:
                val = m["back"][g, d, frm, rows, :]
            val = val.astype(F32)
            block = idx[24 + g * n_z + z - d, frm * n_b]
            for b in range(n_b):
                accs[b] = accs[b] + jnp.where(block == b, val, 0.0)
        for b in range(n_b):
            m["acc"][g, b, rows, :] = accs[b]

    def dn_copy(g, d, part):
        return pltpu.make_async_remote_copy(
            src_ref=m["zs"].at[g, d, part],
            dst_ref=m["zr_dn"].at[g, d - 1, part],
            send_sem=m["sent"].at[4],
            recv_sem=m["r_recv_dn"].at[g, d - 1, part],
            device_id=dn_z,
            device_id_type=MESH,
        )

    def up_copy(g, d, at, part):
        to = n_z - 1 if at else n_z - 1 - d
        return pltpu.make_async_remote_copy(
            src_ref=m["zs"].at[g, d, part],
            dst_ref=m["zr_up"].at[g, at, part],
            send_sem=m["sent"].at[4],
            recv_sem=m["r_recv_up"].at[g, at, part],
            device_id={"kv": to * PLANE + q},
            device_id_type=MESH,
        )

    def add_arrival(g, copy, ref, part):
        copy.wait_recv()
        rows = slice(part * PART_ROWS, (part + 1) * PART_ROWS)
        for b in range(n_b):
            m["acc"][g, b, rows, :] += ref[b].astype(F32)

    def dn_arrival(g, d, part):
        @pl.when(z < n_z - 1)
        def _():
            add_arrival(g, dn_copy(g, d, part), m["zr_dn"].at[g, d - 1, part], part)

    def up_arrival(g, at, part):
        add_arrival(g, up_copy(g, 5, at, part), m["zr_up"].at[g, at, part], part)

    def store_out(g, d, part):
        rows = slice(part * PART_ROWS, (part + 1) * PART_ROWS)
        for b in range(n_b):
            m["zs"][g, d, part, b] = m["acc"][g, b, rows, :].astype(BF16)

    def collect(g, d):
        @pl.when(z - d >= 0)
        def _():
            wait_group(m["back"].at[g, d, others], m["b_recv"].at[g, d])
            for part in range(ROW_PARTS):
                accumulate(g, d, part)
                if d < 4:
                    dn_arrival(g, d + 1, part)
                if d in (6, 7):
                    @pl.when(z == n_z - 1)
                    def _():
                        for at in {6: (2,), 7: (1, 3)}[d]:
                            up_arrival(g, at, part)

                if d == 0:
                    @pl.when(z < 3)
                    def _():
                        up_arrival(g, 0, part)
                    continue
                store_out(g, d, part)
                if d < 5:
                    dn_copy(g, d, part).start()
                else:
                    @pl.when(z == n_z - 1)
                    def _():
                        up_copy(g, d, 0, part).start()

                    for plane, at in {5: ((5, 1), (6, 2)), 6: ((6, 3),), 7: ()}[d]:
                        @pl.when(z == plane)
                        def _():
                            up_copy(g, d, at, part).start()

    def wait_fetch(g):
        landed(g, 0, z, None)
        for step in range(1, 5):
            each_piece(g, step, landed)

    relay_and_pick(1, 1)
    relay_and_pick(1, 2)
    loads[2].wait()
    loads[3].wait()
    wait_fetch(0)
    attention(
        0,
        {
            0: functools.partial(relay_and_pick, 1, 3),
            2: functools.partial(relay_and_pick, 1, 4),
            4: relay_x,
        },
    )
    give_back(0)
    wait_fetch(1)
    attention(1, {2 + i: functools.partial(collect, 0, RETURN_ORDER[i]) for i in range(3)})
    give_back(1)
    out_q = pltpu.make_async_copy(m["qg"], query_grad, m["out_sem"].at[0])
    out_q.start()
    def c_copy(g, i):
        return pltpu.make_async_remote_copy(
            src_ref=m["wpart"].at[g, i, 1 - c],
            dst_ref=m["crecv"].at[g, i],
            send_sem=m["sent"].at[5],
            recv_sem=m["c_recv"].at[g, i],
            device_id={"kv": z * PLANE + y * N_C + (1 - c)},
            device_id_type=MESH,
        )

    def wy_copy(g, part, r):
        to = (y + r) % N_Y
        return pltpu.make_async_remote_copy(
            src_ref=m["wy"].at[g, part, r],
            dst_ref=m["wyr"].at[g, part, r],
            send_sem=m["sent"].at[6],
            recv_sem=m["wy_recv"].at[g, part, r - 1],
            device_id={"kv": z * PLANE + to * N_C + c},
            device_id_type=MESH,
        )

    half = inputs.shape[1] // 2

    def combine(g):
        for b in range(n_b):
            total = m["acc"][g, b] + m["own_tot"][g, b]
            m["acc"][g, b] = total
            m["kg"][b * BLOCK : (b + 1) * BLOCK, :] = total.astype(BF16)
        m["kg_t"][...] = m["kg"][...].T

    def own_terms(g, i):
        w_t = [
            lax.dot_general(
                m["kg_t"][:HD, :], m["xraw"][i, :, h * half : (h + 1) * half],
                (((1,), (0,)), ((), ())), preferred_element_type=F32,
            )
            for h in range(2)
        ]
        w = jnp.concatenate(w_t, axis=0).T.astype(BF16)
        for yy in range(N_Y):
            for cc in range(N_C):
                first = (yy * N_C + cc) * BLOCK
                m["wpart"][g, i, cc, yy] = w[first : first + BLOCK]

    def core_sum(g, i):
        c_copy(g, i).wait_recv()
        for r in range(N_Y):
            yy = (y + r) % N_Y
            both = m["wpart"][g, i, c, yy].astype(F32) + m["crecv"][g, i, yy].astype(F32)
            if r:
                m["wy"][g, i // 2, r, i % 2] = both.astype(BF16)
            else:
                m["wy_own"][g, i] = both
        if i % 2:
            for r in (2, 1, 3):
                wy_copy(g, i // 2, r).start()

    def terms_out(g):
        combine(g)
        for i in range(n_x):
            own_terms(g, i)
            if i:
                c_copy(g, i - 1).start()
        c_copy(g, n_x - 1).start()

    for g, d in [
        (0, 2), (1, 4), (0, 6), (1, 5), (0, 1), (1, 3), (0, 7), (1, 6), (1, 2), (0, 0)
    ]:
        collect(g, d)
    x_copy(True, 1, 1).wait_recv()
    x_copy(False, 1, 0).wait_recv()
    x_copy(True, 2, 0).wait_recv()
    x_copy(False, 2, 1).wait_recv()
    loads[5].wait()
    terms_out(0)
    collect(1, 7)
    for i in range(n_x):
        core_sum(0, i)
    collect(1, 1)
    collect(1, 0)
    combine(1)
    lag = 2
    for i in range(n_x + lag):
        if i < n_x:
            own_terms(1, i)
        if 0 < i <= n_x:
            c_copy(1, i - 1).start()
        if i >= lag:
            core_sum(1, i - lag)
    for b in range(n_b):
        rows = slice(b * BLOCK, (b + 1) * BLOCK)
        t0, t1 = m["acc"][0, b], m["acc"][1, b]
        key_grad[rows, :] = jnp.where(low, t0, pltpu.roll(t1, HD, 1))
        value_grad[rows, :] = jnp.where(low, pltpu.roll(t0, HD, 1), t1)

    def z_of(i):
        return 2 * ((x + n_x - i // 2) % n_x) + i % 2

    def wz_copy(i):
        return pltpu.make_async_remote_copy(
            src_ref=m["wz"].at[i],
            dst_ref=m["wzr"].at[z],
            send_sem=m["sent"].at[7],
            recv_sem=m["wz_recv"].at[z],
            device_id={"kv": z_of(i) * PLANE + q},
            device_id_type=MESH,
        )

    def sent(g, order, z_from, ref):
        wait_group(m["picked"].at[g, order, others], m["sent"].at[2])

    for g in range(2):
        for way in range(2):
            for step in range(1, steps(way) + 1):
                @pl.when(sends(way, step))
                def _():
                    for part in range(PARTS):
                        z_copy(g, way, step, part).wait_send()

        sent(g, 0, z, None)
        for step in range(1, 5):
            each_piece(g, step, sent)
        for d in range(8):
            @pl.when(z - d >= 0)
            def _():
                wait_group(m["back"].at[g, d, others], m["sent"].at[3])

            for part in range(ROW_PARTS):
                if 0 < d < 5:
                    @pl.when(z - d >= 0)
                    def _():
                        dn_copy(g, d, part).wait_send()
                elif d:
                    @pl.when(z - d >= 0)
                    def _():
                        up_copy(g, d, 0, part).wait_send()

    for part in range(2):
        x_copy(True, 1, part).wait_send()
        x_copy(False, 1, part).wait_send()
    x_copy(True, 2, 0).wait_send()
    x_copy(False, 2, 1).wait_send()
    for g in range(2):
        for i in range(n_x):
            c_copy(g, i).wait_send()
    out_q.wait()

    for g, part in ((0, 0), (0, 1), (1, 0), (1, 1)):
        for r in (1, 3, 2):
            wy_copy(g, part, r).wait_recv()
        if g == 0:
            continue
        for i in (2 * part, 2 * part + 1):
            total = []
            for h in range(2):
                total.append(m["wy_own"][h, i])
                for r in range(1, N_Y):
                    total[h] = total[h] + m["wyr"][h, part, r, i % 2].astype(F32)
            tiles = [
                jnp.where(low, total[0], pltpu.roll(total[1], HD, 1)),
                jnp.where(low, pltpu.roll(total[0], HD, 1), total[1]),
            ]
            for h in range(2):
                m["wz_own"][2 * i + h] = tiles[h]
                m["wz"][2 * i + h] = tiles[h].astype(BF16)
        for i in range(4 * part, 4 * part + 4):
            @pl.when(z_of(i) != z)
            def _():
                wz_copy(i).start()
    for g in range(2):
        for part in range(2):
            for r in range(1, N_Y):
                wy_copy(g, part, r).wait_send()
    mine = 2 * ((x + n_x - z // 2) % n_x) + z % 2
    total = m["wz_own"][mine]
    for r in range(1, n_z):
        frm = (z + r) % n_z
        pltpu.make_async_remote_copy(
            src_ref=m["wz"].at[0],
            dst_ref=m["wzr"].at[frm],
            send_sem=m["sent"].at[7],
            recv_sem=m["wz_recv"].at[frm],
            device_id={"kv": frm * PLANE + q},
            device_id_type=MESH,
        ).wait_recv()
        total = total + m["wzr"][frm].astype(F32)
    weight_grad[...] = total
    for i in range(n_z):
        @pl.when(z_of(i) != z)
        def _():
            wz_copy(i).wait_send()


def put_kernel(q_src, k_src, v_src, w_src, q_dst, k_dst, v_dst, w_dst, q_mid, sem):
    rows = q_mid.shape[0] // 3
    part = [pl.ds(i * rows, rows) for i in range(3)]
    into = [
        pltpu.make_async_copy(q_src.at[part[i]], q_mid.at[part[i]], sem.at[i]) for i in range(3)
    ]
    rest = [
        pltpu.make_async_copy(src, dst, sem.at[3 + i])
        for i, (src, dst) in enumerate([(k_src, k_dst), (v_src, v_dst), (w_src, w_dst)])
    ]
    out = [
        pltpu.make_async_copy(q_mid.at[part[i]], q_dst.at[part[i]], sem.at[6 + i]) for i in range(3)
    ]
    for copy in into + rest:
        copy.start()
    for i in range(3):
        into[i].wait()
        out[i].start()
    for copy in rest + out:
        copy.wait()


def put_out(query_grad, key_grad, value_grad, weight_grad):
    hbm = pl.BlockSpec(memory_space=pltpu.HBM)
    vm = pl.BlockSpec(memory_space=pltpu.VMEM)
    arrays = (query_grad, key_grad, value_grad, weight_grad)
    return pl.pallas_call(
        put_kernel,
        out_shape=tuple(jax.ShapeDtypeStruct(a.shape, a.dtype) for a in arrays),
        in_specs=[hbm, vm, vm, vm],
        out_specs=(hbm,) * 4,
        scratch_shapes=[pltpu.VMEM(query_grad.shape, F32), pltpu.SemaphoreType.DMA((9,))],
        compiler_params=pltpu.CompilerParams(vmem_limit_bytes=int(53.4 * 1024 * 1024)),
        name="put_out",
    )(*arrays)


def index_kernel(n_dev, n_b, place_of, lists, out, flat):
    z, q = place_of()
    me = z * PLANE + q
    n_list = lists.shape[1]
    n_z = n_dev // PLANE
    width = lists.shape[2]
    heads = []
    for g in range(2):
        near = pltpu.roll(lists[g], (width - z * PLANE * n_b) % width, 1)[:, :128]
        heads.append(near)
        for plane in range(n_z):
            offs = near - (plane * PLANE + q) * n_b
            offs = jnp.where((offs >= 0) & (offs < n_b), offs, 0)
            out[24 + g * n_z + plane : 25 + g * n_z + plane, :] = offs.max(axis=0, keepdims=True)
    best = out[24 : 24 + 2 * n_z, :]
    widest = best
    for k in range(1, n_b):
        widest = jnp.maximum(widest, pltpu.roll(best, 128 - k, 1))
    out[24 : 24 + 2 * n_z, :] = widest
    both = pltpu.roll(jnp.concatenate(heads, axis=0), (128 - q * n_b) % 128, 1)
    flat[...] = jnp.zeros((128, 128), jnp.int32)
    flat[: 2 * n_list, :] = both
    entry = flat[...].T[:8, :]
    block = lax.broadcasted_iota(jnp.int32, (8, 128), 0)
    lane = lax.broadcasted_iota(jnp.int32, (8, 128), 1)
    owner = jnp.floor((entry.astype(F32) + 0.5) * (1.0 / n_b)).astype(jnp.int32)
    slot = jnp.where(owner == me, n_dev + entry - owner * n_b, jnp.maximum(owner, 0))
    kind = jnp.where(entry < 0, 2, jnp.where(entry == me * n_b + block, 1, 0))
    out[:8, :] = jnp.where(lane < 2 * n_list, slot, pltpu.roll(kind, 2 * n_list, 1))
    used = jnp.where(entry < 0, -1, slot)
    for g in range(2):
        found = jnp.full((8, 128), n_list, jnp.int32)
        for n in range(n_list):
            at = g * n_list + n
            found = jnp.where(used[:, at : at + 1] == lane, n, found)
        out[8 + 8 * g : 16 + 8 * g, :] = found


def index_table(chosen, n_b, n_dev, place_of=place, interpret=False):
    vm = pl.BlockSpec(memory_space=pltpu.VMEM)
    return pl.pallas_call(
        functools.partial(index_kernel, n_dev, n_b, place_of),
        out_shape=jax.ShapeDtypeStruct((24 + 2 * n_dev // PLANE, 128), jnp.int32),
        in_specs=[vm],
        out_specs=vm,
        scratch_shapes=[pltpu.VMEM((128, 128), jnp.int32)],
        compiler_params=pltpu.CompilerParams(vmem_limit_bytes=4 * 1024 * 1024),
        name="index",
        interpret=interpret,
    )(chosen.transpose(0, 2, 1))


def local(queries, key_heads, values, log_sums, out_grad, inputs, chosen):
    n_dev = lax.axis_size("kv")
    n_x = lax.axis_size("tp")
    rows, feats = inputs.shape
    n_b = rows // BLOCK
    heads = log_sums.shape[0]
    n_list = chosen.shape[2]
    idx = index_table(chosen, n_b, n_dev)
    scratch = scratch_list(rows, n_dev, n_x, n_list, feats, heads)
    hbm = pl.BlockSpec(memory_space=pltpu.HBM)
    vm = pl.BlockSpec(memory_space=pltpu.VMEM)
    results = pl.pallas_call(
        functools.partial(
            fused_kernel, [name for name, _ in scratch], n_dev // PLANE, n_x, n_list
        ),
        out_shape=(
            jax.ShapeDtypeStruct(queries.shape, F32),
            jax.ShapeDtypeStruct(key_heads.shape, F32),
            jax.ShapeDtypeStruct(values.shape, F32),
            jax.ShapeDtypeStruct((feats * n_x // n_dev, 128), F32),
        ),
        in_specs=[pl.BlockSpec(memory_space=pltpu.SMEM)] + [hbm] * 6,
        out_specs=(hbm, vm, vm, vm),
        scratch_shapes=[kind for _, kind in scratch],
        compiler_params=pltpu.CompilerParams(
            collective_id=0, has_side_effects=True, vmem_limit_bytes=53 * 1024 * 1024
        ),
        name="fused",
    )(
        idx,
        key_heads.reshape(n_b, BLOCK, -1),
        values.reshape(n_b, BLOCK, -1),
        queries,
        out_grad,
        log_sums,
        inputs,
    )
    return put_out(*results)


def solution(mesh):
    placed = (
        P("kv", "tp"),
        P("kv", "tp"),
        P("kv", "tp"),
        P("tp", "kv"),
        P("kv", "tp"),
        P("kv", "tp"),
        P("tp", None, None),
    )
    return jax.shard_map(
        local,
        mesh=mesh,
        in_specs=placed,
        out_specs=(P("kv", "tp"), P("kv", "tp"), P("kv", "tp"), P("kv", "tp")),
        check_vma=False,
    )
```

```python
import functools

import jax
import jax.numpy as jnp
from jax import lax
from jax.experimental import pallas as pl
from jax.experimental.pallas import tpu as pltpu
from jax.sharding import PartitionSpec as P

HD = 64
BLOCK = 64
NEG = -1e30
LOG2E = 1.4426950408889634
CHUNK = 8
PARTS = 3
ROW_PARTS = 4
PART_ROWS = BLOCK // ROW_PARTS
N_Y = 4
N_C = 2
PLANE = N_Y * N_C
MESH = pl.DeviceIdType.MESH
RETURN_ORDER = (4, 5, 3, 6, 2, 7, 1, 0)
F32, BF16 = jnp.float32, jnp.bfloat16


def place():
    me = lax.axis_index("kv")
    return me // PLANE, me % PLANE


def scratch_list(rows, n_dev, n_x, n_list, feats, heads):
    n_b = rows // BLOCK
    tile = (BLOCK, 128)
    cols = heads // 2 * BLOCK
    dma = pltpu.SemaphoreType.DMA
    out = [
        ("kraw", pltpu.VMEM((n_b,) + tile, BF16)),
        ("vraw", pltpu.VMEM((n_b,) + tile, BF16)),
        ("qraw", pltpu.VMEM((rows, heads * HD), BF16)),
        ("graw", pltpu.VMEM((rows, heads * HD), BF16)),
        ("lraw", pltpu.VMEM((heads, rows), F32)),
        ("xraw", pltpu.VMEM((n_x, rows, feats), BF16)),
        ("lse", pltpu.VMEM((n_b * 2, 1, cols), F32)),
        ("bias", pltpu.VMEM((3,) + (BLOCK, cols), F32)),
        ("shift", pltpu.VMEM((3,) + (BLOCK, cols), F32)),
        ("qg", pltpu.VMEM((rows, heads * HD), F32)),
        ("picked", pltpu.VMEM((2, 8, PLANE) + tile, BF16)),
        ("qd", pltpu.VMEM((2 * cols, 128), BF16)),
        ("cat", pltpu.VMEM((n_list,) + tile, BF16)),
        ("sdp", pltpu.VMEM((n_list, BLOCK, 2 * cols), F32)),
        ("pd", pltpu.VMEM((n_list, BLOCK, 2 * cols), BF16)),
        ("terms", pltpu.VMEM((n_b, n_list + 1) + tile, F32)),
        ("ret", pltpu.VMEM((2, n_dev) + tile, BF16)),
        ("own_tot", pltpu.VMEM((2, n_b) + tile, F32)),
        ("back", pltpu.VMEM((2, 8, PLANE) + tile, BF16)),
        ("acc", pltpu.VMEM((2, n_b) + tile, F32)),
        ("zs", pltpu.VMEM((2, 8, ROW_PARTS, n_b, PART_ROWS, 128), BF16)),
        ("zr_dn", pltpu.VMEM((2, 4, ROW_PARTS, n_b, PART_ROWS, 128), BF16)),
        ("zr_up", pltpu.VMEM((2, 4, ROW_PARTS, n_b, PART_ROWS, 128), BF16)),
        ("kg", pltpu.VMEM((rows, 128), BF16)),
        ("kg_t", pltpu.VMEM((128, rows), BF16)),
        ("wpart", pltpu.VMEM((2, n_x, N_C, N_Y) + tile, BF16)),
        ("crecv", pltpu.VMEM((2, n_x, N_Y) + tile, BF16)),
        ("wy", pltpu.VMEM((2, 2, N_Y, n_x // 2) + tile, BF16)),
        ("wy_own", pltpu.VMEM((2, n_x) + tile, F32)),
        ("wyr", pltpu.VMEM((2, 2, N_Y, n_x // 2) + tile, BF16)),
        ("wz", pltpu.VMEM((8,) + tile, BF16)),
        ("wz_own", pltpu.VMEM((8,) + tile, F32)),
        ("wzr", pltpu.VMEM((8,) + tile, BF16)),
        ("in_sem", dma((6,))),
        ("out_sem", dma((1,))),
        ("sent", dma((8,))),
        ("z_recv", dma((2, 7, PARTS))),
        ("y_recv", dma((2, 8))),
        ("x_recv", dma((2, 3))),
        ("b_recv", dma((2, 8))),
        ("r_recv_dn", dma((2, 4, ROW_PARTS))),
        ("r_recv_up", dma((2, 4, ROW_PARTS))),
        ("c_recv", dma((2, n_x))),
        ("wy_recv", dma((2, 2, N_Y - 1))),
        ("wz_recv", dma((8,))),
    ]
    for g in range(2):
        out.append((f"own{g}", pltpu.VMEM((n_b,) + tile, BF16)))
        out.append((f"tab{g}", pltpu.VMEM((n_dev + n_b,) + tile, BF16)))
        for step in range(1, 5):
            out.append((f"held{g}0{step}", pltpu.VMEM((n_b,) + tile, BF16)))
        for step in range(1, 4):
            out.append((f"held{g}1{step}", pltpu.VMEM((n_b,) + tile, BF16)))
    return out


def fused_kernel(names, n_z, n_x, n_list, *refs):
    idx, keys, vals, queries, out_grad, log_sums, inputs = refs[:7]
    query_grad, key_grad, value_grad, weight_grad = refs[7:11]
    m = dict(zip(names, refs[11:]))
    n_b = m["kraw"].shape[0]
    n_dev = n_z * PLANE
    heads = m["lraw"].shape[0]
    per_group = heads // 2
    cols = per_group * BLOCK
    z, q = place()
    y, c = q // N_C, q % N_C
    x = lax.axis_index("tp")

    barrier = pltpu.get_barrier_semaphore()
    partners = [{"kv": (z + r) % n_z * PLANE + q} for r in range(1, n_z)]
    partners += [{"kv": z * PLANE + (q + r) % PLANE} for r in range(1, PLANE)]
    right, left = {"tp": (x + 1) % n_x}, {"tp": (x + n_x - 1) % n_x}
    partners += [right, left]
    for who in partners:
        pl.semaphore_signal(barrier, inc=1, device_id=who, device_id_type=MESH)

    loads = [
        pltpu.make_async_copy(src, dst, m["in_sem"].at[i])
        for i, (src, dst) in enumerate(
            [
                (keys, m["kraw"]),
                (vals, m["vraw"]),
                (queries, m["qraw"]),
                (out_grad, m["graw"]),
                (log_sums, m["lraw"]),
                (inputs, m["xraw"].at[0]),
            ]
        )
    ]
    for copy in loads:
        copy.start()
    up_z = {"kv": (z + 1) % n_z * PLANE + q}
    dn_z = {"kv": (z + n_z - 1) % n_z * PLANE + q}
    lane = lax.broadcasted_iota(jnp.int32, (BLOCK, 128), 1)
    low = lane < HD
    loads[0].wait()
    loads[1].wait()
    for b in range(n_b):
        k = m["kraw"][b].astype(F32)
        v = m["vraw"][b].astype(F32)
        kv0 = jnp.where(low, k, pltpu.roll(v, HD, 1)).astype(BF16)
        kv1 = jnp.where(low, pltpu.roll(k, HD, 1), v).astype(BF16)
        m["own0"][b] = kv0
        m["own1"][b] = kv1
        m["tab0"][n_dev + b] = kv0
        m["tab1"][n_dev + b] = kv1
    pl.semaphore_wait(barrier, len(partners))

    def held(g, way, step):
        return m[f"own{g}"] if step == 0 else m[f"held{g}{way}{step}"]

    def z_copy(g, way, step, part):
        blocks = pl.ds(part * (n_b // PARTS), n_b // PARTS)
        return pltpu.make_async_remote_copy(
            src_ref=held(g, way, step - 1).at[blocks],
            dst_ref=held(g, way, step).at[blocks],
            send_sem=m["sent"].at[0],
            recv_sem=m["z_recv"].at[g, way * 4 + step - 1, part],
            device_id=dn_z if way else up_z,
            device_id_type=MESH,
        )

    def sends(way, step):
        if way:
            return (z + step - 1) % n_z < 3
        return (z < n_z - 1) & (z - step + 1 >= 0)

    def gets(way, step):
        if way:
            return (z + step) % n_z < 3
        return z - step >= 0

    def steps(way):
        return 3 if way else 4

    def x_copy(to_right, rel, part):
        half = inputs.shape[0] // 2
        rows = pl.ds(part * half, half)
        slot = rel if to_right else n_x - rel
        if rel == 1:
            src = inputs.at[rows]
        else:
            src = m["xraw"].at[1 if to_right else n_x - 1, rows]
        side = 0 if to_right else 1
        return pltpu.make_async_remote_copy(
            src_ref=src,
            dst_ref=m["xraw"].at[slot, rows],
            send_sem=m["sent"].at[1],
            recv_sem=m["x_recv"].at[side, 2 if rel == 2 else part],
            device_id=right if to_right else left,
            device_id_type=MESH,
        )

    def y_copy(g, order, z_from, r):
        to = (q + r) % PLANE
        return pltpu.make_async_remote_copy(
            src_ref=m["picked"].at[g, order, r],
            dst_ref=m[f"tab{g}"].at[z_from * PLANE + q],
            send_sem=m["sent"].at[2],
            recv_sem=m["y_recv"].at[g, order],
            device_id={"kv": z * PLANE + to},
            device_id_type=MESH,
        )

    others = pl.ds(1, PLANE - 1)

    def wait_group(ref, sem):
        pltpu.make_async_copy(ref, ref, sem).wait()

    def pick(g, order, z_from, ref):
        def one(r, carry):
            to = (q + r) % PLANE
            m["picked"][g, order, r] = ref[idx[24 + g * n_z + z_from, to * n_b]]

            @pl.when(r > 1)
            def _():
                y_copy(g, order, z_from, r - 1).start()

            return carry

        lax.fori_loop(1, PLANE, one, 0)
        m[f"tab{g}"][z_from * PLANE + q] = ref[idx[24 + g * n_z + z_from, q * n_b]]
        y_copy(g, order, z_from, PLANE - 1).start()

    def each_piece(g, step, act):
        @pl.when(gets(0, step))
        def _():
            act(g, step, z - step, held(g, 0, step))

        if step < 4:
            @pl.when(gets(1, step) & (z + step >= n_z))
            def _():
                act(g, 4 + step, z + step - n_z, held(g, 1, step))

    def set_out(g):
        for part in range(PARTS):
            for way in range(2):
                @pl.when(sends(way, 1))
                def _():
                    z_copy(g, way, 1, part).start()

    set_out(0)
    for part in range(2):
        x_copy(True, 1, part).start()
        x_copy(False, 1, 1 - part).start()
    pick(0, 0, z, m["own0"])
    pick(1, 0, z, m["own1"])

    def relay(g, step):
        for part in range(PARTS):
            for way in range(2):
                if step <= steps(way):
                    @pl.when(gets(way, step))
                    def _():
                        z_copy(g, way, step, part).wait_recv()

                if step + 1 <= steps(way):
                    @pl.when(sends(way, step + 1))
                    def _():
                        z_copy(g, way, step + 1, part).start()

    key_at = lax.broadcasted_iota(jnp.int32, (BLOCK, cols), 0)
    tok_at = lax.broadcasted_iota(jnp.int32, (BLOCK, cols), 1) % BLOCK
    m["bias"][0] = jnp.zeros((BLOCK, cols), F32)
    m["bias"][1] = jnp.where(key_at <= tok_at, 0.0, NEG)
    m["bias"][2] = jnp.full((BLOCK, cols), NEG, F32)
    for p in range(n_b):
        m["terms"][p, n_list] = jnp.zeros((BLOCK, 128), F32)
    loads[4].wait()
    for p in range(n_b):
        for g in range(2):
            row = [
                m["lraw"][g * per_group + r : g * per_group + r + 1, p * BLOCK : (p + 1) * BLOCK]
                for r in range(per_group)
            ]
            m["lse"][p * 2 + g] = jnp.concatenate(row, axis=1)

    for step in range(1, 5):
        relay(0, step)
        if step == 2:
            set_out(1)
        each_piece(0, step, pick)

    def relay_and_pick(g, step):
        relay(g, step)
        each_piece(g, step, pick)

    def relay_x():
        x_copy(True, 1, 0).wait_recv()
        x_copy(True, 2, 0).start()
        x_copy(False, 1, 1).wait_recv()
        x_copy(False, 2, 1).start()

    def landed(g, order, z_from, ref):
        wait_group(m["picked"].at[g, order, others], m["y_recv"].at[g, order])

    def masked_rows(ref, row, g, factor, side):
        parts = []
        for r in range(per_group):
            col = (g * per_group + r) * HD
            part = ref[pl.ds(row, BLOCK), col // 128 * 128 : col // 128 * 128 + 128]
            part = part.astype(F32) * factor
            if r % 2 != side:
                part = pltpu.roll(part, HD, 1)
            parts.append(jnp.where(low != (side == 1), part, 0.0).astype(BF16))
        return parts

    def attention(g, between):
        tab = m[f"tab{g}"]
        sdp, pd, qd, cat, shift = m["sdp"], m["pd"], m["qd"], m["cat"], m["shift"]
        chunks = [slice(n, n + CHUNK) for n in range(0, n_list, CHUNK)]
        nt = (((1,), (1,)), ((), ()))
        nn = (((1,), (0,)), ((), ()))

        def one_position(p, carry):
            row = pl.multiple_of(p * BLOCK, BLOCK)
            for r, part in enumerate(masked_rows(m["qraw"], row, g, HD ** -0.5, 0)):
                qd[r * BLOCK : (r + 1) * BLOCK, :] = part
            for r, part in enumerate(masked_rows(m["graw"], row, g, 1.0, 1)):
                qd[cols + r * BLOCK : cols + (r + 1) * BLOCK, :] = part
            for n in range(n_list):
                cat[n] = tab[idx[p, g * n_list + n]]
            for kind in range(3):
                shift[kind] = m["bias"][kind] - m["lse"][p * 2 + g] * LOG2E

            acc = jnp.zeros((8, cols), F32)
            for ch in chunks:
                both = lax.dot_general(
                    cat[ch].reshape(CHUNK * BLOCK, 128), qd[...], nt, preferred_element_type=F32
                ).reshape(CHUNK, BLOCK, 2 * cols)
                for n in range(ch.start, ch.stop):
                    prod = both[n - ch.start]
                    pr = jnp.exp2(prod[:, :cols] * LOG2E + shift[idx[p, (2 + g) * n_list + n]])
                    sdp[n, :, :cols] = pr
                    sdp[n, :, cols:] = prod[:, cols:]
                    pd[n, :, cols:] = pr.astype(BF16)
                    pr = pr * prod[:, cols:]
                    acc = acc + pr.reshape(BLOCK // 8, 8, cols).sum(axis=0)
            delta = acc.sum(axis=0, keepdims=True)
            for ch in chunks:
                for n in range(ch.start, ch.stop):
                    ds = sdp[n, :, :cols] * (sdp[n, :, cols:] - delta)
                    pd[n, :, :cols] = ds.astype(BF16)
                m["terms"][p, ch] = lax.dot_general(
                    pd[ch].reshape(CHUNK * BLOCK, 2 * cols), qd[...], nn, preferred_element_type=F32
                ).reshape(CHUNK, BLOCK, 128)
            dq_t = lax.dot_general(
                cat[...].reshape(n_list * BLOCK, 128),
                pd[:, :, :cols].reshape(n_list * BLOCK, cols),
                (((0,), (0,)), ((), ())),
                preferred_element_type=F32,
            )
            dq = dq_t.T * (HD ** -0.5)
            for pair in range(per_group // 2):
                even = dq[(2 * pair) * BLOCK : (2 * pair + 1) * BLOCK]
                odd = dq[(2 * pair + 1) * BLOCK : (2 * pair + 2) * BLOCK]
                col = g * per_group * HD + pair * 128
                m["qg"][pl.ds(row, BLOCK), col : col + 128] = jnp.where(
                    low, even, pltpu.roll(odd, HD, 1)
                )
            for at, act in between.items():
                @pl.when(p == at)
                def _():
                    act()

            return carry

        lax.fori_loop(0, n_b, one_position, 0)

    def summed_terms(g, j):
        total = m["terms"][0, idx[8 + 8 * g, j]]
        for p in range(1, n_b):
            total = total + m["terms"][p, idx[8 + 8 * g + p, j]]
        return total

    def b_copy(g, d, r):
        to = (q + r) % PLANE
        return pltpu.make_async_remote_copy(
            src_ref=m["ret"].at[g, (z - d) * PLANE + to],
            dst_ref=m["back"].at[g, d, q],
            send_sem=m["sent"].at[3],
            recv_sem=m["b_recv"].at[g, d],
            device_id={"kv": z * PLANE + to},
            device_id_type=MESH,
        )

    def give_back(g):
        for d in RETURN_ORDER:
            @pl.when(z - d >= 0)
            def _():
                for r in list(range(1, PLANE)) + [0]:
                    j = (z - d) * PLANE + (q + r) % PLANE
                    m["ret"][g, j] = summed_terms(g, j).astype(BF16)
                for r in range(1, PLANE):
                    b_copy(g, d, r).start()

        def own(b, carry):
            m["own_tot"][g, b] = summed_terms(g, n_dev + b)
            return carry

        lax.fori_loop(0, n_b, own, 0)

    def accumulate(g, d, part):
        rows = slice(part * PART_ROWS, (part + 1) * PART_ROWS)
        accs = [jnp.zeros((PART_ROWS, 128), F32) for _ in range(n_b)]
        for r in range(PLANE):
            frm = (q + r) % PLANE
            if r == 0:
                val = m["ret"][g, (z - d) * PLANE + q, rows, :]
            else:
                val = m["back"][g, d, frm, rows, :]
            val = val.astype(F32)
            block = idx[24 + g * n_z + z - d, frm * n_b]
            for b in range(n_b):
                accs[b] = accs[b] + jnp.where(block == b, val, 0.0)
        for b in range(n_b):
            m["acc"][g, b, rows, :] = accs[b]

    def dn_copy(g, d, part):
        return pltpu.make_async_remote_copy(
            src_ref=m["zs"].at[g, d, part],
            dst_ref=m["zr_dn"].at[g, d - 1, part],
            send_sem=m["sent"].at[4],
            recv_sem=m["r_recv_dn"].at[g, d - 1, part],
            device_id=dn_z,
            device_id_type=MESH,
        )

    def up_copy(g, d, at, part):
        to = n_z - 1 if at else n_z - 1 - d
        return pltpu.make_async_remote_copy(
            src_ref=m["zs"].at[g, d, part],
            dst_ref=m["zr_up"].at[g, at, part],
            send_sem=m["sent"].at[4],
            recv_sem=m["r_recv_up"].at[g, at, part],
            device_id={"kv": to * PLANE + q},
            device_id_type=MESH,
        )

    def add_arrival(g, copy, ref, part):
        copy.wait_recv()
        rows = slice(part * PART_ROWS, (part + 1) * PART_ROWS)
        for b in range(n_b):
            m["acc"][g, b, rows, :] += ref[b].astype(F32)

    def dn_arrival(g, d, part):
        @pl.when(z < n_z - 1)
        def _():
            add_arrival(g, dn_copy(g, d, part), m["zr_dn"].at[g, d - 1, part], part)

    def up_arrival(g, at, part):
        add_arrival(g, up_copy(g, 5, at, part), m["zr_up"].at[g, at, part], part)

    def store_out(g, d, part):
        rows = slice(part * PART_ROWS, (part + 1) * PART_ROWS)
        for b in range(n_b):
            m["zs"][g, d, part, b] = m["acc"][g, b, rows, :].astype(BF16)

    def collect(g, d):
        @pl.when(z - d >= 0)
        def _():
            wait_group(m["back"].at[g, d, others], m["b_recv"].at[g, d])
            for part in range(ROW_PARTS):
                accumulate(g, d, part)
                if d < 4:
                    dn_arrival(g, d + 1, part)
                if d in (6, 7):
                    @pl.when(z == n_z - 1)
                    def _():
                        for at in {6: (2,), 7: (1, 3)}[d]:
                            up_arrival(g, at, part)

                if d == 0:
                    @pl.when(z < 3)
                    def _():
                        up_arrival(g, 0, part)
                    continue
                store_out(g, d, part)
                if d < 5:
                    dn_copy(g, d, part).start()
                else:
                    @pl.when(z == n_z - 1)
                    def _():
                        up_copy(g, d, 0, part).start()

                    for plane, at in {5: ((5, 1), (6, 2)), 6: ((6, 3),), 7: ()}[d]:
                        @pl.when(z == plane)
                        def _():
                            up_copy(g, d, at, part).start()

    def wait_fetch(g):
        landed(g, 0, z, None)
        for step in range(1, 5):
            each_piece(g, step, landed)

    relay_and_pick(1, 1)
    relay_and_pick(1, 2)
    loads[2].wait()
    loads[3].wait()
    wait_fetch(0)
    attention(
        0,
        {
            0: functools.partial(relay_and_pick, 1, 3),
            2: functools.partial(relay_and_pick, 1, 4),
            4: relay_x,
        },
    )
    give_back(0)
    wait_fetch(1)
    attention(1, {2 + i: functools.partial(collect, 0, RETURN_ORDER[i]) for i in range(3)})
    give_back(1)
    out_q = pltpu.make_async_copy(m["qg"], query_grad, m["out_sem"].at[0])
    out_q.start()
    def c_copy(g, i):
        return pltpu.make_async_remote_copy(
            src_ref=m["wpart"].at[g, i, 1 - c],
            dst_ref=m["crecv"].at[g, i],
            send_sem=m["sent"].at[5],
            recv_sem=m["c_recv"].at[g, i],
            device_id={"kv": z * PLANE + y * N_C + (1 - c)},
            device_id_type=MESH,
        )

    def wy_copy(g, part, r):
        to = (y + r) % N_Y
        return pltpu.make_async_remote_copy(
            src_ref=m["wy"].at[g, part, r],
            dst_ref=m["wyr"].at[g, part, r],
            send_sem=m["sent"].at[6],
            recv_sem=m["wy_recv"].at[g, part, r - 1],
            device_id={"kv": z * PLANE + to * N_C + c},
            device_id_type=MESH,
        )

    half = inputs.shape[1] // 2

    def combine(g):
        for b in range(n_b):
            total = m["acc"][g, b] + m["own_tot"][g, b]
            m["acc"][g, b] = total
            m["kg"][b * BLOCK : (b + 1) * BLOCK, :] = total.astype(BF16)
        m["kg_t"][...] = m["kg"][...].T

    def own_terms(g, i):
        w_t = [
            lax.dot_general(
                m["kg_t"][:HD, :], m["xraw"][i, :, h * half : (h + 1) * half],
                (((1,), (0,)), ((), ())), preferred_element_type=F32,
            )
            for h in range(2)
        ]
        w = jnp.concatenate(w_t, axis=0).T.astype(BF16)
        for yy in range(N_Y):
            for cc in range(N_C):
                first = (yy * N_C + cc) * BLOCK
                m["wpart"][g, i, cc, yy] = w[first : first + BLOCK]

    def core_sum(g, i):
        c_copy(g, i).wait_recv()
        for r in range(N_Y):
            yy = (y + r) % N_Y
            both = m["wpart"][g, i, c, yy].astype(F32) + m["crecv"][g, i, yy].astype(F32)
            if r:
                m["wy"][g, i // 2, r, i % 2] = both.astype(BF16)
            else:
                m["wy_own"][g, i] = both
        if i % 2:
            for r in (2, 1, 3):
                wy_copy(g, i // 2, r).start()

    def terms_out(g):
        combine(g)
        for i in range(n_x):
            own_terms(g, i)
            if i:
                c_copy(g, i - 1).start()
        c_copy(g, n_x - 1).start()

    for g, d in [
        (0, 2), (1, 4), (0, 6), (1, 5), (0, 1), (1, 3), (0, 7), (1, 6), (1, 2), (0, 0)
    ]:
        collect(g, d)
    x_copy(True, 1, 1).wait_recv()
    x_copy(False, 1, 0).wait_recv()
    x_copy(True, 2, 0).wait_recv()
    x_copy(False, 2, 1).wait_recv()
    loads[5].wait()
    terms_out(0)
    collect(1, 7)
    for i in range(n_x):
        core_sum(0, i)
    collect(1, 1)
    collect(1, 0)
    combine(1)
    lag = 2
    for i in range(n_x + lag):
        if i < n_x:
            own_terms(1, i)
        if 0 < i <= n_x:
            c_copy(1, i - 1).start()
        if i >= lag:
            core_sum(1, i - lag)
    for b in range(n_b):
        rows = slice(b * BLOCK, (b + 1) * BLOCK)
        t0, t1 = m["acc"][0, b], m["acc"][1, b]
        key_grad[rows, :] = jnp.where(low, t0, pltpu.roll(t1, HD, 1))
        value_grad[rows, :] = jnp.where(low, pltpu.roll(t0, HD, 1), t1)

    def z_of(i):
        return 2 * ((x + n_x - i // 2) % n_x) + i % 2

    def wz_copy(i):
        return pltpu.make_async_remote_copy(
            src_ref=m["wz"].at[i],
            dst_ref=m["wzr"].at[z],
            send_sem=m["sent"].at[7],
            recv_sem=m["wz_recv"].at[z],
            device_id={"kv": z_of(i) * PLANE + q},
            device_id_type=MESH,
        )

    def sent(g, order, z_from, ref):
        wait_group(m["picked"].at[g, order, others], m["sent"].at[2])

    for g in range(2):
        for way in range(2):
            for step in range(1, steps(way) + 1):
                @pl.when(sends(way, step))
                def _():
                    for part in range(PARTS):
                        z_copy(g, way, step, part).wait_send()

        sent(g, 0, z, None)
        for step in range(1, 5):
            each_piece(g, step, sent)
        for d in range(8):
            @pl.when(z - d >= 0)
            def _():
                wait_group(m["back"].at[g, d, others], m["sent"].at[3])

            for part in range(ROW_PARTS):
                if 0 < d < 5:
                    @pl.when(z - d >= 0)
                    def _():
                        dn_copy(g, d, part).wait_send()
                elif d:
                    @pl.when(z - d >= 0)
                    def _():
                        up_copy(g, d, 0, part).wait_send()

    for part in range(2):
        x_copy(True, 1, part).wait_send()
        x_copy(False, 1, part).wait_send()
    x_copy(True, 2, 0).wait_send()
    x_copy(False, 2, 1).wait_send()
    for g in range(2):
        for i in range(n_x):
            c_copy(g, i).wait_send()
    out_q.wait()

    for g, part in ((0, 0), (0, 1), (1, 0), (1, 1)):
        for r in (1, 3, 2):
            wy_copy(g, part, r).wait_recv()
        if g == 0:
            continue
        for i in (2 * part, 2 * part + 1):
            total = []
            for h in range(2):
                total.append(m["wy_own"][h, i])
                for r in range(1, N_Y):
                    total[h] = total[h] + m["wyr"][h, part, r, i % 2].astype(F32)
            tiles = [
                jnp.where(low, total[0], pltpu.roll(total[1], HD, 1)),
                jnp.where(low, pltpu.roll(total[0], HD, 1), total[1]),
            ]
            for h in range(2):
                m["wz_own"][2 * i + h] = tiles[h]
                m["wz"][2 * i + h] = tiles[h].astype(BF16)
        for i in range(4 * part, 4 * part + 4):
            @pl.when(z_of(i) != z)
            def _():
                wz_copy(i).start()
    for g in range(2):
        for part in range(2):
            for r in range(1, N_Y):
                wy_copy(g, part, r).wait_send()
    mine = 2 * ((x + n_x - z // 2) % n_x) + z % 2
    total = m["wz_own"][mine]
    for r in range(1, n_z):
        frm = (z + r) % n_z
        pltpu.make_async_remote_copy(
            src_ref=m["wz"].at[0],
            dst_ref=m["wzr"].at[frm],
            send_sem=m["sent"].at[7],
            recv_sem=m["wz_recv"].at[frm],
            device_id={"kv": frm * PLANE + q},
            device_id_type=MESH,
        ).wait_recv()
        total = total + m["wzr"][frm].astype(F32)
    weight_grad[...] = total
    for i in range(n_z):
        @pl.when(z_of(i) != z)
        def _():
            wz_copy(i).wait_send()


def put_kernel(q_src, k_src, v_src, w_src, q_dst, k_dst, v_dst, w_dst, q_mid, sem):
    rows = q_mid.shape[0] // 3
    part = [pl.ds(i * rows, rows) for i in range(3)]
    into = [
        pltpu.make_async_copy(q_src.at[part[i]], q_mid.at[part[i]], sem.at[i]) for i in range(3)
    ]
    rest = [
        pltpu.make_async_copy(src, dst, sem.at[3 + i])
        for i, (src, dst) in enumerate([(k_src, k_dst), (v_src, v_dst), (w_src, w_dst)])
    ]
    out = [
        pltpu.make_async_copy(q_mid.at[part[i]], q_dst.at[part[i]], sem.at[6 + i]) for i in range(3)
    ]
    for copy in into + rest:
        copy.start()
    for i in range(3):
        into[i].wait()
        out[i].start()
    for copy in rest + out:
        copy.wait()


def put_out(query_grad, key_grad, value_grad, weight_grad):
    hbm = pl.BlockSpec(memory_space=pltpu.HBM)
    vm = pl.BlockSpec(memory_space=pltpu.VMEM)
    arrays = (query_grad, key_grad, value_grad, weight_grad)
    return pl.pallas_call(
        put_kernel,
        out_shape=tuple(jax.ShapeDtypeStruct(a.shape, a.dtype) for a in arrays),
        in_specs=[hbm, vm, vm, vm],
        out_specs=(hbm,) * 4,
        scratch_shapes=[pltpu.VMEM(query_grad.shape, F32), pltpu.SemaphoreType.DMA((9,))],
        compiler_params=pltpu.CompilerParams(vmem_limit_bytes=int(53.4 * 1024 * 1024)),
        name="put_out",
    )(*arrays)


def index_kernel(n_dev, n_b, place_of, lists, out, flat):
    z, q = place_of()
    me = z * PLANE + q
    n_list = lists.shape[1]
    n_z = n_dev // PLANE
    width = lists.shape[2]
    heads = []
    for g in range(2):
        near = pltpu.roll(lists[g], (width - z * PLANE * n_b) % width, 1)[:, :128]
        heads.append(near)
        for plane in range(n_z):
            offs = near - (plane * PLANE + q) * n_b
            offs = jnp.where((offs >= 0) & (offs < n_b), offs, 0)
            out[24 + g * n_z + plane : 25 + g * n_z + plane, :] = offs.max(axis=0, keepdims=True)
    best = out[24 : 24 + 2 * n_z, :]
    widest = best
    for k in range(1, n_b):
        widest = jnp.maximum(widest, pltpu.roll(best, 128 - k, 1))
    out[24 : 24 + 2 * n_z, :] = widest
    both = pltpu.roll(jnp.concatenate(heads, axis=0), (128 - q * n_b) % 128, 1)
    flat[...] = jnp.zeros((128, 128), jnp.int32)
    flat[: 2 * n_list, :] = both
    entry = flat[...].T[:8, :]
    block = lax.broadcasted_iota(jnp.int32, (8, 128), 0)
    lane = lax.broadcasted_iota(jnp.int32, (8, 128), 1)
    owner = jnp.floor((entry.astype(F32) + 0.5) * (1.0 / n_b)).astype(jnp.int32)
    slot = jnp.where(owner == me, n_dev + entry - owner * n_b, jnp.maximum(owner, 0))
    kind = jnp.where(entry < 0, 2, jnp.where(entry == me * n_b + block, 1, 0))
    out[:8, :] = jnp.where(lane < 2 * n_list, slot, pltpu.roll(kind, 2 * n_list, 1))
    used = jnp.where(entry < 0, -1, slot)
    for g in range(2):
        found = jnp.full((8, 128), n_list, jnp.int32)
        for n in range(n_list):
            at = g * n_list + n
            found = jnp.where(used[:, at : at + 1] == lane, n, found)
        out[8 + 8 * g : 16 + 8 * g, :] = found


def index_table(chosen, n_b, n_dev, place_of=place, interpret=False):
    vm = pl.BlockSpec(memory_space=pltpu.VMEM)
    return pl.pallas_call(
        functools.partial(index_kernel, n_dev, n_b, place_of),
        out_shape=jax.ShapeDtypeStruct((24 + 2 * n_dev // PLANE, 128), jnp.int32),
        in_specs=[vm],
        out_specs=vm,
        scratch_shapes=[pltpu.VMEM((128, 128), jnp.int32)],
        compiler_params=pltpu.CompilerParams(vmem_limit_bytes=4 * 1024 * 1024),
        cost_estimate=pl.CostEstimate(flops=10**9, bytes_accessed=8 * 1024 * 1024, transcendentals=0),
        name="index",
        interpret=interpret,
    )(chosen.transpose(0, 2, 1))


def local(queries, key_heads, values, log_sums, out_grad, inputs, chosen):
    n_dev = lax.axis_size("kv")
    n_x = lax.axis_size("tp")
    rows, feats = inputs.shape
    n_b = rows // BLOCK
    heads = log_sums.shape[0]
    n_list = chosen.shape[2]
    idx = index_table(chosen, n_b, n_dev)
    scratch = scratch_list(rows, n_dev, n_x, n_list, feats, heads)
    hbm = pl.BlockSpec(memory_space=pltpu.HBM)
    vm = pl.BlockSpec(memory_space=pltpu.VMEM)
    results = pl.pallas_call(
        functools.partial(
            fused_kernel, [name for name, _ in scratch], n_dev // PLANE, n_x, n_list
        ),
        out_shape=(
            jax.ShapeDtypeStruct(queries.shape, F32),
            jax.ShapeDtypeStruct(key_heads.shape, F32),
            jax.ShapeDtypeStruct(values.shape, F32),
            jax.ShapeDtypeStruct((feats * n_x // n_dev, 128), F32),
        ),
        in_specs=[pl.BlockSpec(memory_space=pltpu.SMEM)] + [hbm] * 6,
        out_specs=(hbm, vm, vm, vm),
        scratch_shapes=[kind for _, kind in scratch],
        compiler_params=pltpu.CompilerParams(
            collective_id=0, has_side_effects=True, vmem_limit_bytes=53 * 1024 * 1024
        ),
        name="fused",
    )(
        idx,
        key_heads.reshape(n_b, BLOCK, -1),
        values.reshape(n_b, BLOCK, -1),
        queries,
        out_grad,
        log_sums,
        inputs,
    )
    return put_out(*results)


def solution(mesh):
    placed = (
        P("kv", "tp"),
        P("kv", "tp"),
        P("kv", "tp"),
        P("tp", "kv"),
        P("kv", "tp"),
        P("kv", "tp"),
        P("tp", None, None),
    )
    return jax.shard_map(
        local,
        mesh=mesh,
        in_specs=placed,
        out_specs=(P("kv", "tp"), P("kv", "tp"), P("kv", "tp"), P("kv", "tp")),
        check_vma=False,
    )
```

```python
import functools

import jax
import jax.numpy as jnp
from jax import lax
from jax.experimental import pallas as pl
from jax.experimental.pallas import tpu as pltpu
from jax.sharding import PartitionSpec as P

HD = 64
BLOCK = 64
NEG = -1e30
LOG2E = 1.4426950408889634
CHUNK = 8
PARTS = 3
ROW_PARTS = 4
PART_ROWS = BLOCK // ROW_PARTS
N_Y = 4
N_C = 2
PLANE = N_Y * N_C
MESH = pl.DeviceIdType.MESH
RETURN_ORDER = (4, 5, 3, 6, 2, 7, 1, 0)
F32, BF16 = jnp.float32, jnp.bfloat16


def place():
    me = lax.axis_index("kv")
    return me // PLANE, me % PLANE


def scratch_list(rows, n_dev, n_x, n_list, feats, heads):
    n_b = rows // BLOCK
    tile = (BLOCK, 128)
    cols = heads // 2 * BLOCK
    dma = pltpu.SemaphoreType.DMA
    out = [
        ("kraw", pltpu.VMEM((n_b,) + tile, BF16)),
        ("vraw", pltpu.VMEM((n_b,) + tile, BF16)),
        ("qraw", pltpu.VMEM((rows, heads * HD), BF16)),
        ("graw", pltpu.VMEM((rows, heads * HD), BF16)),
        ("lraw", pltpu.VMEM((heads, rows), F32)),
        ("xraw", pltpu.VMEM((n_x, rows, feats), BF16)),
        ("lse", pltpu.VMEM((n_b * 2, 1, cols), F32)),
        ("bias", pltpu.VMEM((3,) + (BLOCK, cols), F32)),
        ("shift", pltpu.VMEM((3,) + (BLOCK, cols), F32)),
        ("qg", pltpu.VMEM((rows, heads * HD), F32)),
        ("picked", pltpu.VMEM((2, 8, PLANE) + tile, BF16)),
        ("qd", pltpu.VMEM((2 * cols, 128), BF16)),
        ("cat", pltpu.VMEM((n_list,) + tile, BF16)),
        ("sdp", pltpu.VMEM((n_list, BLOCK, 2 * cols), F32)),
        ("pd", pltpu.VMEM((n_list, BLOCK, 2 * cols), BF16)),
        ("terms", pltpu.VMEM((n_b, n_list + 1) + tile, F32)),
        ("ret", pltpu.VMEM((2, n_dev) + tile, BF16)),
        ("own_tot", pltpu.VMEM((2, n_b) + tile, F32)),
        ("back", pltpu.VMEM((2, 8, PLANE) + tile, BF16)),
        ("acc", pltpu.VMEM((2, n_b) + tile, F32)),
        ("zs", pltpu.VMEM((2, 8, ROW_PARTS, n_b, PART_ROWS, 128), BF16)),
        ("zr_dn", pltpu.VMEM((2, 4, ROW_PARTS, n_b, PART_ROWS, 128), BF16)),
        ("zr_up", pltpu.VMEM((2, 4, ROW_PARTS, n_b, PART_ROWS, 128), BF16)),
        ("kg", pltpu.VMEM((rows, 128), BF16)),
        ("kg_t", pltpu.VMEM((128, rows), BF16)),
        ("wpart", pltpu.VMEM((2, n_x, N_C, N_Y) + tile, BF16)),
        ("crecv", pltpu.VMEM((2, n_x, N_Y) + tile, BF16)),
        ("wy", pltpu.VMEM((2, 2, N_Y, n_x // 2) + tile, BF16)),
        ("wy_own", pltpu.VMEM((2, n_x) + tile, F32)),
        ("wyr", pltpu.VMEM((2, 2, N_Y, n_x // 2) + tile, BF16)),
        ("wz", pltpu.VMEM((8,) + tile, BF16)),
        ("wz_own", pltpu.VMEM((8,) + tile, F32)),
        ("wzr", pltpu.VMEM((8,) + tile, BF16)),
        ("in_sem", dma((6,))),
        ("out_sem", dma((1,))),
        ("sent", dma((8,))),
        ("z_recv", dma((2, 7, PARTS))),
        ("y_recv", dma((2, 8))),
        ("x_recv", dma((2, 3))),
        ("b_recv", dma((2, 8))),
        ("r_recv_dn", dma((2, 4, ROW_PARTS))),
        ("r_recv_up", dma((2, 4, ROW_PARTS))),
        ("c_recv", dma((2, n_x))),
        ("wy_recv", dma((2, 2, N_Y - 1))),
        ("wz_recv", dma((8,))),
    ]
    for g in range(2):
        out.append((f"own{g}", pltpu.VMEM((n_b,) + tile, BF16)))
        out.append((f"tab{g}", pltpu.VMEM((n_dev + n_b,) + tile, BF16)))
        for step in range(1, 5):
            out.append((f"held{g}0{step}", pltpu.VMEM((n_b,) + tile, BF16)))
        for step in range(1, 4):
            out.append((f"held{g}1{step}", pltpu.VMEM((n_b,) + tile, BF16)))
    return out


def fused_kernel(names, n_z, n_x, n_list, *refs):
    idx, keys, vals, queries, out_grad, log_sums, inputs = refs[:7]
    query_grad, key_grad, value_grad, weight_grad = refs[7:11]
    m = dict(zip(names, refs[11:]))
    n_b = m["kraw"].shape[0]
    n_dev = n_z * PLANE
    heads = m["lraw"].shape[0]
    per_group = heads // 2
    cols = per_group * BLOCK
    z, q = place()
    y, c = q // N_C, q % N_C
    x = lax.axis_index("tp")

    barrier = pltpu.get_barrier_semaphore()
    partners = [{"kv": (z + r) % n_z * PLANE + q} for r in range(1, n_z)]
    partners += [{"kv": z * PLANE + (q + r) % PLANE} for r in range(1, PLANE)]
    right, left = {"tp": (x + 1) % n_x}, {"tp": (x + n_x - 1) % n_x}
    partners += [right, left]
    for who in partners:
        pl.semaphore_signal(barrier, inc=1, device_id=who, device_id_type=MESH)

    loads = [
        pltpu.make_async_copy(src, dst, m["in_sem"].at[i])
        for i, (src, dst) in enumerate(
            [
                (keys, m["kraw"]),
                (vals, m["vraw"]),
                (queries, m["qraw"]),
                (out_grad, m["graw"]),
                (log_sums, m["lraw"]),
                (inputs, m["xraw"].at[0]),
            ]
        )
    ]
    for copy in loads:
        copy.start()
    up_z = {"kv": (z + 1) % n_z * PLANE + q}
    dn_z = {"kv": (z + n_z - 1) % n_z * PLANE + q}
    lane = lax.broadcasted_iota(jnp.int32, (BLOCK, 128), 1)
    low = lane < HD
    loads[0].wait()
    loads[1].wait()
    for b in range(n_b):
        k = m["kraw"][b].astype(F32)
        v = m["vraw"][b].astype(F32)
        kv0 = jnp.where(low, k, pltpu.roll(v, HD, 1)).astype(BF16)
        kv1 = jnp.where(low, pltpu.roll(k, HD, 1), v).astype(BF16)
        m["own0"][b] = kv0
        m["own1"][b] = kv1
        m["tab0"][n_dev + b] = kv0
        m["tab1"][n_dev + b] = kv1
    pl.semaphore_wait(barrier, len(partners))

    def held(g, way, step):
        return m[f"own{g}"] if step == 0 else m[f"held{g}{way}{step}"]

    def z_copy(g, way, step, part):
        blocks = pl.ds(part * (n_b // PARTS), n_b // PARTS)
        return pltpu.make_async_remote_copy(
            src_ref=held(g, way, step - 1).at[blocks],
            dst_ref=held(g, way, step).at[blocks],
            send_sem=m["sent"].at[0],
            recv_sem=m["z_recv"].at[g, way * 4 + step - 1, part],
            device_id=dn_z if way else up_z,
            device_id_type=MESH,
        )

    def sends(way, step):
        if way:
            return (z + step - 1) % n_z < 3
        return (z < n_z - 1) & (z - step + 1 >= 0)

    def gets(way, step):
        if way:
            return (z + step) % n_z < 3
        return z - step >= 0

    def steps(way):
        return 3 if way else 4

    def x_copy(to_right, rel, part):
        half = inputs.shape[0] // 2
        rows = pl.ds(part * half, half)
        slot = rel if to_right else n_x - rel
        if rel == 1:
            src = inputs.at[rows]
        else:
            src = m["xraw"].at[1 if to_right else n_x - 1, rows]
        side = 0 if to_right else 1
        return pltpu.make_async_remote_copy(
            src_ref=src,
            dst_ref=m["xraw"].at[slot, rows],
            send_sem=m["sent"].at[1],
            recv_sem=m["x_recv"].at[side, 2 if rel == 2 else part],
            device_id=right if to_right else left,
            device_id_type=MESH,
        )

    def y_copy(g, order, z_from, r):
        to = (q + r) % PLANE
        return pltpu.make_async_remote_copy(
            src_ref=m["picked"].at[g, order, r],
            dst_ref=m[f"tab{g}"].at[z_from * PLANE + q],
            send_sem=m["sent"].at[2],
            recv_sem=m["y_recv"].at[g, order],
            device_id={"kv": z * PLANE + to},
            device_id_type=MESH,
        )

    others = pl.ds(1, PLANE - 1)

    def wait_group(ref, sem):
        pltpu.make_async_copy(ref, ref, sem).wait()

    def pick(g, order, z_from, ref):
        def one(r, carry):
            to = (q + r) % PLANE
            m["picked"][g, order, r] = ref[idx[24 + g * n_z + z_from, to * n_b]]

            @pl.when(r > 1)
            def _():
                y_copy(g, order, z_from, r - 1).start()

            return carry

        lax.fori_loop(1, PLANE, one, 0)
        m[f"tab{g}"][z_from * PLANE + q] = ref[idx[24 + g * n_z + z_from, q * n_b]]
        y_copy(g, order, z_from, PLANE - 1).start()

    def each_piece(g, step, act):
        @pl.when(gets(0, step))
        def _():
            act(g, step, z - step, held(g, 0, step))

        if step < 4:
            @pl.when(gets(1, step) & (z + step >= n_z))
            def _():
                act(g, 4 + step, z + step - n_z, held(g, 1, step))

    def set_out(g):
        for part in range(PARTS):
            for way in range(2):
                @pl.when(sends(way, 1))
                def _():
                    z_copy(g, way, 1, part).start()

    set_out(0)
    for part in range(2):
        x_copy(True, 1, part).start()
        x_copy(False, 1, 1 - part).start()
    pick(0, 0, z, m["own0"])
    pick(1, 0, z, m["own1"])

    def relay(g, step):
        for part in range(PARTS):
            for way in range(2):
                if step <= steps(way):
                    @pl.when(gets(way, step))
                    def _():
                        z_copy(g, way, step, part).wait_recv()

                if step + 1 <= steps(way):
                    @pl.when(sends(way, step + 1))
                    def _():
                        z_copy(g, way, step + 1, part).start()

    key_at = lax.broadcasted_iota(jnp.int32, (BLOCK, cols), 0)
    tok_at = lax.broadcasted_iota(jnp.int32, (BLOCK, cols), 1) % BLOCK
    m["bias"][0] = jnp.zeros((BLOCK, cols), F32)
    m["bias"][1] = jnp.where(key_at <= tok_at, 0.0, NEG)
    m["bias"][2] = jnp.full((BLOCK, cols), NEG, F32)
    for p in range(n_b):
        m["terms"][p, n_list] = jnp.zeros((BLOCK, 128), F32)
    loads[4].wait()
    for p in range(n_b):
        for g in range(2):
            row = [
                m["lraw"][g * per_group + r : g * per_group + r + 1, p * BLOCK : (p + 1) * BLOCK]
                for r in range(per_group)
            ]
            m["lse"][p * 2 + g] = jnp.concatenate(row, axis=1)

    for step in range(1, 5):
        relay(0, step)
        if step == 2:
            set_out(1)
        each_piece(0, step, pick)

    def relay_and_pick(g, step):
        relay(g, step)
        each_piece(g, step, pick)

    def relay_x():
        x_copy(True, 1, 0).wait_recv()
        x_copy(True, 2, 0).start()
        x_copy(False, 1, 1).wait_recv()
        x_copy(False, 2, 1).start()

    def landed(g, order, z_from, ref):
        wait_group(m["picked"].at[g, order, others], m["y_recv"].at[g, order])

    def masked_rows(ref, row, g, factor, side):
        parts = []
        for r in range(per_group):
            col = (g * per_group + r) * HD
            part = ref[pl.ds(row, BLOCK), col // 128 * 128 : col // 128 * 128 + 128]
            part = part.astype(F32) * factor
            if r % 2 != side:
                part = pltpu.roll(part, HD, 1)
            parts.append(jnp.where(low != (side == 1), part, 0.0).astype(BF16))
        return parts

    def attention(g, between):
        tab = m[f"tab{g}"]
        sdp, pd, qd, cat, shift = m["sdp"], m["pd"], m["qd"], m["cat"], m["shift"]
        chunks = [slice(n, n + CHUNK) for n in range(0, n_list, CHUNK)]
        nt = (((1,), (1,)), ((), ()))
        nn = (((1,), (0,)), ((), ()))

        def one_position(p, carry):
            row = pl.multiple_of(p * BLOCK, BLOCK)
            for r, part in enumerate(masked_rows(m["qraw"], row, g, HD ** -0.5, 0)):
                qd[r * BLOCK : (r + 1) * BLOCK, :] = part
            for r, part in enumerate(masked_rows(m["graw"], row, g, 1.0, 1)):
                qd[cols + r * BLOCK : cols + (r + 1) * BLOCK, :] = part
            for n in range(n_list):
                cat[n] = tab[idx[p, g * n_list + n]]
            for kind in range(3):
                shift[kind] = m["bias"][kind] - m["lse"][p * 2 + g] * LOG2E

            acc = jnp.zeros((8, cols), F32)
            for ch in chunks:
                both = lax.dot_general(
                    cat[ch].reshape(CHUNK * BLOCK, 128), qd[...], nt, preferred_element_type=F32
                ).reshape(CHUNK, BLOCK, 2 * cols)
                for n in range(ch.start, ch.stop):
                    prod = both[n - ch.start]
                    pr = jnp.exp2(prod[:, :cols] * LOG2E + shift[idx[p, (2 + g) * n_list + n]])
                    sdp[n, :, :cols] = pr
                    sdp[n, :, cols:] = prod[:, cols:]
                    pd[n, :, cols:] = pr.astype(BF16)
                    pr = pr * prod[:, cols:]
                    acc = acc + pr.reshape(BLOCK // 8, 8, cols).sum(axis=0)
            delta = acc.sum(axis=0, keepdims=True)
            for ch in chunks:
                for n in range(ch.start, ch.stop):
                    ds = sdp[n, :, :cols] * (sdp[n, :, cols:] - delta)
                    pd[n, :, :cols] = ds.astype(BF16)
                m["terms"][p, ch] = lax.dot_general(
                    pd[ch].reshape(CHUNK * BLOCK, 2 * cols), qd[...], nn, preferred_element_type=F32
                ).reshape(CHUNK, BLOCK, 128)
            dq_t = lax.dot_general(
                cat[...].reshape(n_list * BLOCK, 128),
                pd[:, :, :cols].reshape(n_list * BLOCK, cols),
                (((0,), (0,)), ((), ())),
                preferred_element_type=F32,
            )
            dq = dq_t.T * (HD ** -0.5)
            for pair in range(per_group // 2):
                even = dq[(2 * pair) * BLOCK : (2 * pair + 1) * BLOCK]
                odd = dq[(2 * pair + 1) * BLOCK : (2 * pair + 2) * BLOCK]
                col = g * per_group * HD + pair * 128
                m["qg"][pl.ds(row, BLOCK), col : col + 128] = jnp.where(
                    low, even, pltpu.roll(odd, HD, 1)
                )
            for at, act in between.items():
                @pl.when(p == at)
                def _():
                    act()

            return carry

        lax.fori_loop(0, n_b, one_position, 0)

    def summed_terms(g, j):
        total = m["terms"][0, idx[8 + 8 * g, j]]
        for p in range(1, n_b):
            total = total + m["terms"][p, idx[8 + 8 * g + p, j]]
        return total

    def b_copy(g, d, r):
        to = (q + r) % PLANE
        return pltpu.make_async_remote_copy(
            src_ref=m["ret"].at[g, (z - d) * PLANE + to],
            dst_ref=m["back"].at[g, d, q],
            send_sem=m["sent"].at[3],
            recv_sem=m["b_recv"].at[g, d],
            device_id={"kv": z * PLANE + to},
            device_id_type=MESH,
        )

    def give_back(g):
        for d in RETURN_ORDER:
            @pl.when(z - d >= 0)
            def _():
                for r in list(range(1, PLANE)) + [0]:
                    j = (z - d) * PLANE + (q + r) % PLANE
                    m["ret"][g, j] = summed_terms(g, j).astype(BF16)
                for r in range(1, PLANE):
                    b_copy(g, d, r).start()

        def own(b, carry):
            m["own_tot"][g, b] = summed_terms(g, n_dev + b)
            return carry

        lax.fori_loop(0, n_b, own, 0)

    def accumulate(g, d, part):
        rows = slice(part * PART_ROWS, (part + 1) * PART_ROWS)
        accs = [jnp.zeros((PART_ROWS, 128), F32) for _ in range(n_b)]
        for r in range(PLANE):
            frm = (q + r) % PLANE
            if r == 0:
                val = m["ret"][g, (z - d) * PLANE + q, rows, :]
            else:
                val = m["back"][g, d, frm, rows, :]
            val = val.astype(F32)
            block = idx[24 + g * n_z + z - d, frm * n_b]
            for b in range(n_b):
                accs[b] = accs[b] + jnp.where(block == b, val, 0.0)
        for b in range(n_b):
            m["acc"][g, b, rows, :] = accs[b]

    def dn_copy(g, d, part):
        return pltpu.make_async_remote_copy(
            src_ref=m["zs"].at[g, d, part],
            dst_ref=m["zr_dn"].at[g, d - 1, part],
            send_sem=m["sent"].at[4],
            recv_sem=m["r_recv_dn"].at[g, d - 1, part],
            device_id=dn_z,
            device_id_type=MESH,
        )

    def up_copy(g, d, at, part):
        to = n_z - 1 if at else n_z - 1 - d
        return pltpu.make_async_remote_copy(
            src_ref=m["zs"].at[g, d, part],
            dst_ref=m["zr_up"].at[g, at, part],
            send_sem=m["sent"].at[4],
            recv_sem=m["r_recv_up"].at[g, at, part],
            device_id={"kv": to * PLANE + q},
            device_id_type=MESH,
        )

    def add_arrival(g, copy, ref, part):
        copy.wait_recv()
        rows = slice(part * PART_ROWS, (part + 1) * PART_ROWS)
        for b in range(n_b):
            m["acc"][g, b, rows, :] += ref[b].astype(F32)

    def dn_arrival(g, d, part):
        @pl.when(z < n_z - 1)
        def _():
            add_arrival(g, dn_copy(g, d, part), m["zr_dn"].at[g, d - 1, part], part)

    def up_arrival(g, at, part):
        add_arrival(g, up_copy(g, 5, at, part), m["zr_up"].at[g, at, part], part)

    def store_out(g, d, part):
        rows = slice(part * PART_ROWS, (part + 1) * PART_ROWS)
        for b in range(n_b):
            m["zs"][g, d, part, b] = m["acc"][g, b, rows, :].astype(BF16)

    def collect(g, d):
        @pl.when(z - d >= 0)
        def _():
            wait_group(m["back"].at[g, d, others], m["b_recv"].at[g, d])
            for part in range(ROW_PARTS):
                accumulate(g, d, part)
                if d < 4:
                    dn_arrival(g, d + 1, part)
                if d in (6, 7):
                    @pl.when(z == n_z - 1)
                    def _():
                        for at in {6: (2,), 7: (1, 3)}[d]:
                            up_arrival(g, at, part)

                if d == 0:
                    @pl.when(z < 3)
                    def _():
                        up_arrival(g, 0, part)
                    continue
                store_out(g, d, part)
                if d < 5:
                    dn_copy(g, d, part).start()
                else:
                    @pl.when(z == n_z - 1)
                    def _():
                        up_copy(g, d, 0, part).start()

                    for plane, at in {5: ((5, 1), (6, 2)), 6: ((6, 3),), 7: ()}[d]:
                        @pl.when(z == plane)
                        def _():
                            up_copy(g, d, at, part).start()

    def wait_fetch(g):
        landed(g, 0, z, None)
        for step in range(1, 5):
            each_piece(g, step, landed)

    relay_and_pick(1, 1)
    relay_and_pick(1, 2)
    loads[2].wait()
    loads[3].wait()
    wait_fetch(0)
    attention(
        0,
        {
            1: functools.partial(relay_and_pick, 1, 3),
            3: functools.partial(relay_and_pick, 1, 4),
            4: relay_x,
        },
    )
    give_back(0)
    wait_fetch(1)
    attention(1, {2 + i: functools.partial(collect, 0, RETURN_ORDER[i]) for i in range(3)})
    give_back(1)
    out_q = pltpu.make_async_copy(m["qg"], query_grad, m["out_sem"].at[0])
    out_q.start()
    def c_copy(g, i):
        return pltpu.make_async_remote_copy(
            src_ref=m["wpart"].at[g, i, 1 - c],
            dst_ref=m["crecv"].at[g, i],
            send_sem=m["sent"].at[5],
            recv_sem=m["c_recv"].at[g, i],
            device_id={"kv": z * PLANE + y * N_C + (1 - c)},
            device_id_type=MESH,
        )

    def wy_copy(g, part, r):
        to = (y + r) % N_Y
        return pltpu.make_async_remote_copy(
            src_ref=m["wy"].at[g, part, r],
            dst_ref=m["wyr"].at[g, part, r],
            send_sem=m["sent"].at[6],
            recv_sem=m["wy_recv"].at[g, part, r - 1],
            device_id={"kv": z * PLANE + to * N_C + c},
            device_id_type=MESH,
        )

    half = inputs.shape[1] // 2

    def combine(g):
        for b in range(n_b):
            total = m["acc"][g, b] + m["own_tot"][g, b]
            m["acc"][g, b] = total
            m["kg"][b * BLOCK : (b + 1) * BLOCK, :] = total.astype(BF16)
        m["kg_t"][...] = m["kg"][...].T

    def own_terms(g, i):
        w_t = [
            lax.dot_general(
                m["kg_t"][:HD, :], m["xraw"][i, :, h * half : (h + 1) * half],
                (((1,), (0,)), ((), ())), preferred_element_type=F32,
            )
            for h in range(2)
        ]
        w = jnp.concatenate(w_t, axis=0).T.astype(BF16)
        for yy in range(N_Y):
            for cc in range(N_C):
                first = (yy * N_C + cc) * BLOCK
                m["wpart"][g, i, cc, yy] = w[first : first + BLOCK]

    def core_sum(g, i):
        c_copy(g, i).wait_recv()
        for r in range(N_Y):
            yy = (y + r) % N_Y
            both = m["wpart"][g, i, c, yy].astype(F32) + m["crecv"][g, i, yy].astype(F32)
            if r:
                m["wy"][g, i // 2, r, i % 2] = both.astype(BF16)
            else:
                m["wy_own"][g, i] = both
        if i % 2:
            for r in (2, 1, 3):
                wy_copy(g, i // 2, r).start()

    def terms_out(g):
        combine(g)
        for i in range(n_x):
            own_terms(g, i)
            if i:
                c_copy(g, i - 1).start()
        c_copy(g, n_x - 1).start()

    for g, d in [
        (0, 2), (1, 4), (0, 6), (1, 5), (0, 1), (1, 3), (0, 7), (1, 6), (1, 2), (0, 0)
    ]:
        collect(g, d)
    x_copy(True, 1, 1).wait_recv()
    x_copy(False, 1, 0).wait_recv()
    x_copy(True, 2, 0).wait_recv()
    x_copy(False, 2, 1).wait_recv()
    loads[5].wait()
    terms_out(0)
    collect(1, 7)
    for i in range(n_x):
        core_sum(0, i)
    collect(1, 1)
    collect(1, 0)
    combine(1)
    lag = 2
    for i in range(n_x + lag):
        if i < n_x:
            own_terms(1, i)
        if 0 < i <= n_x:
            c_copy(1, i - 1).start()
        if i >= lag:
            core_sum(1, i - lag)
    for b in range(n_b):
        rows = slice(b * BLOCK, (b + 1) * BLOCK)
        t0, t1 = m["acc"][0, b], m["acc"][1, b]
        key_grad[rows, :] = jnp.where(low, t0, pltpu.roll(t1, HD, 1))
        value_grad[rows, :] = jnp.where(low, pltpu.roll(t0, HD, 1), t1)

    def z_of(i):
        return 2 * ((x + n_x - i // 2) % n_x) + i % 2

    def wz_copy(i):
        return pltpu.make_async_remote_copy(
            src_ref=m["wz"].at[i],
            dst_ref=m["wzr"].at[z],
            send_sem=m["sent"].at[7],
            recv_sem=m["wz_recv"].at[z],
            device_id={"kv": z_of(i) * PLANE + q},
            device_id_type=MESH,
        )

    def sent(g, order, z_from, ref):
        wait_group(m["picked"].at[g, order, others], m["sent"].at[2])

    for g in range(2):
        for way in range(2):
            for step in range(1, steps(way) + 1):
                @pl.when(sends(way, step))
                def _():
                    for part in range(PARTS):
                        z_copy(g, way, step, part).wait_send()

        sent(g, 0, z, None)
        for step in range(1, 5):
            each_piece(g, step, sent)
        for d in range(8):
            @pl.when(z - d >= 0)
            def _():
                wait_group(m["back"].at[g, d, others], m["sent"].at[3])

            for part in range(ROW_PARTS):
                if 0 < d < 5:
                    @pl.when(z - d >= 0)
                    def _():
                        dn_copy(g, d, part).wait_send()
                elif d:
                    @pl.when(z - d >= 0)
                    def _():
                        up_copy(g, d, 0, part).wait_send()

    for part in range(2):
        x_copy(True, 1, part).wait_send()
        x_copy(False, 1, part).wait_send()
    x_copy(True, 2, 0).wait_send()
    x_copy(False, 2, 1).wait_send()
    for g in range(2):
        for i in range(n_x):
            c_copy(g, i).wait_send()
    out_q.wait()

    for g, part in ((0, 0), (0, 1), (1, 0), (1, 1)):
        for r in (1, 3, 2):
            wy_copy(g, part, r).wait_recv()
        if g == 0:
            continue
        for i in (2 * part, 2 * part + 1):
            total = []
            for h in range(2):
                total.append(m["wy_own"][h, i])
                for r in range(1, N_Y):
                    total[h] = total[h] + m["wyr"][h, part, r, i % 2].astype(F32)
            tiles = [
                jnp.where(low, total[0], pltpu.roll(total[1], HD, 1)),
                jnp.where(low, pltpu.roll(total[0], HD, 1), total[1]),
            ]
            for h in range(2):
                m["wz_own"][2 * i + h] = tiles[h]
                m["wz"][2 * i + h] = tiles[h].astype(BF16)
        for i in range(4 * part, 4 * part + 4):
            @pl.when(z_of(i) != z)
            def _():
                wz_copy(i).start()
    for g in range(2):
        for part in range(2):
            for r in range(1, N_Y):
                wy_copy(g, part, r).wait_send()
    mine = 2 * ((x + n_x - z // 2) % n_x) + z % 2
    total = m["wz_own"][mine]
    for r in range(1, n_z):
        frm = (z + r) % n_z
        pltpu.make_async_remote_copy(
            src_ref=m["wz"].at[0],
            dst_ref=m["wzr"].at[frm],
            send_sem=m["sent"].at[7],
            recv_sem=m["wz_recv"].at[frm],
            device_id={"kv": frm * PLANE + q},
            device_id_type=MESH,
        ).wait_recv()
        total = total + m["wzr"][frm].astype(F32)
    weight_grad[...] = total
    for i in range(n_z):
        @pl.when(z_of(i) != z)
        def _():
            wz_copy(i).wait_send()


def put_kernel(q_src, k_src, v_src, w_src, q_dst, k_dst, v_dst, w_dst, q_mid, sem):
    rows = q_mid.shape[0] // 3
    part = [pl.ds(i * rows, rows) for i in range(3)]
    into = [
        pltpu.make_async_copy(q_src.at[part[i]], q_mid.at[part[i]], sem.at[i]) for i in range(3)
    ]
    rest = [
        pltpu.make_async_copy(src, dst, sem.at[3 + i])
        for i, (src, dst) in enumerate([(k_src, k_dst), (v_src, v_dst), (w_src, w_dst)])
    ]
    out = [
        pltpu.make_async_copy(q_mid.at[part[i]], q_dst.at[part[i]], sem.at[6 + i]) for i in range(3)
    ]
    for copy in into + rest:
        copy.start()
    for i in range(3):
        into[i].wait()
        out[i].start()
    for copy in rest + out:
        copy.wait()


def put_out(query_grad, key_grad, value_grad, weight_grad):
    hbm = pl.BlockSpec(memory_space=pltpu.HBM)
    vm = pl.BlockSpec(memory_space=pltpu.VMEM)
    arrays = (query_grad, key_grad, value_grad, weight_grad)
    return pl.pallas_call(
        put_kernel,
        out_shape=tuple(jax.ShapeDtypeStruct(a.shape, a.dtype) for a in arrays),
        in_specs=[hbm, vm, vm, vm],
        out_specs=(hbm,) * 4,
        scratch_shapes=[pltpu.VMEM(query_grad.shape, F32), pltpu.SemaphoreType.DMA((9,))],
        compiler_params=pltpu.CompilerParams(vmem_limit_bytes=int(53.4 * 1024 * 1024)),
        name="put_out",
    )(*arrays)


def index_kernel(n_dev, n_b, place_of, lists, out, flat):
    z, q = place_of()
    me = z * PLANE + q
    n_list = lists.shape[1]
    n_z = n_dev // PLANE
    width = lists.shape[2]
    heads = []
    for g in range(2):
        near = pltpu.roll(lists[g], (width - z * PLANE * n_b) % width, 1)[:, :128]
        heads.append(near)
        for plane in range(n_z):
            offs = near - (plane * PLANE + q) * n_b
            offs = jnp.where((offs >= 0) & (offs < n_b), offs, 0)
            out[24 + g * n_z + plane : 25 + g * n_z + plane, :] = offs.max(axis=0, keepdims=True)
    best = out[24 : 24 + 2 * n_z, :]
    widest = best
    for k in range(1, n_b):
        widest = jnp.maximum(widest, pltpu.roll(best, 128 - k, 1))
    out[24 : 24 + 2 * n_z, :] = widest
    both = pltpu.roll(jnp.concatenate(heads, axis=0), (128 - q * n_b) % 128, 1)
    flat[...] = jnp.zeros((128, 128), jnp.int32)
    flat[: 2 * n_list, :] = both
    entry = flat[...].T[:8, :]
    block = lax.broadcasted_iota(jnp.int32, (8, 128), 0)
    lane = lax.broadcasted_iota(jnp.int32, (8, 128), 1)
    owner = jnp.floor((entry.astype(F32) + 0.5) * (1.0 / n_b)).astype(jnp.int32)
    slot = jnp.where(owner == me, n_dev + entry - owner * n_b, jnp.maximum(owner, 0))
    kind = jnp.where(entry < 0, 2, jnp.where(entry == me * n_b + block, 1, 0))
    out[:8, :] = jnp.where(lane < 2 * n_list, slot, pltpu.roll(kind, 2 * n_list, 1))
    used = jnp.where(entry < 0, -1, slot)
    for g in range(2):
        found = jnp.full((8, 128), n_list, jnp.int32)
        for n in range(n_list):
            at = g * n_list + n
            found = jnp.where(used[:, at : at + 1] == lane, n, found)
        out[8 + 8 * g : 16 + 8 * g, :] = found


def index_table(chosen, n_b, n_dev, place_of=place, interpret=False):
    vm = pl.BlockSpec(memory_space=pltpu.VMEM)
    return pl.pallas_call(
        functools.partial(index_kernel, n_dev, n_b, place_of),
        out_shape=jax.ShapeDtypeStruct((24 + 2 * n_dev // PLANE, 128), jnp.int32),
        in_specs=[vm],
        out_specs=vm,
        scratch_shapes=[pltpu.VMEM((128, 128), jnp.int32)],
        compiler_params=pltpu.CompilerParams(vmem_limit_bytes=4 * 1024 * 1024),
        cost_estimate=pl.CostEstimate(flops=10**9, bytes_accessed=8 * 1024 * 1024, transcendentals=0),
        name="index",
        interpret=interpret,
    )(chosen.transpose(0, 2, 1))


def local(queries, key_heads, values, log_sums, out_grad, inputs, chosen):
    n_dev = lax.axis_size("kv")
    n_x = lax.axis_size("tp")
    rows, feats = inputs.shape
    n_b = rows // BLOCK
    heads = log_sums.shape[0]
    n_list = chosen.shape[2]
    idx = index_table(chosen, n_b, n_dev)
    scratch = scratch_list(rows, n_dev, n_x, n_list, feats, heads)
    hbm = pl.BlockSpec(memory_space=pltpu.HBM)
    vm = pl.BlockSpec(memory_space=pltpu.VMEM)
    results = pl.pallas_call(
        functools.partial(
            fused_kernel, [name for name, _ in scratch], n_dev // PLANE, n_x, n_list
        ),
        out_shape=(
            jax.ShapeDtypeStruct(queries.shape, F32),
            jax.ShapeDtypeStruct(key_heads.shape, F32),
            jax.ShapeDtypeStruct(values.shape, F32),
            jax.ShapeDtypeStruct((feats * n_x // n_dev, 128), F32),
        ),
        in_specs=[pl.BlockSpec(memory_space=pltpu.SMEM)] + [hbm] * 6,
        out_specs=(hbm, vm, vm, vm),
        scratch_shapes=[kind for _, kind in scratch],
        compiler_params=pltpu.CompilerParams(
            collective_id=0, has_side_effects=True, vmem_limit_bytes=53 * 1024 * 1024
        ),
        name="fused",
    )(
        idx,
        key_heads.reshape(n_b, BLOCK, -1),
        values.reshape(n_b, BLOCK, -1),
        queries,
        out_grad,
        log_sums,
        inputs,
    )
    return put_out(*results)


def solution(mesh):
    placed = (
        P("kv", "tp"),
        P("kv", "tp"),
        P("kv", "tp"),
        P("tp", "kv"),
        P("kv", "tp"),
        P("kv", "tp"),
        P("tp", None, None),
    )
    return jax.shard_map(
        local,
        mesh=mesh,
        in_specs=placed,
        out_specs=(P("kv", "tp"), P("kv", "tp"), P("kv", "tp"), P("kv", "tp")),
        check_vma=False,
    )
```

```python
import functools

import jax
import jax.numpy as jnp
from jax import lax
from jax.experimental import pallas as pl
from jax.experimental.pallas import tpu as pltpu
from jax.sharding import PartitionSpec as P

HD = 64
BLOCK = 64
NEG = -1e30
LOG2E = 1.4426950408889634
CHUNK = 8
PARTS = 3
ROW_PARTS = 4
PART_ROWS = BLOCK // ROW_PARTS
N_Y = 4
N_C = 2
PLANE = N_Y * N_C
MESH = pl.DeviceIdType.MESH
RETURN_ORDER = (4, 5, 3, 6, 2, 7, 1, 0)
F32, BF16 = jnp.float32, jnp.bfloat16


def place():
    me = lax.axis_index("kv")
    return me // PLANE, me % PLANE


def scratch_list(rows, n_dev, n_x, n_list, feats, heads):
    n_b = rows // BLOCK
    tile = (BLOCK, 128)
    cols = heads // 2 * BLOCK
    dma = pltpu.SemaphoreType.DMA
    out = [
        ("kraw", pltpu.VMEM((n_b,) + tile, BF16)),
        ("vraw", pltpu.VMEM((n_b,) + tile, BF16)),
        ("qraw", pltpu.VMEM((rows, heads * HD), BF16)),
        ("graw", pltpu.VMEM((rows, heads * HD), BF16)),
        ("lraw", pltpu.VMEM((heads, rows), F32)),
        ("xraw", pltpu.VMEM((n_x, rows, feats), BF16)),
        ("lse", pltpu.VMEM((n_b * 2, 1, cols), F32)),
        ("bias", pltpu.VMEM((3,) + (BLOCK, cols), F32)),
        ("shift", pltpu.VMEM((3,) + (BLOCK, cols), F32)),
        ("qg", pltpu.VMEM((rows, heads * HD), F32)),
        ("picked", pltpu.VMEM((2, 8, PLANE) + tile, BF16)),
        ("qd", pltpu.VMEM((2 * cols, 128), BF16)),
        ("cat", pltpu.VMEM((n_list,) + tile, BF16)),
        ("sdp", pltpu.VMEM((n_list, BLOCK, 2 * cols), F32)),
        ("pd", pltpu.VMEM((n_list, BLOCK, 2 * cols), BF16)),
        ("terms", pltpu.VMEM((n_b, n_list + 1) + tile, F32)),
        ("ret", pltpu.VMEM((2, n_dev) + tile, BF16)),
        ("own_tot", pltpu.VMEM((2, n_b) + tile, F32)),
        ("back", pltpu.VMEM((2, 8, PLANE) + tile, BF16)),
        ("acc", pltpu.VMEM((2, n_b) + tile, F32)),
        ("zs", pltpu.VMEM((2, 8, ROW_PARTS, n_b, PART_ROWS, 128), BF16)),
        ("zr_dn", pltpu.VMEM((2, 4, ROW_PARTS, n_b, PART_ROWS, 128), BF16)),
        ("zr_up", pltpu.VMEM((2, 4, ROW_PARTS, n_b, PART_ROWS, 128), BF16)),
        ("kg", pltpu.VMEM((rows, 128), BF16)),
        ("kg_t", pltpu.VMEM((128, rows), BF16)),
        ("wpart", pltpu.VMEM((2, n_x, N_C, N_Y) + tile, BF16)),
        ("crecv", pltpu.VMEM((2, n_x, N_Y) + tile, BF16)),
        ("wy", pltpu.VMEM((2, 2, N_Y, n_x // 2) + tile, BF16)),
        ("wy_own", pltpu.VMEM((2, n_x) + tile, F32)),
        ("wyr", pltpu.VMEM((2, 2, N_Y, n_x // 2) + tile, BF16)),
        ("wz", pltpu.VMEM((8,) + tile, BF16)),
        ("wz_own", pltpu.VMEM((8,) + tile, F32)),
        ("wzr", pltpu.VMEM((8,) + tile, BF16)),
        ("in_sem", dma((6,))),
        ("out_sem", dma((1,))),
        ("sent", dma((8,))),
        ("z_recv", dma((2, 7, PARTS))),
        ("y_recv", dma((2, 8))),
        ("x_recv", dma((2, 3))),
        ("b_recv", dma((2, 8))),
        ("r_recv_dn", dma((2, 4, ROW_PARTS))),
        ("r_recv_up", dma((2, 4, ROW_PARTS))),
        ("c_recv", dma((2, n_x))),
        ("wy_recv", dma((2, 2, N_Y - 1))),
        ("wz_recv", dma((8,))),
    ]
    for g in range(2):
        out.append((f"own{g}", pltpu.VMEM((n_b,) + tile, BF16)))
        out.append((f"tab{g}", pltpu.VMEM((n_dev + n_b,) + tile, BF16)))
        for step in range(1, 5):
            out.append((f"held{g}0{step}", pltpu.VMEM((n_b,) + tile, BF16)))
        for step in range(1, 4):
            out.append((f"held{g}1{step}", pltpu.VMEM((n_b,) + tile, BF16)))
    return out


def fused_kernel(names, n_z, n_x, n_list, *refs):
    idx, keys, vals, queries, out_grad, log_sums, inputs = refs[:7]
    query_grad, key_grad, value_grad, weight_grad = refs[7:11]
    m = dict(zip(names, refs[11:]))
    n_b = m["kraw"].shape[0]
    n_dev = n_z * PLANE
    heads = m["lraw"].shape[0]
    per_group = heads // 2
    cols = per_group * BLOCK
    z, q = place()
    y, c = q // N_C, q % N_C
    x = lax.axis_index("tp")

    barrier = pltpu.get_barrier_semaphore()
    partners = [{"kv": (z + r) % n_z * PLANE + q} for r in range(1, n_z)]
    partners += [{"kv": z * PLANE + (q + r) % PLANE} for r in range(1, PLANE)]
    right, left = {"tp": (x + 1) % n_x}, {"tp": (x + n_x - 1) % n_x}
    partners += [right, left]
    for who in partners:
        pl.semaphore_signal(barrier, inc=1, device_id=who, device_id_type=MESH)

    loads = [
        pltpu.make_async_copy(src, dst, m["in_sem"].at[i])
        for i, (src, dst) in enumerate(
            [
                (keys, m["kraw"]),
                (vals, m["vraw"]),
                (queries, m["qraw"]),
                (out_grad, m["graw"]),
                (log_sums, m["lraw"]),
                (inputs, m["xraw"].at[0]),
            ]
        )
    ]
    for copy in loads:
        copy.start()
    up_z = {"kv": (z + 1) % n_z * PLANE + q}
    dn_z = {"kv": (z + n_z - 1) % n_z * PLANE + q}
    lane = lax.broadcasted_iota(jnp.int32, (BLOCK, 128), 1)
    low = lane < HD
    loads[0].wait()
    loads[1].wait()
    for b in range(n_b):
        k = m["kraw"][b].astype(F32)
        v = m["vraw"][b].astype(F32)
        kv0 = jnp.where(low, k, pltpu.roll(v, HD, 1)).astype(BF16)
        kv1 = jnp.where(low, pltpu.roll(k, HD, 1), v).astype(BF16)
        m["own0"][b] = kv0
        m["own1"][b] = kv1
        m["tab0"][n_dev + b] = kv0
        m["tab1"][n_dev + b] = kv1
    pl.semaphore_wait(barrier, len(partners))

    def held(g, way, step):
        return m[f"own{g}"] if step == 0 else m[f"held{g}{way}{step}"]

    def z_copy(g, way, step, part):
        blocks = pl.ds(part * (n_b // PARTS), n_b // PARTS)
        return pltpu.make_async_remote_copy(
            src_ref=held(g, way, step - 1).at[blocks],
            dst_ref=held(g, way, step).at[blocks],
            send_sem=m["sent"].at[0],
            recv_sem=m["z_recv"].at[g, way * 4 + step - 1, part],
            device_id=dn_z if way else up_z,
            device_id_type=MESH,
        )

    def sends(way, step):
        if way:
            return (z + step - 1) % n_z < 3
        return (z < n_z - 1) & (z - step + 1 >= 0)

    def gets(way, step):
        if way:
            return (z + step) % n_z < 3
        return z - step >= 0

    def steps(way):
        return 3 if way else 4

    def x_copy(to_right, rel, part):
        half = inputs.shape[0] // 2
        rows = pl.ds(part * half, half)
        slot = rel if to_right else n_x - rel
        if rel == 1:
            src = inputs.at[rows]
        else:
            src = m["xraw"].at[1 if to_right else n_x - 1, rows]
        side = 0 if to_right else 1
        return pltpu.make_async_remote_copy(
            src_ref=src,
            dst_ref=m["xraw"].at[slot, rows],
            send_sem=m["sent"].at[1],
            recv_sem=m["x_recv"].at[side, 2 if rel == 2 else part],
            device_id=right if to_right else left,
            device_id_type=MESH,
        )

    def y_copy(g, order, z_from, r):
        to = (q + r) % PLANE
        return pltpu.make_async_remote_copy(
            src_ref=m["picked"].at[g, order, r],
            dst_ref=m[f"tab{g}"].at[z_from * PLANE + q],
            send_sem=m["sent"].at[2],
            recv_sem=m["y_recv"].at[g, order],
            device_id={"kv": z * PLANE + to},
            device_id_type=MESH,
        )

    others = pl.ds(1, PLANE - 1)

    def wait_group(ref, sem):
        pltpu.make_async_copy(ref, ref, sem).wait()

    def pick(g, order, z_from, ref):
        def one(r, carry):
            to = (q + r) % PLANE
            m["picked"][g, order, r] = ref[idx[24 + g * n_z + z_from, to * n_b]]

            @pl.when(r > 1)
            def _():
                y_copy(g, order, z_from, r - 1).start()

            return carry

        lax.fori_loop(1, PLANE, one, 0)
        m[f"tab{g}"][z_from * PLANE + q] = ref[idx[24 + g * n_z + z_from, q * n_b]]
        y_copy(g, order, z_from, PLANE - 1).start()

    def each_piece(g, step, act):
        @pl.when(gets(0, step))
        def _():
            act(g, step, z - step, held(g, 0, step))

        if step < 4:
            @pl.when(gets(1, step) & (z + step >= n_z))
            def _():
                act(g, 4 + step, z + step - n_z, held(g, 1, step))

    def set_out(g):
        for part in range(PARTS):
            for way in range(2):
                @pl.when(sends(way, 1))
                def _():
                    z_copy(g, way, 1, part).start()

    set_out(0)
    for part in range(2):
        x_copy(True, 1, part).start()
        x_copy(False, 1, 1 - part).start()
    pick(0, 0, z, m["own0"])
    pick(1, 0, z, m["own1"])

    def relay(g, step):
        for part in range(PARTS):
            for way in range(2):
                if step <= steps(way):
                    @pl.when(gets(way, step))
                    def _():
                        z_copy(g, way, step, part).wait_recv()

                if step + 1 <= steps(way):
                    @pl.when(sends(way, step + 1))
                    def _():
                        z_copy(g, way, step + 1, part).start()

    key_at = lax.broadcasted_iota(jnp.int32, (BLOCK, cols), 0)
    tok_at = lax.broadcasted_iota(jnp.int32, (BLOCK, cols), 1) % BLOCK
    m["bias"][0] = jnp.zeros((BLOCK, cols), F32)
    m["bias"][1] = jnp.where(key_at <= tok_at, 0.0, NEG)
    m["bias"][2] = jnp.full((BLOCK, cols), NEG, F32)
    for p in range(n_b):
        m["terms"][p, n_list] = jnp.zeros((BLOCK, 128), F32)
    loads[4].wait()
    for p in range(n_b):
        for g in range(2):
            row = [
                m["lraw"][g * per_group + r : g * per_group + r + 1, p * BLOCK : (p + 1) * BLOCK]
                for r in range(per_group)
            ]
            m["lse"][p * 2 + g] = jnp.concatenate(row, axis=1)

    for step in range(1, 5):
        relay(0, step)
        if step == 2:
            set_out(1)
        each_piece(0, step, pick)

    def relay_and_pick(g, step):
        relay(g, step)
        each_piece(g, step, pick)

    def relay_x():
        x_copy(True, 1, 0).wait_recv()
        x_copy(True, 2, 0).start()
        x_copy(False, 1, 1).wait_recv()
        x_copy(False, 2, 1).start()

    def landed(g, order, z_from, ref):
        wait_group(m["picked"].at[g, order, others], m["y_recv"].at[g, order])

    def masked_rows(ref, row, g, factor, side):
        parts = []
        for r in range(per_group):
            col = (g * per_group + r) * HD
            part = ref[pl.ds(row, BLOCK), col // 128 * 128 : col // 128 * 128 + 128]
            part = part.astype(F32) * factor
            if r % 2 != side:
                part = pltpu.roll(part, HD, 1)
            parts.append(jnp.where(low != (side == 1), part, 0.0).astype(BF16))
        return parts

    def attention(g, between):
        tab = m[f"tab{g}"]
        sdp, pd, qd, cat, shift = m["sdp"], m["pd"], m["qd"], m["cat"], m["shift"]
        chunks = [slice(n, n + CHUNK) for n in range(0, n_list, CHUNK)]
        nt = (((1,), (1,)), ((), ()))
        nn = (((1,), (0,)), ((), ()))

        def one_position(p, carry):
            row = pl.multiple_of(p * BLOCK, BLOCK)
            for r, part in enumerate(masked_rows(m["qraw"], row, g, HD ** -0.5, 0)):
                qd[r * BLOCK : (r + 1) * BLOCK, :] = part
            for r, part in enumerate(masked_rows(m["graw"], row, g, 1.0, 1)):
                qd[cols + r * BLOCK : cols + (r + 1) * BLOCK, :] = part
            for n in range(n_list):
                cat[n] = tab[idx[p, g * n_list + n]]
            for kind in range(3):
                shift[kind] = m["bias"][kind] - m["lse"][p * 2 + g] * LOG2E

            acc = jnp.zeros((8, cols), F32)
            for ch in chunks:
                both = lax.dot_general(
                    cat[ch].reshape(CHUNK * BLOCK, 128), qd[...], nt, preferred_element_type=F32
                ).reshape(CHUNK, BLOCK, 2 * cols)
                for n in range(ch.start, ch.stop):
                    prod = both[n - ch.start]
                    pr = jnp.exp2(prod[:, :cols] * LOG2E + shift[idx[p, (2 + g) * n_list + n]])
                    sdp[n, :, :cols] = pr
                    sdp[n, :, cols:] = prod[:, cols:]
                    pd[n, :, cols:] = pr.astype(BF16)
                    pr = pr * prod[:, cols:]
                    acc = acc + pr.reshape(BLOCK // 8, 8, cols).sum(axis=0)
            delta = acc.sum(axis=0, keepdims=True)
            for ch in chunks:
                for n in range(ch.start, ch.stop):
                    ds = sdp[n, :, :cols] * (sdp[n, :, cols:] - delta)
                    pd[n, :, :cols] = ds.astype(BF16)
                m["terms"][p, ch] = lax.dot_general(
                    pd[ch].reshape(CHUNK * BLOCK, 2 * cols), qd[...], nn, preferred_element_type=F32
                ).reshape(CHUNK, BLOCK, 128)
            dq_t = lax.dot_general(
                cat[...].reshape(n_list * BLOCK, 128),
                pd[:, :, :cols].reshape(n_list * BLOCK, cols),
                (((0,), (0,)), ((), ())),
                preferred_element_type=F32,
            )
            dq = dq_t.T * (HD ** -0.5)
            for pair in range(per_group // 2):
                even = dq[(2 * pair) * BLOCK : (2 * pair + 1) * BLOCK]
                odd = dq[(2 * pair + 1) * BLOCK : (2 * pair + 2) * BLOCK]
                col = g * per_group * HD + pair * 128
                m["qg"][pl.ds(row, BLOCK), col : col + 128] = jnp.where(
                    low, even, pltpu.roll(odd, HD, 1)
                )
            for at, act in between.items():
                @pl.when(p == at)
                def _():
                    act()

            return carry

        lax.fori_loop(0, n_b, one_position, 0)

    def summed_terms(g, j):
        total = m["terms"][0, idx[8 + 8 * g, j]]
        for p in range(1, n_b):
            total = total + m["terms"][p, idx[8 + 8 * g + p, j]]
        return total

    def b_copy(g, d, r):
        to = (q + r) % PLANE
        return pltpu.make_async_remote_copy(
            src_ref=m["ret"].at[g, (z - d) * PLANE + to],
            dst_ref=m["back"].at[g, d, q],
            send_sem=m["sent"].at[3],
            recv_sem=m["b_recv"].at[g, d],
            device_id={"kv": z * PLANE + to},
            device_id_type=MESH,
        )

    def give_back(g):
        for d in RETURN_ORDER:
            @pl.when(z - d >= 0)
            def _():
                for r in list(range(1, PLANE)) + [0]:
                    j = (z - d) * PLANE + (q + r) % PLANE
                    m["ret"][g, j] = summed_terms(g, j).astype(BF16)
                for r in range(1, PLANE):
                    b_copy(g, d, r).start()

        def own(b, carry):
            m["own_tot"][g, b] = summed_terms(g, n_dev + b)
            return carry

        lax.fori_loop(0, n_b, own, 0)

    def accumulate(g, d, part):
        rows = slice(part * PART_ROWS, (part + 1) * PART_ROWS)
        accs = [jnp.zeros((PART_ROWS, 128), F32) for _ in range(n_b)]
        for r in range(PLANE):
            frm = (q + r) % PLANE
            if r == 0:
                val = m["ret"][g, (z - d) * PLANE + q, rows, :]
            else:
                val = m["back"][g, d, frm, rows, :]
            val = val.astype(F32)
            block = idx[24 + g * n_z + z - d, frm * n_b]
            for b in range(n_b):
                accs[b] = accs[b] + jnp.where(block == b, val, 0.0)
        for b in range(n_b):
            m["acc"][g, b, rows, :] = accs[b]

    def dn_copy(g, d, part):
        return pltpu.make_async_remote_copy(
            src_ref=m["zs"].at[g, d, part],
            dst_ref=m["zr_dn"].at[g, d - 1, part],
            send_sem=m["sent"].at[4],
            recv_sem=m["r_recv_dn"].at[g, d - 1, part],
            device_id=dn_z,
            device_id_type=MESH,
        )

    def up_copy(g, d, at, part):
        to = n_z - 1 if at else n_z - 1 - d
        return pltpu.make_async_remote_copy(
            src_ref=m["zs"].at[g, d, part],
            dst_ref=m["zr_up"].at[g, at, part],
            send_sem=m["sent"].at[4],
            recv_sem=m["r_recv_up"].at[g, at, part],
            device_id={"kv": to * PLANE + q},
            device_id_type=MESH,
        )

    def add_arrival(g, copy, ref, part):
        copy.wait_recv()
        rows = slice(part * PART_ROWS, (part + 1) * PART_ROWS)
        for b in range(n_b):
            m["acc"][g, b, rows, :] += ref[b].astype(F32)

    def dn_arrival(g, d, part):
        @pl.when(z < n_z - 1)
        def _():
            add_arrival(g, dn_copy(g, d, part), m["zr_dn"].at[g, d - 1, part], part)

    def up_arrival(g, at, part):
        add_arrival(g, up_copy(g, 5, at, part), m["zr_up"].at[g, at, part], part)

    def store_out(g, d, part):
        rows = slice(part * PART_ROWS, (part + 1) * PART_ROWS)
        for b in range(n_b):
            m["zs"][g, d, part, b] = m["acc"][g, b, rows, :].astype(BF16)

    def collect(g, d):
        @pl.when(z - d >= 0)
        def _():
            wait_group(m["back"].at[g, d, others], m["b_recv"].at[g, d])
            for part in range(ROW_PARTS):
                accumulate(g, d, part)
                if d < 4:
                    dn_arrival(g, d + 1, part)
                if d in (6, 7):
                    @pl.when(z == n_z - 1)
                    def _():
                        for at in {6: (2,), 7: (1, 3)}[d]:
                            up_arrival(g, at, part)

                if d == 0:
                    @pl.when(z < 3)
                    def _():
                        up_arrival(g, 0, part)
                    continue
                store_out(g, d, part)
                if d < 5:
                    dn_copy(g, d, part).start()
                else:
                    @pl.when(z == n_z - 1)
                    def _():
                        up_copy(g, d, 0, part).start()

                    for plane, at in {5: ((5, 1), (6, 2)), 6: ((6, 3),), 7: ()}[d]:
                        @pl.when(z == plane)
                        def _():
                            up_copy(g, d, at, part).start()

    def wait_fetch(g):
        landed(g, 0, z, None)
        for step in range(1, 5):
            each_piece(g, step, landed)

    relay_and_pick(1, 1)
    relay_and_pick(1, 2)
    loads[2].wait()
    loads[3].wait()
    wait_fetch(0)
    attention(
        0,
        {
            1: functools.partial(relay_and_pick, 1, 3),
            3: functools.partial(relay_and_pick, 1, 4),
            4: relay_x,
        },
    )
    give_back(0)
    wait_fetch(1)
    attention(1, {2 + i: functools.partial(collect, 0, RETURN_ORDER[i]) for i in range(3)})
    give_back(1)
    out_q = pltpu.make_async_copy(m["qg"], query_grad, m["out_sem"].at[0])
    out_q.start()
    def c_copy(g, i):
        return pltpu.make_async_remote_copy(
            src_ref=m["wpart"].at[g, i, 1 - c],
            dst_ref=m["crecv"].at[g, i],
            send_sem=m["sent"].at[5],
            recv_sem=m["c_recv"].at[g, i],
            device_id={"kv": z * PLANE + y * N_C + (1 - c)},
            device_id_type=MESH,
        )

    def wy_copy(g, part, r):
        to = (y + r) % N_Y
        return pltpu.make_async_remote_copy(
            src_ref=m["wy"].at[g, part, r],
            dst_ref=m["wyr"].at[g, part, r],
            send_sem=m["sent"].at[6],
            recv_sem=m["wy_recv"].at[g, part, r - 1],
            device_id={"kv": z * PLANE + to * N_C + c},
            device_id_type=MESH,
        )

    half = inputs.shape[1] // 2

    def combine(g):
        for b in range(n_b):
            total = m["acc"][g, b] + m["own_tot"][g, b]
            m["acc"][g, b] = total
            m["kg"][b * BLOCK : (b + 1) * BLOCK, :] = total.astype(BF16)
        m["kg_t"][...] = m["kg"][...].T

    def own_terms(g, i):
        w_t = [
            lax.dot_general(
                m["kg_t"][:HD, :], m["xraw"][i, :, h * half : (h + 1) * half],
                (((1,), (0,)), ((), ())), preferred_element_type=F32,
            )
            for h in range(2)
        ]
        w = jnp.concatenate(w_t, axis=0).T.astype(BF16)
        for yy in range(N_Y):
            for cc in range(N_C):
                first = (yy * N_C + cc) * BLOCK
                m["wpart"][g, i, cc, yy] = w[first : first + BLOCK]

    def core_sum(g, i):
        c_copy(g, i).wait_recv()
        for r in range(N_Y):
            yy = (y + r) % N_Y
            both = m["wpart"][g, i, c, yy].astype(F32) + m["crecv"][g, i, yy].astype(F32)
            if r:
                m["wy"][g, i // 2, r, i % 2] = both.astype(BF16)
            else:
                m["wy_own"][g, i] = both
        if i % 2:
            for r in (2, 1, 3):
                wy_copy(g, i // 2, r).start()

    def terms_out(g):
        combine(g)
        for i in range(n_x):
            own_terms(g, i)
            if i:
                c_copy(g, i - 1).start()
        c_copy(g, n_x - 1).start()

    for g, d in [
        (0, 2), (1, 4), (0, 6), (1, 5), (0, 1), (1, 3), (0, 7), (1, 6), (1, 2), (0, 0)
    ]:
        collect(g, d)
    x_copy(True, 1, 1).wait_recv()
    x_copy(False, 1, 0).wait_recv()
    x_copy(True, 2, 0).wait_recv()
    x_copy(False, 2, 1).wait_recv()
    loads[5].wait()
    terms_out(0)
    collect(1, 7)
    for i in range(n_x):
        core_sum(0, i)
    collect(1, 1)
    collect(1, 0)
    combine(1)
    lag = 2
    for i in range(n_x + lag):
        if i < n_x:
            own_terms(1, i)
        if 0 < i <= n_x:
            c_copy(1, i - 1).start()
        if i >= lag:
            core_sum(1, i - lag)
    for b in range(n_b):
        rows = slice(b * BLOCK, (b + 1) * BLOCK)
        t0, t1 = m["acc"][0, b], m["acc"][1, b]
        key_grad[rows, :] = jnp.where(low, t0, pltpu.roll(t1, HD, 1))
        value_grad[rows, :] = jnp.where(low, pltpu.roll(t0, HD, 1), t1)

    def z_of(i):
        return 2 * ((x + n_x - i // 2) % n_x) + i % 2

    def wz_copy(i):
        return pltpu.make_async_remote_copy(
            src_ref=m["wz"].at[i],
            dst_ref=m["wzr"].at[z],
            send_sem=m["sent"].at[7],
            recv_sem=m["wz_recv"].at[z],
            device_id={"kv": z_of(i) * PLANE + q},
            device_id_type=MESH,
        )

    def sent(g, order, z_from, ref):
        wait_group(m["picked"].at[g, order, others], m["sent"].at[2])

    for g in range(2):
        for way in range(2):
            for step in range(1, steps(way) + 1):
                @pl.when(sends(way, step))
                def _():
                    for part in range(PARTS):
                        z_copy(g, way, step, part).wait_send()

        sent(g, 0, z, None)
        for step in range(1, 5):
            each_piece(g, step, sent)
        for d in range(8):
            @pl.when(z - d >= 0)
            def _():
                wait_group(m["back"].at[g, d, others], m["sent"].at[3])

            for part in range(ROW_PARTS):
                if 0 < d < 5:
                    @pl.when(z - d >= 0)
                    def _():
                        dn_copy(g, d, part).wait_send()
                elif d:
                    @pl.when(z - d >= 0)
                    def _():
                        up_copy(g, d, 0, part).wait_send()

    for part in range(2):
        x_copy(True, 1, part).wait_send()
        x_copy(False, 1, part).wait_send()
    x_copy(True, 2, 0).wait_send()
    x_copy(False, 2, 1).wait_send()
    for g in range(2):
        for i in range(n_x):
            c_copy(g, i).wait_send()
    out_q.wait()

    for g, part in ((0, 0), (0, 1), (1, 0), (1, 1)):
        for r in (1, 3, 2):
            wy_copy(g, part, r).wait_recv()
        if g == 0:
            continue
        for i in (2 * part, 2 * part + 1):
            total = []
            for h in range(2):
                total.append(m["wy_own"][h, i])
                for r in range(1, N_Y):
                    total[h] = total[h] + m["wyr"][h, part, r, i % 2].astype(F32)
            tiles = [
                jnp.where(low, total[0], pltpu.roll(total[1], HD, 1)),
                jnp.where(low, pltpu.roll(total[0], HD, 1), total[1]),
            ]
            for h in range(2):
                m["wz_own"][2 * i + h] = tiles[h]
                m["wz"][2 * i + h] = tiles[h].astype(BF16)
        for i in range(4 * part, 4 * part + 4):
            @pl.when(z_of(i) != z)
            def _():
                wz_copy(i).start()
    for g in range(2):
        for part in range(2):
            for r in range(1, N_Y):
                wy_copy(g, part, r).wait_send()
    mine = 2 * ((x + n_x - z // 2) % n_x) + z % 2
    total = m["wz_own"][mine]
    for r in range(1, n_z):
        frm = (z + r) % n_z
        pltpu.make_async_remote_copy(
            src_ref=m["wz"].at[0],
            dst_ref=m["wzr"].at[frm],
            send_sem=m["sent"].at[7],
            recv_sem=m["wz_recv"].at[frm],
            device_id={"kv": frm * PLANE + q},
            device_id_type=MESH,
        ).wait_recv()
        total = total + m["wzr"][frm].astype(F32)
    weight_grad[...] = total
    for i in range(n_z):
        @pl.when(z_of(i) != z)
        def _():
            wz_copy(i).wait_send()


def put_kernel(q_src, k_src, v_src, w_src, q_dst, k_dst, v_dst, w_dst, sem):
    pairs = [(q_src, q_dst), (k_src, k_dst), (v_src, v_dst), (w_src, w_dst)]
    copies = [pltpu.make_async_copy(src, dst, sem.at[i]) for i, (src, dst) in enumerate(pairs)]
    for copy in copies:
        copy.start()
    for copy in copies:
        copy.wait()


def put_out(query_grad, key_grad, value_grad, weight_grad):
    hbm = pl.BlockSpec(memory_space=pltpu.HBM)
    vm = pl.BlockSpec(memory_space=pltpu.VMEM)
    arrays = (query_grad, key_grad, value_grad, weight_grad)
    return pl.pallas_call(
        put_kernel,
        out_shape=tuple(jax.ShapeDtypeStruct(a.shape, a.dtype) for a in arrays),
        in_specs=[vm] * 4,
        out_specs=(hbm,) * 4,
        scratch_shapes=[pltpu.SemaphoreType.DMA((4,))],
        compiler_params=pltpu.CompilerParams(vmem_limit_bytes=50 * 1024 * 1024),
        name="put_out",
    )(*arrays)


def index_kernel(n_dev, n_b, place_of, lists, out, flat):
    z, q = place_of()
    me = z * PLANE + q
    n_list = lists.shape[1]
    n_z = n_dev // PLANE
    width = lists.shape[2]
    heads = []
    for g in range(2):
        near = pltpu.roll(lists[g], (width - z * PLANE * n_b) % width, 1)[:, :128]
        heads.append(near)
        for plane in range(n_z):
            offs = near - (plane * PLANE + q) * n_b
            offs = jnp.where((offs >= 0) & (offs < n_b), offs, 0)
            out[24 + g * n_z + plane : 25 + g * n_z + plane, :] = offs.max(axis=0, keepdims=True)
    best = out[24 : 24 + 2 * n_z, :]
    widest = best
    for k in range(1, n_b):
        widest = jnp.maximum(widest, pltpu.roll(best, 128 - k, 1))
    out[24 : 24 + 2 * n_z, :] = widest
    both = pltpu.roll(jnp.concatenate(heads, axis=0), (128 - q * n_b) % 128, 1)
    flat[...] = jnp.zeros((128, 128), jnp.int32)
    flat[: 2 * n_list, :] = both
    entry = flat[...].T[:8, :]
    block = lax.broadcasted_iota(jnp.int32, (8, 128), 0)
    lane = lax.broadcasted_iota(jnp.int32, (8, 128), 1)
    owner = jnp.floor((entry.astype(F32) + 0.5) * (1.0 / n_b)).astype(jnp.int32)
    slot = jnp.where(owner == me, n_dev + entry - owner * n_b, jnp.maximum(owner, 0))
    kind = jnp.where(entry < 0, 2, jnp.where(entry == me * n_b + block, 1, 0))
    out[:8, :] = jnp.where(lane < 2 * n_list, slot, pltpu.roll(kind, 2 * n_list, 1))
    used = jnp.where(entry < 0, -1, slot)
    for g in range(2):
        found = jnp.full((8, 128), n_list, jnp.int32)
        for n in range(n_list):
            at = g * n_list + n
            found = jnp.where(used[:, at : at + 1] == lane, n, found)
        out[8 + 8 * g : 16 + 8 * g, :] = found


def index_table(chosen, n_b, n_dev, place_of=place, interpret=False):
    vm = pl.BlockSpec(memory_space=pltpu.VMEM)
    return pl.pallas_call(
        functools.partial(index_kernel, n_dev, n_b, place_of),
        out_shape=jax.ShapeDtypeStruct((24 + 2 * n_dev // PLANE, 128), jnp.int32),
        in_specs=[vm],
        out_specs=vm,
        scratch_shapes=[pltpu.VMEM((128, 128), jnp.int32)],
        compiler_params=pltpu.CompilerParams(vmem_limit_bytes=4 * 1024 * 1024),
        cost_estimate=pl.CostEstimate(flops=10**9, bytes_accessed=8 * 1024 * 1024, transcendentals=0),
        name="index",
        interpret=interpret,
    )(chosen.transpose(0, 2, 1))


def local(queries, key_heads, values, log_sums, out_grad, inputs, chosen):
    n_dev = lax.axis_size("kv")
    n_x = lax.axis_size("tp")
    rows, feats = inputs.shape
    n_b = rows // BLOCK
    heads = log_sums.shape[0]
    n_list = chosen.shape[2]
    idx = index_table(chosen, n_b, n_dev)
    scratch = scratch_list(rows, n_dev, n_x, n_list, feats, heads)
    hbm = pl.BlockSpec(memory_space=pltpu.HBM)
    vm = pl.BlockSpec(memory_space=pltpu.VMEM)
    results = pl.pallas_call(
        functools.partial(
            fused_kernel, [name for name, _ in scratch], n_dev // PLANE, n_x, n_list
        ),
        out_shape=(
            jax.ShapeDtypeStruct(queries.shape, F32),
            jax.ShapeDtypeStruct(key_heads.shape, F32),
            jax.ShapeDtypeStruct(values.shape, F32),
            jax.ShapeDtypeStruct((feats * n_x // n_dev, 128), F32),
        ),
        in_specs=[pl.BlockSpec(memory_space=pltpu.SMEM)] + [hbm] * 6,
        out_specs=(hbm, vm, vm, vm),
        scratch_shapes=[kind for _, kind in scratch],
        compiler_params=pltpu.CompilerParams(
            collective_id=0, has_side_effects=True, vmem_limit_bytes=50 * 1024 * 1024
        ),
        name="fused",
    )(
        idx,
        key_heads.reshape(n_b, BLOCK, -1),
        values.reshape(n_b, BLOCK, -1),
        queries,
        out_grad,
        log_sums,
        inputs,
    )
    return put_out(*results)


def solution(mesh):
    placed = (
        P("kv", "tp"),
        P("kv", "tp"),
        P("kv", "tp"),
        P("tp", "kv"),
        P("kv", "tp"),
        P("kv", "tp"),
        P("tp", None, None),
    )
    return jax.shard_map(
        local,
        mesh=mesh,
        in_specs=placed,
        out_specs=(P("kv", "tp"), P("kv", "tp"), P("kv", "tp"), P("kv", "tp")),
        check_vma=False,
    )
```
